32 devices in a mesh: grp: 2 (over y), sp: 4 (over z), tp: 4 (over x, core).
Axes of the slice: x: 2, y: 2, z: 4, core: 2. Of those that a mesh axis runs over, the one named last changes fastest.
Arguments:
- hidden: bfloat16 [3072, 2048], P(('grp', 'sp'), 'tp'), parts along dimension 0, may hold values from -45 to 45
- norm_gain: bfloat16 [2048], replicated, may hold values from 0.099609375 to 1.8984375
- w_query: bfloat16 [2048, 1024], P(None, 'tp'), may hold values from -0.125 to 0.125
- w_key: bfloat16 [2048, 1024], P(None, 'tp'), may hold values from -0.125 to 0.125
- w_value: bfloat16 [2048, 1024], P(None, 'tp'), may hold values from -0.125 to 0.125
- query_gain: float32 [8, 128], P('tp'), may hold values from 0.3 to 16
- key_gain: float32 [8, 128], P('tp'), may hold values from 0.3 to 16
- w_out: bfloat16 [1024, 2048], P('tp'), may hold values from -1.5 to 1.5
Outputs:
- mixed: bfloat16 [3072, 2048], P(('grp', 'sp'), 'tp'), parts along dimension 0
- log_total: float32 [3072, 8], P(('grp', 'sp'), 'tp'), parts along dimension 0
The draws below stay inside these ranges and needn't reach their ends.
There are 2 independent parts, one for each index of `grp`. The reference program is written for one: setup_inputs(seed, part) draws one part's arguments, and reference() takes and returns one part's arrays. A program takes and returns all parts, laid end to end along the dimension named above; an argument that names none is the same for every part. Nothing has to cross between parts.
All inputs are finite; a program needn't handle non-finite values.
Results may differ from the reference program's by a relative error of at most 0.015.
The reference program's roundings to bfloat16 on the way count: a program that leaves them out, or rounds other values in their place, can miss the bound.
Values may be sent and summed in bfloat16 or wider, within the bound.
No kernel may reach another device: no remote copies, remote signals or barrier semaphores. Data moves between devices by JAX's collectives and lax.ppermute only.
A program may use at most 64 MiB of HBM per device.

```python
import jax
import jax.numpy as jnp
from jax import lax

D = 2048
HEADS = 8
HEAD_DIM = 128
KEYS_BEHIND = 128
MIDDLE_DILATION = 4
WIDEST_DILATION = 16
TOKENS = 1536


def draw_hidden(key, part):
    row_key, col_key, base_key = jax.random.split(jax.random.fold_in(key, 17), 3)
    row_factor = jnp.exp(jax.random.uniform(row_key, (TOKENS, 1), jnp.float32, -1.2, 1.1))
    rising = 1.0 + 2.0 * jnp.arange(D, dtype=jnp.float32) / D
    col_factor = jnp.exp(jax.random.uniform(col_key, (1, D), jnp.float32, 0.0, 2.3)) * rising * 0.125
    base = jnp.clip(jax.random.normal(base_key, (TOKENS, D), jnp.float32), -4.0, 4.0)
    return (base * row_factor * col_factor).astype(jnp.bfloat16)


def head_gains(key, salt):
    channel_key = jax.random.fold_in(jax.random.fold_in(key, salt), 1)
    noise = jnp.clip(jax.random.normal(channel_key, (HEADS, HEAD_DIM), jnp.float32), -3.5, 3.5)
    return (1.0 + 0.18 * noise).astype(jnp.float32)


def draw_query_gain(key, part):
    return head_gains(key, 31)


def draw_key_gain(key, part):
    return head_gains(key, 47)


def block_levels(stream_key, shape, pieces, low, high):
    factor_of = 1.0
    for dim, parts in pieces:
        draws = jax.random.uniform(jax.random.fold_in(jax.random.fold_in(stream_key, 6), dim), (parts,), jnp.float32, low / len(pieces), high / len(pieces))
        factor_of = factor_of * jnp.repeat(jnp.exp(draws), shape[dim] // parts).reshape((-1,) + (1,) * (len(shape) - 1 - dim))
    return factor_of


def centred(key, dims, scale, bound, cuts=(), held_as=jnp.bfloat16):
    drawn = jax.random.normal(key, dims, jnp.float32) * scale
    if len(cuts) > 0:
        drawn = block_levels(key, dims, cuts, -0.22, 0.18) * drawn
    return jnp.clip(drawn, min=-bound, max=bound).astype(held_as)


def setup_inputs(seed: int = 0, part: int = 0) -> dict:
    seeds = jax.random.split(jax.random.key(seed), 9)
    part_splits = jax.random.split(jax.random.fold_in(seeds[8], part), 9)
    return {
        "hidden": draw_hidden(jax.random.fold_in(jax.random.fold_in(seeds[8], part), 71), part),
        "norm_gain": jnp.clip(1.0 + 0.18 * jax.random.normal(seeds[1], (D,), jnp.float32), 0.099609375, 1.8984375).astype(jnp.bfloat16),
        "w_query": centred(seeds[2], (D, HEADS * HEAD_DIM), D ** -0.5, 0.125, ((1, 4),)),
        "w_key": centred(seeds[3], (D, HEADS * HEAD_DIM), D ** -0.5, 0.125, ((1, 4),)),
        "w_value": centred(seeds[4], (D, HEADS * HEAD_DIM), D ** -0.5, 0.125, ((1, 4),)),
        "query_gain": draw_query_gain(jax.random.fold_in(seeds[8], 71), part),
        "key_gain": draw_key_gain(jax.random.fold_in(seeds[8], 71), part),
        "w_out": centred(seeds[7], (HEADS * HEAD_DIM, D), 16 ** -0.5, 1.5, ((0, 4),)),
    }


EPSILON = 1e-06
ROTARY_BASE = 500000.0

def rotate(values, positions):
    head_width = values.shape[-1]
    inverse = ROTARY_BASE ** (-jnp.arange(0, head_width, 2, dtype=jnp.float32) / head_width)
    angles = positions[:, None] * inverse[None, :]
    cosine = jnp.cos(angles)[:, None, :]
    sine = jnp.sin(angles)[:, None, :]
    half_width = head_width // 2
    first_half = values[..., :half_width]
    second_half = values[..., half_width:]
    return jnp.concatenate([first_half * cosine - second_half * sine, second_half * cosine + first_half * sine], axis=-1)

def head_norm(values, gains):
    normed = values * lax.rsqrt(lax.optimization_barrier(jnp.mean(values * values, axis=-1, keepdims=True)) + EPSILON)
    return normed * gains[None, :, :]

def dilated_branch(query, key_all, value_all, dilation_step):
    sequence_rows, head_count, head_width = query.shape
    class_rows = sequence_rows // dilation_step
    block_count = -(-class_rows // KEYS_BEHIND)
    padded_rows = block_count * KEYS_BEHIND

    def by_class(values):
        return values.reshape(class_rows, dilation_step, head_count, head_width).transpose(1, 0, 2, 3).astype(jnp.float32)
    query_blocks = jnp.pad(by_class(query), ((0, 0), (0, padded_rows - class_rows), (0, 0), (0, 0)))
    query_blocks = query_blocks.reshape(dilation_step, block_count, KEYS_BEHIND, head_count, head_width)

    def windows(values):
        padded = jnp.pad(by_class(values), ((0, 0), (KEYS_BEHIND, padded_rows - class_rows), (0, 0), (0, 0)))
        padded = padded.reshape(dilation_step, block_count + 1, KEYS_BEHIND, head_count, head_width)
        return jnp.concatenate([padded[:, :-1], padded[:, 1:]], axis=2)
    key_windows = windows(key_all)
    value_windows = windows(value_all)
    scores = jnp.einsum('rnqhd,rnkhd->rnhqk', query_blocks, key_windows) * head_width ** (-0.5)
    row_index = jnp.arange(KEYS_BEHIND, dtype=jnp.int32)[:, None]
    col_index = jnp.arange(2 * KEYS_BEHIND, dtype=jnp.int32)[None, :]
    distance = row_index + KEYS_BEHIND - col_index
    in_band = (distance >= 0) & (distance <= KEYS_BEHIND)
    class_index = jnp.arange(block_count, dtype=jnp.int32)[:, None] * KEYS_BEHIND + col_index - KEYS_BEHIND
    allowed = in_band[None, :, :] & (class_index >= 0)[:, None, :]
    scores = jnp.where(allowed[None, :, None, :, :], scores, -jnp.inf)
    row_max = lax.optimization_barrier(jnp.max(scores, axis=-1, keepdims=True))
    weights = jnp.exp(scores - row_max)
    weight_sum = lax.optimization_barrier(jnp.sum(weights, axis=-1))
    rounded = lax.optimization_barrier(weights.astype(jnp.bfloat16)).astype(jnp.float32)
    weighted = jnp.einsum('rnhqk,rnkhd->rnqhd', rounded, value_windows)
    branch_out = weighted / jnp.transpose(weight_sum, (0, 1, 3, 2))[..., None]
    branch_out = branch_out.reshape(dilation_step, padded_rows, head_count, head_width)[:, :class_rows]
    branch_out = branch_out.transpose(1, 0, 2, 3).reshape(sequence_rows, head_count, head_width)
    log_sum = jnp.transpose(row_max[..., 0] + jnp.log(weight_sum), (0, 1, 3, 2))
    log_sum = log_sum.reshape(dilation_step, padded_rows, head_count)[:, :class_rows]
    log_sum = log_sum.transpose(1, 0, 2).reshape(sequence_rows, head_count)
    return (branch_out, log_sum)

def reference(hidden, norm_gain, w_query, w_key, w_value, query_gain, key_gain, w_out):
    sequence_rows = hidden.shape[0]
    hidden_float = hidden.astype(jnp.float32)
    row_scale = lax.rsqrt(lax.optimization_barrier(jnp.mean(hidden_float * hidden_float, axis=1, keepdims=True)) + EPSILON)
    scaled = (hidden_float * norm_gain.astype(jnp.float32)[None, :]).astype(jnp.bfloat16)
    query_raw = jnp.dot(scaled, w_query, preferred_element_type=jnp.float32) * row_scale
    key_raw = jnp.dot(scaled, w_key, preferred_element_type=jnp.float32) * row_scale
    value_raw = jnp.dot(scaled, w_value, preferred_element_type=jnp.float32) * row_scale
    positions = jnp.arange(sequence_rows, dtype=jnp.int32).astype(jnp.float32)
    query = rotate(head_norm(query_raw.reshape(sequence_rows, HEADS, HEAD_DIM), query_gain), positions).astype(jnp.bfloat16)
    key_all = rotate(head_norm(key_raw.reshape(sequence_rows, HEADS, HEAD_DIM), key_gain), positions).astype(jnp.bfloat16)
    value_all = value_raw.astype(jnp.bfloat16).reshape(sequence_rows, HEADS, HEAD_DIM)
    branch_outs = []
    branch_logs = []
    for dilation_step in (1, MIDDLE_DILATION, WIDEST_DILATION):
        branch_out, log_sum = dilated_branch(query, key_all, value_all, dilation_step)
        branch_outs.append(branch_out)
        branch_logs.append(log_sum)
    stacked_logs = jnp.stack(branch_logs, axis=0)
    peak = lax.optimization_barrier(jnp.max(stacked_logs, axis=0))
    log_total = peak + jnp.log(lax.optimization_barrier(jnp.sum(jnp.exp(stacked_logs - peak[None]), axis=0)))
    shares = jnp.exp(stacked_logs - log_total[None])
    attended = lax.optimization_barrier(jnp.sum(shares[..., None] * jnp.stack(branch_outs, axis=0), axis=0))
    attended = attended.astype(jnp.bfloat16).reshape(sequence_rows, HEADS * HEAD_DIM)
    mixed = jnp.dot(attended, w_out, preferred_element_type=jnp.float32).astype(jnp.bfloat16)
    return (mixed, log_total)
```

```python
import functools
import math

import jax
import jax.numpy as jnp
from jax import lax
from jax.experimental import pallas as pl
from jax.experimental.pallas import tpu as pltpu
from jax.sharding import PartitionSpec as P

KEYS_BEHIND = 128
DILATIONS = (1, 4, 16)
EPSILON = 1e-06
ROTARY_BASE = 500000.0
MASKED = -1e30
ROW_BLOCK = 128

VMEM = pl.BlockSpec(memory_space=pltpu.VMEM)
SMEM = pl.BlockSpec(memory_space=pltpu.SMEM)


def swap(value, distance):
    count = lax.axis_size("tp")
    return lax.ppermute(value, "tp", [(i, i ^ distance) for i in range(count)])


def shift(value, steps):
    count = lax.axis_size("sp")
    return lax.ppermute(value, "sp", [(s, s + steps) for s in range(count - steps)])


def gather_blocks(block):
    count = lax.axis_size("tp")
    blocks = {0: block}
    distance = count // 2
    while distance:
        for k in list(blocks):
            blocks[k ^ distance] = swap(blocks[k], distance)
        distance //= 2
    return [blocks[k] for k in range(count)]


def turn_tables(positions, head_width):
    inverse = ROTARY_BASE ** (-jnp.arange(0, head_width, 2, dtype=jnp.float32) / head_width)
    angles = positions[:, None] * inverse[None, :]
    cosine = jnp.cos(angles)
    sine = jnp.sin(angles)
    return jnp.concatenate([cosine, cosine], 1), jnp.concatenate([-sine, sine], 1)


def project_kernel(where, *refs, count, head_count, width):
    hidden = refs[:count]
    gain, wq, wk, wv, qg, kg, cosine, sine, q_out, kv_out = refs[count:]
    me = where[0]
    piece = hidden[0].shape[1]
    rows = hidden[0].shape[0]
    head_width = qg.shape[1]
    for start in range(0, rows, ROW_BLOCK):
        span = pl.ds(start, ROW_BLOCK)
        sums = [None, None, None]
        squares = None
        for k in range(count):
            source = me ^ k
            raw = hidden[k][span, :].astype(jnp.float32)
            scaled = (raw * gain[pl.ds(source, 1), :]).astype(jnp.bfloat16)
            part = jnp.sum(raw * raw, axis=1, keepdims=True)
            squares = part if squares is None else squares + part
            at = pl.ds(pl.multiple_of(source * piece, piece), piece)
            for n, weight in enumerate((wq, wk, wv)):
                product = jnp.dot(scaled, weight[at, :], preferred_element_type=jnp.float32)
                sums[n] = product if sums[n] is None else sums[n] + product
        scale = lax.rsqrt(squares / width + EPSILON)
        turn_c = cosine[span, :]
        turn_s = sine[span, :]
        for n, (gains, out) in enumerate(((qg, q_out), (kg, kv_out.at[0]))):
            total = sums[n] * scale
            for h in range(head_count):
                values = total[:, h * head_width : (h + 1) * head_width]
                mean = jnp.mean(values * values, axis=1, keepdims=True)
                values = values * lax.rsqrt(mean + EPSILON) * gains[h : h + 1, :]
                turned = values * turn_c + pltpu.roll(values, head_width // 2, 1) * turn_s
                out[span, h * head_width : (h + 1) * head_width] = turned.astype(jnp.bfloat16)
        kv_out.at[1][span, :] = (sums[2] * scale).astype(jnp.bfloat16)


def project(where, blocks, gain, weights, gains, tables):
    rows, piece = blocks[0].shape
    count = len(blocks)
    local_width = weights[0].shape[1]
    head_count = gains[0].shape[0]
    return pl.pallas_call(
        functools.partial(
            project_kernel, count=count, head_count=head_count, width=piece * count
        ),
        out_shape=(
            jax.ShapeDtypeStruct((rows, local_width), jnp.bfloat16),
            jax.ShapeDtypeStruct((2, rows, local_width), jnp.bfloat16),
        ),
        in_specs=[SMEM] + [VMEM] * (count + 8),
        out_specs=(VMEM, VMEM),
        name="project",
    )(where, *blocks, gain, *weights, *gains, *tables)


def pair_bias(rows, distance):
    row = lax.broadcasted_iota(jnp.int32, (rows, rows), 0)
    col = lax.broadcasted_iota(jnp.int32, (rows, rows), 1)
    behind = row - col + distance * rows
    times = jnp.zeros((rows, rows), jnp.int32)
    for dilation in DILATIONS:
        read = (behind >= 0) & (behind <= KEYS_BEHIND * dilation) & (behind % dilation == 0)
        times = times + read.astype(jnp.int32)
    return jnp.where(
        times == 0,
        MASKED,
        jnp.where(times == 3, math.log2(3.0), (times - 1).astype(jnp.float32)),
    )


def attend_kernel(where, *refs, distance, first, last, head_width, factor):
    if first:
        q, kv, bias = refs[:3]
        outs = refs[3:]
    else:
        q, kv, bias, top_in, sum_in, acc_in = refs[:6]
        outs = refs[6:]
    rows, local_width = q.shape
    head_count = local_width // head_width

    def work(active):
        for start in range(0, rows, ROW_BLOCK):
            span = pl.ds(start, ROW_BLOCK)
            keys = start + ROW_BLOCK if distance == 0 else rows
            for h in range(head_count):
                lanes = slice(h * head_width, (h + 1) * head_width)
                if not first:
                    top = top_in[span, h : h + 1]
                    total = sum_in[span, h : h + 1]
                    acc = acc_in[span, lanes]
                if active:
                    scores = lax.dot_general(
                        q[span, lanes],
                        kv[0, :keys, lanes],
                        (((1,), (1,)), ((), ())),
                        preferred_element_type=jnp.float32,
                    )
                    scores = scores * factor + bias[span, :keys]
                    peak = jnp.max(scores, axis=1, keepdims=True)
                    if not first:
                        peak = jnp.maximum(peak, top)
                    weights = jnp.exp2(scores - peak)
                    part = jnp.sum(weights, axis=1, keepdims=True)
                    out = jnp.dot(
                        weights.astype(jnp.bfloat16),
                        kv[1, :keys, lanes],
                        preferred_element_type=jnp.float32,
                    )
                    if not first:
                        decay = jnp.exp2(top - peak)
                        part = part + total * decay
                        out = out + acc * decay
                    top, total, acc = peak, part, out
                if last:
                    outs[0][span, lanes] = (acc / total).astype(jnp.bfloat16)
                    outs[1][span, h : h + 1] = top * math.log(2.0) + jnp.log(total)
                else:
                    outs[0][span, h : h + 1] = top
                    outs[1][span, h : h + 1] = total
                    outs[2][span, lanes] = acc

    if first:
        work(True)
    else:
        pl.when(where[1] >= distance)(lambda: work(True))
        pl.when(where[1] < distance)(lambda: work(False))


def attend(where, q, kv, bias, carry, distance, last, head_width):
    rows, local_width = q.shape
    head_count = local_width // head_width
    first = carry is None
    if last:
        shapes = (
            jax.ShapeDtypeStruct((rows, local_width), jnp.bfloat16),
            jax.ShapeDtypeStruct((rows, head_count), jnp.float32),
        )
    else:
        shapes = (
            jax.ShapeDtypeStruct((rows, head_count), jnp.float32),
            jax.ShapeDtypeStruct((rows, head_count), jnp.float32),
            jax.ShapeDtypeStruct((rows, local_width), jnp.float32),
        )
    extra = () if first else carry
    return pl.pallas_call(
        functools.partial(
            attend_kernel,
            distance=distance,
            first=first,
            last=last,
            head_width=head_width,
            factor=head_width ** (-0.5) * math.log2(math.e),
        ),
        out_shape=shapes,
        in_specs=[SMEM] + [VMEM] * (3 + len(extra)),
        out_specs=(VMEM,) * len(shapes),
        name=f"attend{distance}",
    )(where, q, kv, bias, *extra)


def mix_kernel(where, attended, *refs):
    pieces, out = refs[:-1], refs[-1]
    me = where[0]
    for start in range(0, out.shape[0], ROW_BLOCK):
        span = pl.ds(start, ROW_BLOCK)
        total = None
        for k, piece in enumerate(pieces):
            product = jnp.dot(
                attended[me ^ k, span, :], piece[...], preferred_element_type=jnp.float32
            )
            total = product if total is None else total + product
        out[span, :] = total.astype(jnp.bfloat16)


def local(hidden, norm_gain, w_query, w_key, w_value, query_gain, key_gain, w_out):
    rows, piece = hidden.shape
    head_width = query_gain.shape[1]
    count = lax.axis_size("tp")
    shards = lax.axis_size("sp")
    me = lax.axis_index("tp")
    shard = lax.axis_index("sp")
    where = jnp.stack([me, shard]).astype(jnp.int32)

    positions = (jnp.arange(rows, dtype=jnp.int32) + shard * rows).astype(jnp.float32)
    tables = turn_tables(positions, head_width)
    gain = norm_gain.astype(jnp.float32).reshape(count, piece)
    reach = -(-KEYS_BEHIND * DILATIONS[-1] // rows)
    distances = range(1, min(shards - 1, reach) + 1)

    blocks = gather_blocks(hidden)
    q, kv = project(
        where, blocks, gain, (w_query, w_key, w_value), (query_gain, key_gain), tables
    )
    w_late, _ = lax.optimization_barrier((w_out, kv))
    others = [shift(kv, d) for d in distances]

    columns = w_out.shape[1] // count
    slices = [
        lax.dynamic_slice_in_dim(w_late, (me ^ k) * columns, columns, axis=1) for k in range(count)
    ]
    pieces = [slices[0]] + [swap(slices[k], k) for k in range(1, count)]

    carry = attend(where, q, kv, pair_bias(rows, 0), None, 0, not others, head_width)
    for d, other in zip(distances, others):
        carry = attend(where, q, other, pair_bias(rows, d), carry, d, d == len(others), head_width)
    attended, log_total = carry

    gathered = lax.all_gather(attended, "tp", axis=0, tiled=False)
    mixed = pl.pallas_call(
        mix_kernel,
        out_shape=jax.ShapeDtypeStruct((rows, columns), jnp.bfloat16),
        in_specs=[SMEM] + [VMEM] * (1 + count),
        out_specs=VMEM,
        name="mix",
    )(where, gathered, *pieces)
    return mixed, log_total


def solution(mesh):
    placed = (
        P(("grp", "sp"), "tp"),
        P(),
        P(None, "tp"),
        P(None, "tp"),
        P(None, "tp"),
        P("tp", None),
        P("tp", None),
        P("tp", None),
    )
    return jax.shard_map(
        local,
        mesh=mesh,
        in_specs=placed,
        out_specs=(P(("grp", "sp"), "tp"), P(("grp", "sp"), "tp")),
        check_vma=False,
    )
```

```python
import functools
import math

import jax
import jax.numpy as jnp
from jax import lax
from jax.experimental import pallas as pl
from jax.experimental.pallas import tpu as pltpu
from jax.sharding import PartitionSpec as P

KEYS_BEHIND = 128
DILATIONS = (1, 4, 16)
EPSILON = 1e-06
ROTARY_BASE = 500000.0
MASKED = -1e30
LANES = 128
LOG2_E = math.log2(math.e)

VMEM = pl.BlockSpec(memory_space=pltpu.VMEM)
SMEM = pl.BlockSpec(memory_space=pltpu.SMEM)


def shape_of(shape, dtype):
    return jax.ShapeDtypeStruct(shape, dtype)


def call(body, name, where, operands, outs, limit=24 << 20):
    return pl.pallas_call(
        body,
        out_shape=tuple(outs),
        in_specs=[SMEM] + [VMEM] * len(operands),
        out_specs=(VMEM,) * len(outs),
        compiler_params=pltpu.CompilerParams(vmem_limit_bytes=limit),
        name=name,
    )(where, *operands)


def wide(column):
    return jnp.broadcast_to(column, (column.shape[0], LANES))


def pair_bias(rows, distance):
    row = lax.broadcasted_iota(jnp.int32, (rows, rows), 0)
    col = lax.broadcasted_iota(jnp.int32, (rows, rows), 1)
    behind = row - col + distance * rows
    times = jnp.zeros((rows, rows), jnp.int32)
    for dilation in DILATIONS:
        read = (behind >= 0) & (behind <= KEYS_BEHIND * dilation)
        read = read & ((behind & (dilation - 1)) == 0)
        times = times + read.astype(jnp.int32)
    return jnp.where(
        times == 0,
        MASKED,
        jnp.where(times == 3, math.log2(3.0), (times - 1).astype(jnp.float32)),
    )


def sums_of(where, hidden, gain, weights, offsets):
    me = where[0]
    sums = [None] * len(weights)
    squares = None
    for block, k in zip(hidden, offsets):
        piece = block.shape[1]
        source = me ^ k
        raw = block[...].astype(jnp.float32)
        scaled = (raw * gain[pl.ds(source, 1), :]).astype(jnp.bfloat16)
        part = jnp.sum(raw * raw, axis=1, keepdims=True)
        squares = part if squares is None else squares + part
        at = pl.ds(pl.multiple_of(source * piece, piece), piece)
        for n, weight in enumerate(weights):
            product = jnp.dot(scaled, weight[at, :], preferred_element_type=jnp.float32)
            sums[n] = product if sums[n] is None else sums[n] + product
    return sums, squares


def early_kernel(where, *refs, offsets, kinds, biases):
    count = len(offsets)
    hidden = refs[:count]
    gain = refs[count]
    weights = refs[count + 1 : count + 1 + kinds]
    outs = refs[count + 1 + kinds :]
    sums, squares = sums_of(where, hidden, gain, weights, offsets)
    for out, total in zip(outs[:kinds], sums):
        out[...] = total
    outs[kinds][...] = wide(squares)
    for d, out in zip(biases, outs[kinds + 1 :]):
        out[...] = pair_bias(out.shape[0], d)


def head_turn(values, gains, cosine, sine):
    mean = jnp.mean(values * values, axis=1, keepdims=True)
    values = values * lax.rsqrt(mean + EPSILON) * gains
    return values * cosine + pltpu.roll(values, values.shape[1] // 2, 1) * sine


def late_kernel(where, *refs, offsets, kinds, width):
    count = len(offsets)
    hidden = refs[:count]
    gain = refs[count]
    weights = refs[count + 1 : count + 1 + kinds]
    rest = refs[count + 1 + kinds :]
    before = rest[:kinds]
    squares_before = rest[kinds]
    gains = rest[kinds + 1 : 2 * kinds]
    cosine, sine = rest[2 * kinds : 2 * kinds + 2]
    outs = rest[2 * kinds + 2 :]
    sums, squares = sums_of(where, hidden, gain, weights, offsets)
    scale = lax.rsqrt((squares + squares_before[...]) / width + EPSILON)
    head_width = gains[0].shape[1]
    turn_c = cosine[...]
    turn_s = sine[...]
    for n in range(kinds):
        for start in range(0, sums[n].shape[1], head_width):
            lanes = slice(start, start + head_width)
            h = start // head_width
            values = (sums[n][:, lanes] + before[n][:, lanes]) * scale
            if n < kinds - 1:
                values = head_turn(values, gains[n][h : h + 1, :], turn_c, turn_s)
            outs[n][:, lanes] = values.astype(jnp.bfloat16)


def softmax_part(q, blocks, lanes, factor):
    scores = []
    for key, _, bias in blocks:
        product = lax.dot_general(
            q[:, lanes], key[:, lanes], (((1,), (1,)), ((), ())), preferred_element_type=jnp.float32
        )
        scores.append(product * factor + bias)
    top = functools.reduce(
        jnp.maximum, [jnp.max(s, axis=1, keepdims=True) for s in scores]
    )
    total = None
    acc = None
    for s, (_, value, _) in zip(scores, blocks):
        weights = jnp.exp2(s - top)
        part = jnp.sum(weights, axis=1, keepdims=True)
        out = jnp.dot(
            weights.astype(jnp.bfloat16), value[:, lanes], preferred_element_type=jnp.float32
        )
        total = part if total is None else total + part
        acc = out if acc is None else acc + out
    return top, total, acc


def merge(parts):
    top = functools.reduce(jnp.maximum, [part[0] for part in parts])
    total = None
    acc = None
    for part_top, part_total, part_acc in parts:
        decay = jnp.exp2(part_top - top)
        total = part_total * decay if total is None else total + part_total * decay
        acc = part_acc * decay if acc is None else acc + part_acc * decay
    return acc / total, top + jnp.log2(total)


def head_lanes(q, head_width):
    count = q.shape[1] // head_width
    return [slice(h * head_width, (h + 1) * head_width) for h in range(count)]


def part_kernel(where, q, key, value, bias, tops, totals, accs, *, head_width, factor):
    for lanes in head_lanes(q, head_width):
        blocks = [(key, value, bias[...])]
        top, total, acc = softmax_part(q, blocks, lanes, factor)
        tops[:, lanes] = wide(top)
        totals[:, lanes] = wide(total)
        accs[:, lanes] = acc


def help_kernel(where, q, *refs, blocks, head_width, factor, helper):
    out, logs = refs[3 * blocks :]

    @pl.when(where[1] == helper)
    def _():
        for h, lanes in enumerate(head_lanes(q, head_width)):
            ready = [(refs[3 * n], refs[3 * n + 1], refs[3 * n + 2][...]) for n in range(blocks)]
            top, total, acc = softmax_part(q, ready, lanes, factor)
            out[:, lanes] = (acc / total).astype(jnp.bfloat16)
            logs[h : h + 1, :] = wide(top + jnp.log2(total)).T[:1, :]


def final_kernel(where, q, *refs, far, only, helped, head_width, factor):
    shard = where[1]
    near = refs[:6]
    kvs = refs[6 : 6 + 3 * len(far)]
    given = refs[6 + 3 * len(far) : -2]
    attended, logs = refs[-2:]
    rows = q.shape[0]

    def finish(use_far, use_given):
        for h, lanes in enumerate(head_lanes(q, head_width)):
            before = jnp.where(shard >= 1, near[3][:, lanes], MASKED)
            parts = [
                (near[0][:, lanes], near[1][:, lanes], near[2][:, lanes]),
                (before, near[4][:, lanes], near[5][:, lanes]),
            ]
            if use_far:
                blocks = [
                    (
                        kvs[3 * n],
                        kvs[3 * n + 1],
                        jnp.where(shard >= d, kvs[3 * n + 2][...], MASKED),
                    )
                    for n, d in enumerate(far)
                ]
                top, total, acc = softmax_part(q, blocks, lanes, factor)
                parts.append((wide(top), wide(total), acc))
            if use_given:
                top = jnp.broadcast_to(given[1][h : h + 1, :], (LANES, rows)).T
                parts.append((top, jnp.ones_like(top), given[0][:, lanes].astype(jnp.float32)))
            out, log_sum = merge(parts)
            attended[:, lanes] = out.astype(jnp.bfloat16)
            logs[h : h + 1, :] = (log_sum * math.log(2.0)).T[:1, :]

    with_far = (shard == only) if only is not None else (shard >= 2)
    with_given = (shard == helped) if helped is not None else (shard < 0)
    if far:
        pl.when(with_far)(lambda: finish(True, False))
    if helped is not None:
        pl.when(with_given)(lambda: finish(False, True))
    pl.when(jnp.logical_not(with_far | with_given))(lambda: finish(False, False))


def mix_kernel(where, attended, *refs):
    pieces, out = refs[:-1], refs[-1]
    me = where[0]
    total = None
    for k, piece in enumerate(pieces):
        product = jnp.dot(attended[me ^ k], piece[...], preferred_element_type=jnp.float32)
        total = product if total is None else total + product
    out[...] = total.astype(jnp.bfloat16)


def swap(value, distance):
    count = lax.axis_size("tp")
    return lax.ppermute(value, "tp", [(i, i ^ distance) for i in range(count)])


def behind(value, steps):
    count = lax.axis_size("sp")
    return lax.ppermute(value, "sp", [(s, s + steps) for s in range(count - steps)])


def near_blocks(block):
    blocks = {0: block}
    distance = lax.axis_size("tp") // 4
    while distance:
        for k in list(blocks):
            blocks[k ^ distance] = swap(blocks[k], distance)
        distance //= 2
    return [blocks[k] for k in sorted(blocks)]


def turn_tables(positions, head_width):
    inverse = ROTARY_BASE ** (-jnp.arange(0, head_width, 2, dtype=jnp.float32) / head_width)
    angles = positions[:, None] * inverse[None, :]
    cosine = jnp.cos(angles)
    sine = jnp.sin(angles)
    return jnp.concatenate([cosine, cosine], 1), jnp.concatenate([-sine, sine], 1)


def local(hidden, norm_gain, w_query, w_key, w_value, query_gain, key_gain, w_out):
    rows, piece = hidden.shape
    head_count, head_width = query_gain.shape
    local_width = head_count * head_width
    count = lax.axis_size("tp")
    shards = lax.axis_size("sp")
    half = count // 2
    me = lax.axis_index("tp")
    shard = lax.axis_index("sp")
    where = jnp.stack([me, shard]).astype(jnp.int32)
    factor = head_width ** (-0.5) * LOG2_E
    reach = -(-KEYS_BEHIND * DILATIONS[-1] // rows)
    distances = list(range(min(shards - 1, reach) + 1))
    helped = shards - 1 if shards == 4 and reach >= shards - 1 else None
    far = [2] if helped is not None else distances[2:]

    first = shard * rows
    steps = jnp.arange(rows, dtype=jnp.int32)
    tables = turn_tables((steps + first).astype(jnp.float32), head_width)
    tables_before = turn_tables((steps + first - rows).astype(jnp.float32), head_width)
    gain = norm_gain.astype(jnp.float32).reshape(count, piece)
    gains = (query_gain, key_gain)
    weights = (w_query, w_key, w_value)
    sums = shape_of((rows, local_width), jnp.float32)
    half_sum = shape_of((rows, local_width), jnp.bfloat16)
    lane_wide = shape_of((rows, LANES), jnp.float32)
    square = shape_of((rows, rows), jnp.float32)
    early = tuple(range(half))
    late = tuple(range(half, count))

    def begin(name, blocks, kinds, biases):
        return call(
            functools.partial(early_kernel, offsets=early, kinds=kinds, biases=biases),
            name,
            where,
            [*blocks, gain, *weights[3 - kinds :]],
            [sums] * kinds + [lane_wide] + [square] * len(biases),
        )

    def finish(name, blocks, kinds, begun, turn):
        return call(
            functools.partial(late_kernel, offsets=late, kinds=kinds, width=piece * count),
            name,
            where,
            [*blocks, gain, *weights[3 - kinds :], *begun, *gains[3 - kinds :], *turn],
            [half_sum] * kinds,
        )

    across = swap(hidden, half)
    own_near = near_blocks(hidden)
    before = behind(hidden, 1)

    begun = begin("early_own", own_near, 3, tuple(distances))
    biases = begun[4:]
    own_far = near_blocks(across)
    before_across = swap(before, half)
    q, key, value = finish("late_own", own_far, 3, begun[:4], tables)

    if helped is not None:
        visitor = lax.ppermute(q, "sp", [(helped, 1)])
        far_keys = [
            (lax.ppermute(key, "sp", [(0, 2)]), lax.ppermute(value, "sp", [(0, 2)]), biases[2])
        ]
    else:
        far_keys = [(behind(key, d), behind(value, d), biases[d]) for d in far]

    begun_before = begin("early_before", near_blocks(before), 2, ())
    own_part = call(
        functools.partial(part_kernel, head_width=head_width, factor=factor),
        "own_part",
        where,
        [q, key, value, biases[0]],
        [sums] * 3,
    )
    key_before, value_before = finish(
        "late_before", near_blocks(before_across), 2, begun_before, tables_before
    )
    given = []
    if helped is not None:
        out, logs = call(
            functools.partial(
                help_kernel, blocks=2, head_width=head_width, factor=factor, helper=1
            ),
            "help",
            where,
            [visitor, key, value, biases[2], key_before, value_before, biases[3]],
            [half_sum, shape_of((8, rows), jnp.float32)],
        )
        given = [lax.ppermute(out, "sp", [(1, helped)]), lax.ppermute(logs, "sp", [(1, helped)])]
    before_part = call(
        functools.partial(part_kernel, head_width=head_width, factor=factor),
        "before_part",
        where,
        [q, key_before, value_before, biases[1]],
        [sums] * 3,
    )

    columns = w_out.shape[1] // count
    w_late, _ = lax.optimization_barrier((w_out, before_across))
    slices = [
        lax.dynamic_slice_in_dim(w_late, (me ^ k) * columns, columns, axis=1) for k in range(count)
    ]
    pieces = [slices[0]] + [swap(slices[k], k) for k in range(1, count)]

    attended, logs = call(
        functools.partial(
            final_kernel,
            far=tuple(far),
            only=2 if helped is not None else None,
            helped=helped,
            head_width=head_width,
            factor=factor,
        ),
        "final",
        where,
        [q, *own_part, *before_part, *[x for block in far_keys for x in block], *given],
        [half_sum, shape_of((head_count, rows), jnp.float32)],
    )
    gathered = lax.all_gather(attended, "tp", axis=0, tiled=False)
    (mixed,) = call(
        mix_kernel, "mix", where, [gathered, *pieces], [shape_of((rows, columns), jnp.bfloat16)]
    )
    return mixed, logs.T


def solution(mesh):
    placed = (
        P(("grp", "sp"), "tp"),
        P(),
        P(None, "tp"),
        P(None, "tp"),
        P(None, "tp"),
        P("tp", None),
        P("tp", None),
        P("tp", None),
    )
    return jax.shard_map(
        local,
        mesh=mesh,
        in_specs=placed,
        out_specs=(P(("grp", "sp"), "tp"), P(("grp", "sp"), "tp")),
        check_vma=False,
    )
```

```python
import functools
import math

import jax
import jax.numpy as jnp
from jax import lax
from jax.experimental import pallas as pl
from jax.experimental.pallas import tpu as pltpu
from jax.sharding import PartitionSpec as P


KEYS_BEHIND = 128
DILATIONS = (1, 4, 16)
EPSILON = 1e-06
ROTARY_BASE = 500000.0
MASKED = -1e30
LANES = 128
LOG2_E = math.log2(math.e)


VMEM = pl.BlockSpec(memory_space=pltpu.VMEM)
SMEM = pl.BlockSpec(memory_space=pltpu.SMEM)


def shape_of(shape, dtype):
    return jax.ShapeDtypeStruct(shape, dtype)


def call(body, where, operands, outs, limit=24 << 20):
    return pl.pallas_call(
        body,
        out_shape=tuple(outs),
        in_specs=[SMEM] + [VMEM] * len(operands),
        out_specs=(VMEM,) * len(outs),
        compiler_params=pltpu.CompilerParams(vmem_limit_bytes=limit),
    )(where, *operands)


def wide(column):
    return jnp.broadcast_to(column, (column.shape[0], LANES))


def pair_bias(rows, distance):
    row = lax.broadcasted_iota(jnp.int32, (rows, rows), 0)
    col = lax.broadcasted_iota(jnp.int32, (rows, rows), 1)
    behind = row - col + distance * rows
    times = jnp.zeros((rows, rows), jnp.int32)
    for dilation in DILATIONS:
        read = (behind >= 0) & (behind <= KEYS_BEHIND * dilation)
        read = read & ((behind & (dilation - 1)) == 0)
        times = times + read.astype(jnp.int32)
    return jnp.where(
        times == 0,
        MASKED,
        jnp.where(times == 3, math.log2(3.0), (times - 1).astype(jnp.float32)),
    )


def sums_of(where, hidden, gain, weights, offsets):
    me = where[0]
    sums = [None] * len(weights)
    squares = None
    for block, k in zip(hidden, offsets):
        piece = block.shape[1]
        source = me ^ k
        raw = block[...].astype(jnp.float32)
        scaled = (raw * gain[pl.ds(source, 1), :]).astype(jnp.bfloat16)
        part = jnp.sum(raw * raw, axis=1, keepdims=True)
        squares = part if squares is None else squares + part
        at = pl.ds(pl.multiple_of(source * piece, piece), piece)
        for n, weight in enumerate(weights):
            product = jnp.dot(scaled, weight[at, :], preferred_element_type=jnp.float32)
            sums[n] = product if sums[n] is None else sums[n] + product
    return sums, squares


def early_kernel(where, *refs, offsets, kinds, biases):
    count = len(offsets)
    hidden = refs[:count]
    gain = refs[count]
    weights = refs[count + 1 : count + 1 + kinds]
    outs = refs[count + 1 + kinds :]
    sums, squares = sums_of(where, hidden, gain, weights, offsets)
    for out, total in zip(outs[:kinds], sums):
        out[...] = total
    outs[kinds][...] = wide(squares)
    for d, out in zip(biases, outs[kinds + 1 :]):
        out[...] = pair_bias(out.shape[0], d)


def head_turn(values, gains, cosine, sine):
    mean = jnp.mean(values * values, axis=1, keepdims=True)
    values = values * lax.rsqrt(mean + EPSILON) * gains
    return values * cosine + pltpu.roll(values, values.shape[1] // 2, 1) * sine


def late_kernel(where, *refs, offsets, kinds, width):
    count = len(offsets)
    hidden = refs[:count]
    gain = refs[count]
    weights = refs[count + 1 : count + 1 + kinds]
    rest = refs[count + 1 + kinds :]
    before = rest[:kinds]
    squares_before = rest[kinds]
    gains = rest[kinds + 1 : 2 * kinds]
    cosine, sine = rest[2 * kinds : 2 * kinds + 2]
    outs = rest[2 * kinds + 2 :]
    outs = [*outs[:-1], outs[-1].at[0], outs[-1].at[1]]
    sums, squares = sums_of(where, hidden, gain, weights, offsets)
    scale = lax.rsqrt((squares + squares_before[...]) / width + EPSILON)
    head_width = gains[0].shape[1]
    turn_c = jnp.concatenate([cosine[...], cosine[...]], axis=1)
    turn_s = jnp.concatenate([-sine[...], sine[...]], axis=1)
    for n in range(kinds):
        for start in range(0, sums[n].shape[1], head_width):
            lanes = slice(start, start + head_width)
            h = start // head_width
            values = (sums[n][:, lanes] + before[n][:, lanes]) * scale
            if n < kinds - 1:
                values = head_turn(values, gains[n][h : h + 1, :], turn_c, turn_s)
            outs[n][:, lanes] = values.astype(jnp.bfloat16)


def softmax_part(q, blocks, lanes, factor):
    scores = []
    for kv, bias in blocks:
        product = lax.dot_general(
            q[:, lanes], kv[0, :, lanes], (((1,), (1,)), ((), ())),
            preferred_element_type=jnp.float32,
        )
        scores.append(product * factor + bias)
    top = functools.reduce(jnp.maximum, [jnp.max(s, axis=1, keepdims=True) for s in scores])
    total = None
    acc = None
    for s, (kv, _) in zip(scores, blocks):
        weights = jnp.exp2(s - top)
        part = jnp.sum(weights, axis=1, keepdims=True)
        out = jnp.dot(
            weights.astype(jnp.bfloat16), kv[1, :, lanes], preferred_element_type=jnp.float32
        )
        total = part if total is None else total + part
        acc = out if acc is None else acc + out
    return top, total, acc


def merge(parts):
    top = functools.reduce(jnp.maximum, [part[0] for part in parts])
    total = None
    acc = None
    for part_top, part_total, part_acc in parts:
        decay = jnp.exp2(part_top - top)
        total = part_total * decay if total is None else total + part_total * decay
        acc = part_acc * decay if acc is None else acc + part_acc * decay
    return acc / total, top + jnp.log2(total)


def head_lanes(q, head_width):
    count = q.shape[1] // head_width
    return [slice(h * head_width, (h + 1) * head_width) for h in range(count)]


def part_kernel(where, q, kv, bias, tops, totals, accs, *, head_width, factor):
    for lanes in head_lanes(q, head_width):
        blocks = [(kv, bias[...])]
        top, total, acc = softmax_part(q, blocks, lanes, factor)
        tops[:, lanes] = wide(top)
        totals[:, lanes] = wide(total)
        accs[:, lanes] = acc


def help_kernel(where, q, *refs, blocks, head_width, factor, helper):
    out, logs = refs[2 * blocks :]

    @pl.when(where[1] == helper)
    def _():
        for h, lanes in enumerate(head_lanes(q, head_width)):
            ready = [(refs[2 * n], refs[2 * n + 1][...]) for n in range(blocks)]
            top, total, acc = softmax_part(q, ready, lanes, factor)
            out[:, lanes] = (acc / total).astype(jnp.bfloat16)
            logs[h : h + 1, :] = wide(top + jnp.log2(total)).T[:1, :]


def final_kernel(where, q, *refs, far, only, helped, head_width, factor):
    shard = where[1]
    near = refs[:6]
    kvs = refs[6 : 6 + 2 * len(far)]
    given = refs[6 + 2 * len(far) : -2]
    attended, logs = refs[-2:]
    rows = q.shape[0]

    def finish(use_far, use_given):
        for h, lanes in enumerate(head_lanes(q, head_width)):
            before = jnp.where(shard >= 1, near[3][:, lanes], MASKED)
            parts = [
                (near[0][:, lanes], near[1][:, lanes], near[2][:, lanes]),
                (before, near[4][:, lanes], near[5][:, lanes]),
            ]
            if use_far:
                blocks = [
                    (kvs[2 * n], jnp.where(shard >= d, kvs[2 * n + 1][...], MASKED))
                    for n, d in enumerate(far)
                ]
                top, total, acc = softmax_part(q, blocks, lanes, factor)
                parts.append((wide(top), wide(total), acc))
            if use_given:
                top = jnp.broadcast_to(given[1][h : h + 1, :], (LANES, rows)).T
                parts.append((top, jnp.ones_like(top), given[0][:, lanes].astype(jnp.float32)))
            out, log_sum = merge(parts)
            attended[:, lanes] = out.astype(jnp.bfloat16)
            logs[h : h + 1, :] = (log_sum * math.log(2.0)).T[:1, :]

    with_far = (shard == only) if only is not None else (shard >= 2)
    with_given = (shard == helped) if helped is not None else (shard < 0)
    if far:
        pl.when(with_far)(lambda: finish(True, False))
    if helped is not None:
        pl.when(with_given)(lambda: finish(False, True))
    pl.when(jnp.logical_not(with_far | with_given))(lambda: finish(False, False))


def mix_kernel(where, attended, *refs):
    pieces, out = refs[:-1], refs[-1]
    me = where[0]
    total = None
    for k, piece in enumerate(pieces):
        product = jnp.dot(attended[me ^ k], piece[...], preferred_element_type=jnp.float32)
        total = product if total is None else total + product
    out[...] = total.astype(jnp.bfloat16)


def swap(value, distance):
    count = lax.axis_size("tp")
    return lax.ppermute(value, "tp", [(i, i ^ distance) for i in range(count)])


def send(value, pairs):
    return lax.ppermute(value, "sp", pairs)


def behind(value, steps):
    count = lax.axis_size("sp")
    return send(value, [(s, s + steps) for s in range(count - steps)])


def near_blocks(block):
    blocks = {0: block}
    distance = lax.axis_size("tp") // 4
    while distance:
        for k in list(blocks):
            blocks[k ^ distance] = swap(blocks[k], distance)
        distance //= 2
    return [blocks[k] for k in sorted(blocks)]


def turn_tables(positions, head_width):
    inverse = ROTARY_BASE ** (-jnp.arange(0, head_width, 2, dtype=jnp.float32) / head_width)
    angles = positions[:, None] * inverse[None, :]
    return jnp.cos(angles), jnp.sin(angles)


def layer(hidden, norm_gain, w_query, w_key, w_value, query_gain, key_gain, w_out):
    rows, piece = hidden.shape
    head_count, head_width = query_gain.shape
    local_width = head_count * head_width
    count = lax.axis_size("tp")
    shards = lax.axis_size("sp")
    half = count // 2
    me = lax.axis_index("tp")
    shard = lax.axis_index("sp")
    where = jnp.stack([me, shard]).astype(jnp.int32)
    factor = head_width ** (-0.5) * LOG2_E
    reach = -(-KEYS_BEHIND * DILATIONS[-1] // rows)
    distances = list(range(min(shards - 1, reach) + 1))
    helped = shards - 1 if shards == 4 and reach >= shards - 1 else None
    far = [2] if helped is not None else distances[2:]

    first = shard * rows
    steps = jnp.arange(rows, dtype=jnp.int32)
    tables = turn_tables((steps + first).astype(jnp.float32), head_width)
    tables_before = turn_tables((steps + first - rows).astype(jnp.float32), head_width)
    gain = norm_gain.astype(jnp.float32).reshape(count, piece)
    gains = (query_gain, key_gain)
    weights = (w_query, w_key, w_value)
    sums = shape_of((rows, local_width), jnp.float32)
    half_sum = shape_of((rows, local_width), jnp.bfloat16)
    pair = shape_of((2, rows, local_width), jnp.bfloat16)
    lane_wide = shape_of((rows, LANES), jnp.float32)
    square = shape_of((rows, rows), jnp.float32)
    early = tuple(range(half))
    late = tuple(range(half, count))
    columns = w_out.shape[1] // count
    slices = [
        lax.dynamic_slice_in_dim(w_out, (me ^ k) * columns, columns, axis=1)
        for k in range(count)
    ]

    def begin(blocks, kinds, biases):
        return call(
            functools.partial(early_kernel, offsets=early, kinds=kinds, biases=biases),
            where,
            [*blocks, gain, *weights[3 - kinds :]],
            [sums] * kinds + [lane_wide] + [square] * len(biases),
        )

    def finish(blocks, kinds, begun, turn):
        return call(
            functools.partial(late_kernel, offsets=late, kinds=kinds, width=piece * count),
            where,
            [*blocks, gain, *weights[3 - kinds :], *begun, *gains[3 - kinds :], *turn],
            [half_sum] * (kinds - 2) + [pair],
        )

    def part(kv, bias):
        return call(
            functools.partial(part_kernel, head_width=head_width, factor=factor),
            where,
            [q, kv, bias],
            [sums] * 3,
        )

    across = swap(hidden, half)
    own_near = near_blocks(hidden)
    before = behind(hidden, 1)

    begun = begin(own_near, 3, tuple(distances))
    biases = begun[4:]
    own_far = near_blocks(across)
    before_across = swap(before, half)
    q, kv = finish(own_far, 3, begun[:4], tables)

    if helped is not None:
        visitor = send(q, [(helped, 1)])
        far_blocks = [(send(kv, [(0, 2)]), biases[2])]
    else:
        far_blocks = [(behind(kv, d), biases[d]) for d in far]

    begun_before = begin(near_blocks(before), 2, ())
    own_part = part(kv, biases[0])
    (kv_before,) = finish(near_blocks(before_across), 2, begun_before, tables_before)
    given = []
    if helped is not None:
        out, logs = call(
            functools.partial(
                help_kernel, blocks=2, head_width=head_width, factor=factor, helper=1
            ),
            where,
            [visitor, kv, biases[2], kv_before, biases[3]],
            [half_sum, shape_of((8, rows), jnp.float32)],
        )
        given = [send(out, [(1, helped)]), send(logs, [(1, helped)])]
    before_part = part(kv_before, biases[1])

    w_first, _ = lax.optimization_barrier((slices[-1], begun[3]))
    *w_rest, _ = lax.optimization_barrier((*slices[1:-1], begun_before[2]))
    pieces = [slices[0]]
    pieces += [swap(w_rest[k - 1], k) for k in range(1, count - 1)]
    pieces += [swap(w_first, count - 1)]

    attended, logs = call(
        functools.partial(
            final_kernel,
            far=tuple(far),
            only=2 if helped is not None else None,
            helped=helped,
            head_width=head_width,
            factor=factor,
        ),
        where,
        [q, *own_part, *before_part, *[x for block in far_blocks for x in block], *given],
        [half_sum, shape_of((head_count, rows), jnp.float32)],
    )
    gathered = lax.all_gather(attended, "tp", axis=0, tiled=False)
    (mixed,) = call(
        mix_kernel, where, [gathered, *pieces], [shape_of((rows, columns), jnp.bfloat16)]
    )
    return mixed, logs.T


def solution(mesh):
    placed = (
        P(("grp", "sp"), "tp"),
        P(),
        P(None, "tp"),
        P(None, "tp"),
        P(None, "tp"),
        P("tp", None),
        P("tp", None),
        P("tp", None),
    )
    return jax.shard_map(
        layer,
        mesh=mesh,
        in_specs=placed,
        out_specs=(P(("grp", "sp"), "tp"), P(("grp", "sp"), "tp")),
        check_vma=False,
    )
```

```python
import functools
import math

import jax
import jax.numpy as jnp
from jax import lax
from jax.experimental import pallas as pl
from jax.experimental.pallas import tpu as pltpu
from jax.sharding import PartitionSpec as P


KEYS_BEHIND = 128
DILATIONS = (1, 4, 16)
EPSILON = 1e-06
ROTARY_BASE = 500000.0
MASKED = -1e30
LANES = 128
LOG2_E = math.log2(math.e)


VMEM = pl.BlockSpec(memory_space=pltpu.VMEM)
SMEM = pl.BlockSpec(memory_space=pltpu.SMEM)


def shape_of(shape, dtype):
    return jax.ShapeDtypeStruct(shape, dtype)


def call(body, where, operands, outs, limit=24 << 20):
    return pl.pallas_call(
        body,
        out_shape=tuple(outs),
        in_specs=[SMEM] + [VMEM] * len(operands),
        out_specs=(VMEM,) * len(outs),
        compiler_params=pltpu.CompilerParams(vmem_limit_bytes=limit),
    )(where, *operands)


def wide(column):
    return jnp.broadcast_to(column, (column.shape[0], LANES))


def pair_bias(rows, distance):
    row = lax.broadcasted_iota(jnp.int32, (rows, rows), 0)
    col = lax.broadcasted_iota(jnp.int32, (rows, rows), 1)
    behind = row - col + distance * rows
    times = jnp.zeros((rows, rows), jnp.int32)
    for dilation in DILATIONS:
        read = (behind >= 0) & (behind <= KEYS_BEHIND * dilation)
        read = read & ((behind & (dilation - 1)) == 0)
        times = times + read.astype(jnp.int32)
    return jnp.where(
        times == 0,
        MASKED,
        jnp.where(times == 3, math.log2(3.0), (times - 1).astype(jnp.float32)),
    )


def sums_of(where, hidden, gain, weights, offsets):
    me = where[0]
    sums = [None] * len(weights)
    squares = None
    for block, k in zip(hidden, offsets):
        piece = block.shape[1]
        source = me ^ k
        raw = block[...].astype(jnp.float32)
        scaled = (raw * gain[pl.ds(source, 1), :]).astype(jnp.bfloat16)
        part = jnp.sum(raw * raw, axis=1, keepdims=True)
        squares = part if squares is None else squares + part
        at = pl.ds(pl.multiple_of(source * piece, piece), piece)
        for n, weight in enumerate(weights):
            product = jnp.dot(scaled, weight[at, :], preferred_element_type=jnp.float32)
            sums[n] = product if sums[n] is None else sums[n] + product
    return sums, squares


def early_kernel(where, *refs, offsets, kinds, biases, copies):
    count = len(offsets)
    hidden = refs[:count]
    gain = refs[count]
    weights = refs[count + 1 : count + 1 + kinds]
    small = refs[count + 1 + kinds : count + 1 + kinds + copies]
    outs = refs[count + 1 + kinds + copies :]
    sums, squares = sums_of(where, hidden, gain, weights, offsets)
    for out, total in zip(outs[:kinds], sums):
        out[...] = total
    outs[kinds][...] = wide(squares)
    for ref, out in zip(small, outs[kinds + 1 :]):
        out[...] = ref[...]
    for d, out in zip(biases, outs[kinds + 1 + copies :]):
        out[...] = pair_bias(out.shape[0], d)


def head_turn(values, gains, cosine, sine):
    mean = jnp.mean(values * values, axis=1, keepdims=True)
    values = values * lax.rsqrt(mean + EPSILON) * gains
    return values * cosine + pltpu.roll(values, values.shape[1] // 2, 1) * sine


def late_kernel(where, *refs, offsets, kinds, width):
    count = len(offsets)
    hidden = refs[:count]
    gain = refs[count]
    weights = refs[count + 1 : count + 1 + kinds]
    rest = refs[count + 1 + kinds :]
    before = rest[:kinds]
    squares_before = rest[kinds]
    gains = rest[kinds + 1 : 2 * kinds]
    cosine, sine = rest[2 * kinds : 2 * kinds + 2]
    outs = rest[2 * kinds + 2 :]
    outs = [*outs[:-1], outs[-1].at[0], outs[-1].at[1]]
    sums, squares = sums_of(where, hidden, gain, weights, offsets)
    scale = lax.rsqrt((squares + squares_before[...]) / width + EPSILON)
    head_width = gains[0].shape[1]
    turn_c = jnp.concatenate([cosine[...], cosine[...]], axis=1)
    turn_s = jnp.concatenate([-sine[...], sine[...]], axis=1)
    for n in range(kinds):
        for start in range(0, sums[n].shape[1], head_width):
            lanes = slice(start, start + head_width)
            h = start // head_width
            values = (sums[n][:, lanes] + before[n][:, lanes]) * scale
            if n < kinds - 1:
                values = head_turn(values, gains[n][h : h + 1, :], turn_c, turn_s)
            outs[n][:, lanes] = values.astype(jnp.bfloat16)


def softmax_part(q, blocks, lanes, factor):
    scores = []
    for kv, bias in blocks:
        product = lax.dot_general(
            q[:, lanes], kv[0, :, lanes], (((1,), (1,)), ((), ())),
            preferred_element_type=jnp.float32,
        )
        scores.append(product * factor + bias)
    top = functools.reduce(jnp.maximum, [jnp.max(s, axis=1, keepdims=True) for s in scores])
    total = None
    acc = None
    for s, (kv, _) in zip(scores, blocks):
        weights = jnp.exp2(s - top)
        part = jnp.sum(weights, axis=1, keepdims=True)
        out = jnp.dot(
            weights.astype(jnp.bfloat16), kv[1, :, lanes], preferred_element_type=jnp.float32
        )
        total = part if total is None else total + part
        acc = out if acc is None else acc + out
    return top, total, acc


def merge(parts):
    top = functools.reduce(jnp.maximum, [part[0] for part in parts])
    total = None
    acc = None
    for part_top, part_total, part_acc in parts:
        decay = jnp.exp2(part_top - top)
        total = part_total * decay if total is None else total + part_total * decay
        acc = part_acc * decay if acc is None else acc + part_acc * decay
    return acc / total, top + jnp.log2(total)


def head_lanes(q, head_width):
    count = q.shape[1] // head_width
    return [slice(h * head_width, (h + 1) * head_width) for h in range(count)]


def near_kernel(where, q, *refs, distances, head_width, factor):
    count = len(distances)
    tops, totals, accs = refs[2 * count :]
    for lanes in head_lanes(q, head_width):
        blocks = []
        for n, d in enumerate(distances):
            bias = refs[2 * n + 1][...]
            blocks.append((refs[2 * n], jnp.where(where[1] >= d, bias, MASKED) if d else bias))
        top, total, acc = softmax_part(q, blocks, lanes, factor)
        tops[:, lanes] = wide(top)
        totals[:, lanes] = wide(total)
        accs[:, lanes] = acc


def help_kernel(where, q, *refs, blocks, head_width, factor, helper):
    out, logs = refs[2 * blocks :]

    @pl.when(where[1] == helper)
    def _():
        for h, lanes in enumerate(head_lanes(q, head_width)):
            ready = [(refs[2 * n], refs[2 * n + 1][...]) for n in range(blocks)]
            top, total, acc = softmax_part(q, ready, lanes, factor)
            out[:, lanes] = (acc / total).astype(jnp.bfloat16)
            logs[h : h + 1, :] = wide(top + jnp.log2(total)).T[:1, :]


def final_kernel(where, q, *refs, far, only, helped, head_width, factor):
    shard = where[1]
    near = refs[:3]
    kvs = refs[3 : 3 + 2 * len(far)]
    given = refs[3 + 2 * len(far) : -2]
    attended, logs = refs[-2:]
    rows = q.shape[0]

    def finish(use_far, use_given):
        for h, lanes in enumerate(head_lanes(q, head_width)):
            parts = [tuple(ref[:, lanes] for ref in near)]
            if use_far:
                blocks = [
                    (kvs[2 * n], jnp.where(shard >= d, kvs[2 * n + 1][...], MASKED))
                    for n, d in enumerate(far)
                ]
                top, total, acc = softmax_part(q, blocks, lanes, factor)
                parts.append((wide(top), wide(total), acc))
            if use_given:
                top = jnp.broadcast_to(given[1][h : h + 1, :], (LANES, rows)).T
                parts.append((top, jnp.ones_like(top), given[0][:, lanes].astype(jnp.float32)))
            out, log_sum = merge(parts)
            attended[:, lanes] = out.astype(jnp.bfloat16)
            logs[:, lanes] = log_sum

    with_far = (shard == only) if only is not None else (shard >= 2)
    with_given = (shard == helped) if helped is not None else (shard < 0)
    if far:
        pl.when(with_far)(lambda: finish(True, False))
    if helped is not None:
        pl.when(with_given)(lambda: finish(False, True))
    pl.when(jnp.logical_not(with_far | with_given))(lambda: finish(False, False))


def products(blocks, pieces):
    total = None
    for block, piece in zip(blocks, pieces):
        product = jnp.dot(block[...], piece[...], preferred_element_type=jnp.float32)
        total = product if total is None else total + product
    return total


def mix_early_kernel(where, logs, *refs, count):
    total, rows = refs[2 * count :]
    total[...] = products(refs[:count], refs[count : 2 * count])
    for h in range(rows.shape[0]):
        lanes = slice(h * LANES, (h + 1) * LANES)
        rows[h : h + 1, :] = (logs[:, lanes] * math.log(2.0)).T[:1, :]


def mix_late_kernel(where, before, *refs, count):
    total = before[...] + products(refs[:count], refs[count : 2 * count])
    refs[-1][...] = total.astype(jnp.bfloat16)


def swap(value, distance):
    count = lax.axis_size("tp")
    return lax.ppermute(value, "tp", [(i, i ^ distance) for i in range(count)])


def send(value, pairs):
    return lax.ppermute(value, "sp", pairs)


def behind(value, steps):
    count = lax.axis_size("sp")
    return send(value, [(s, s + steps) for s in range(count - steps)])


def near_blocks(block):
    blocks = {0: block}
    distance = lax.axis_size("tp") // 4
    while distance:
        for k in list(blocks):
            blocks[k ^ distance] = swap(blocks[k], distance)
        distance //= 2
    return [blocks[k] for k in sorted(blocks)]


def turn_tables(positions, head_width):
    inverse = ROTARY_BASE ** (-jnp.arange(0, head_width, 2, dtype=jnp.float32) / head_width)
    angles = positions[:, None] * inverse[None, :]
    return jnp.cos(angles), jnp.sin(angles)


def layer(hidden, norm_gain, w_query, w_key, w_value, query_gain, key_gain, w_out):
    rows, piece = hidden.shape
    head_count, head_width = query_gain.shape
    local_width = head_count * head_width
    count = lax.axis_size("tp")
    shards = lax.axis_size("sp")
    half = count // 2
    me = lax.axis_index("tp")
    shard = lax.axis_index("sp")
    where = jnp.stack([me, shard]).astype(jnp.int32)
    factor = head_width ** (-0.5) * LOG2_E
    reach = -(-KEYS_BEHIND * DILATIONS[-1] // rows)
    distances = list(range(min(shards - 1, reach) + 1))
    helped = shards - 1 if shards == 4 and reach >= shards - 1 else None
    far = [2] if helped is not None else distances[2:]

    first = shard * rows
    steps = jnp.arange(rows, dtype=jnp.int32)
    tables = turn_tables((steps + first).astype(jnp.float32), head_width)
    tables_before = turn_tables((steps + first - rows).astype(jnp.float32), head_width)
    gain = norm_gain.astype(jnp.float32).reshape(count, piece)
    gains = (query_gain, key_gain)
    weights = (w_query, w_key, w_value)
    sums = shape_of((rows, local_width), jnp.float32)
    half_sum = shape_of((rows, local_width), jnp.bfloat16)
    pair = shape_of((2, rows, local_width), jnp.bfloat16)
    lane_wide = shape_of((rows, LANES), jnp.float32)
    square = shape_of((rows, rows), jnp.float32)
    early = tuple(range(half))
    late = tuple(range(half, count))
    columns = w_out.shape[1] // count
    slices = [
        lax.dynamic_slice_in_dim(w_out, (me ^ k) * columns, columns, axis=1)
        for k in range(count)
    ]

    def begin(blocks, kinds, biases, copied):
        return call(
            functools.partial(
                early_kernel, offsets=early, kinds=kinds, biases=biases, copies=len(copied)
            ),
            where,
            [*blocks, gain, *weights[3 - kinds :], *copied],
            [sums] * kinds
            + [lane_wide]
            + [shape_of(x.shape, x.dtype) for x in copied]
            + [square] * len(biases),
        )

    def finish(blocks, kinds, begun, turn):
        return call(
            functools.partial(late_kernel, offsets=late, kinds=kinds, width=piece * count),
            where,
            [*blocks, gain, *weights[3 - kinds :], *begun, *gains[3 - kinds :], *turn],
            [half_sum] * (kinds - 2) + [pair],
        )

    across = swap(hidden, half)
    own_near = near_blocks(hidden)
    before = behind(hidden, 1)

    begun = begin(own_near, 3, tuple(distances), gains)
    gains = begun[4:6]
    biases = begun[6:]
    own_far = near_blocks(across)
    before_across = swap(before, half)
    q, kv = finish(own_far, 3, begun[:4], tables)

    if helped is not None:
        visitor = send(q, [(helped, 1)])
        far_blocks = [(send(kv, [(0, 2)]), biases[2])]
    else:
        far_blocks = [(behind(kv, d), biases[d]) for d in far]

    begun_before = begin(near_blocks(before), 2, (), ())
    (kv_before,) = finish(near_blocks(before_across), 2, begun_before, tables_before)
    given = []
    if helped is not None:
        out, logs = call(
            functools.partial(
                help_kernel, blocks=2, head_width=head_width, factor=factor, helper=1
            ),
            where,
            [visitor, kv, biases[2], kv_before, biases[3]],
            [half_sum, shape_of((8, rows), jnp.float32)],
        )
        given = [send(out, [(1, helped)]), send(logs, [(1, helped)])]
    near = call(
        functools.partial(
            near_kernel, distances=(0, 1), head_width=head_width, factor=factor
        ),
        where,
        [q, kv, biases[0], kv_before, biases[1]],
        [sums] * 3,
    )

    w_first, _ = lax.optimization_barrier((slices[-1], begun_before[2]))
    *w_rest, _ = lax.optimization_barrier((*slices[1:-1], begun_before[2]))
    pieces = [slices[0]]
    pieces += [swap(w_rest[k - 1], k) for k in range(1, count - 1)]
    pieces += [swap(w_first, count - 1)]

    attended, logs = call(
        functools.partial(
            final_kernel,
            far=tuple(far),
            only=2 if helped is not None else None,
            helped=helped,
            head_width=head_width,
            factor=factor,
        ),
        where,
        [q, *near, *[x for block in far_blocks for x in block], *given],
        [half_sum, sums],
    )
    attended_across = swap(attended, half)
    mixed_shape = (rows, columns)
    partial_mix, log_rows = call(
        functools.partial(mix_early_kernel, count=half),
        where,
        [logs, *near_blocks(attended), *pieces[:half]],
        [shape_of(mixed_shape, jnp.float32), shape_of((head_count, rows), jnp.float32)],
    )
    (mixed,) = call(
        functools.partial(mix_late_kernel, count=half),
        where,
        [partial_mix, *near_blocks(attended_across), *pieces[half:]],
        [shape_of(mixed_shape, jnp.bfloat16)],
    )
    return mixed, log_rows.T


def solution(mesh):
    placed = (
        P(("grp", "sp"), "tp"),
        P(),
        P(None, "tp"),
        P(None, "tp"),
        P(None, "tp"),
        P("tp", None),
        P("tp", None),
        P("tp", None),
    )
    return jax.shard_map(
        layer,
        mesh=mesh,
        in_specs=placed,
        out_specs=(P(("grp", "sp"), "tp"), P(("grp", "sp"), "tp")),
        check_vma=False,
    )
```

```python
import functools
import math

import jax
import jax.numpy as jnp
from jax import lax
from jax.experimental import pallas as pl
from jax.experimental.pallas import tpu as pltpu
from jax.sharding import PartitionSpec as P


KEYS_BEHIND = 128
DILATIONS = (1, 4, 16)
EPSILON = 1e-06
ROTARY_BASE = 500000.0
MASKED = -1e30
LANES = 128
LOG2_E = math.log2(math.e)


VMEM = pl.BlockSpec(memory_space=pltpu.VMEM)


def shape_of(shape, dtype):
    return jax.ShapeDtypeStruct(shape, dtype)


def call(body, operands, outs, limit=24 << 20):
    return pl.pallas_call(
        body,
        out_shape=tuple(outs),
        in_specs=[VMEM] * len(operands),
        out_specs=(VMEM,) * len(outs),
        compiler_params=pltpu.CompilerParams(vmem_limit_bytes=limit),
    )(*operands)


def wide(column):
    return jnp.broadcast_to(column, (column.shape[0], LANES))


def pair_bias(rows, distance):
    row = lax.broadcasted_iota(jnp.int32, (rows, rows), 0)
    col = lax.broadcasted_iota(jnp.int32, (rows, rows), 1)
    behind = row - col + distance * rows
    times = jnp.zeros((rows, rows), jnp.int32)
    for dilation in DILATIONS:
        read = (behind >= 0) & (behind <= KEYS_BEHIND * dilation)
        read = read & ((behind & (dilation - 1)) == 0)
        times = times + read.astype(jnp.int32)
    return jnp.where(
        times == 0,
        MASKED,
        jnp.where(times == 3, math.log2(3.0), (times - 1).astype(jnp.float32)),
    )


def sums_of(hidden, gain, weights, offsets):
    me = lax.axis_index("tp")
    sums = [None] * len(weights)
    squares = None
    for block, k in zip(hidden, offsets):
        piece = block.shape[1]
        source = me ^ k
        raw = block[...].astype(jnp.float32)
        scaled = (raw * gain[pl.ds(source, 1), :]).astype(jnp.bfloat16)
        part = jnp.sum(raw * raw, axis=1, keepdims=True)
        squares = part if squares is None else squares + part
        at = pl.ds(pl.multiple_of(source * piece, piece), piece)
        for n, weight in enumerate(weights):
            product = jnp.dot(scaled, weight[at, :], preferred_element_type=jnp.float32)
            sums[n] = product if sums[n] is None else sums[n] + product
    return sums, squares


def early_kernel(*refs, offsets, kinds, biases, copies):
    count = len(offsets)
    hidden = refs[:count]
    gain = refs[count]
    weights = refs[count + 1 : count + 1 + kinds]
    small = refs[count + 1 + kinds : count + 1 + kinds + copies]
    outs = refs[count + 1 + kinds + copies :]
    sums, squares = sums_of(hidden, gain, weights, offsets)
    for out, total in zip(outs[:kinds], sums):
        out[...] = total
    outs[kinds][...] = wide(squares)
    for ref, out in zip(small, outs[kinds + 1 :]):
        out[...] = ref[...]
    for d, out in zip(biases, outs[kinds + 1 + copies :]):
        out[...] = pair_bias(out.shape[0], d)


def head_turn(values, gains, cosine, sine):
    mean = jnp.mean(values * values, axis=1, keepdims=True)
    values = values * lax.rsqrt(mean + EPSILON) * gains
    return values * cosine + pltpu.roll(values, values.shape[1] // 2, 1) * sine


def late_kernel(*refs, offsets, kinds, width):
    count = len(offsets)
    hidden = refs[:count]
    gain = refs[count]
    weights = refs[count + 1 : count + 1 + kinds]
    rest = refs[count + 1 + kinds :]
    before = rest[:kinds]
    squares_before = rest[kinds]
    gains = rest[kinds + 1 : 2 * kinds]
    cosine, sine = rest[2 * kinds : 2 * kinds + 2]
    outs = rest[2 * kinds + 2 :]
    outs = [*outs[:-1], outs[-1].at[0], outs[-1].at[1]]
    sums, squares = sums_of(hidden, gain, weights, offsets)
    scale = lax.rsqrt((squares + squares_before[...]) / width + EPSILON)
    head_width = gains[0].shape[1]
    turn_c = jnp.concatenate([cosine[...], cosine[...]], axis=1)
    turn_s = jnp.concatenate([-sine[...], sine[...]], axis=1)
    for n in range(kinds):
        for start in range(0, sums[n].shape[1], head_width):
            lanes = slice(start, start + head_width)
            h = start // head_width
            values = (sums[n][:, lanes] + before[n][:, lanes]) * scale
            if n < kinds - 1:
                values = head_turn(values, gains[n][h : h + 1, :], turn_c, turn_s)
            outs[n][:, lanes] = values.astype(jnp.bfloat16)


def softmax_part(q, blocks, lanes, factor):
    scores = []
    for kv, bias in blocks:
        product = lax.dot_general(
            q[:, lanes], kv[0, :, lanes], (((1,), (1,)), ((), ())),
            preferred_element_type=jnp.float32,
        )
        scores.append(product * factor + bias)
    top = functools.reduce(jnp.maximum, [jnp.max(s, axis=1, keepdims=True) for s in scores])
    total = None
    acc = None
    for s, (kv, _) in zip(scores, blocks):
        weights = jnp.exp2(s - top)
        part = jnp.sum(weights, axis=1, keepdims=True)
        out = jnp.dot(
            weights.astype(jnp.bfloat16), kv[1, :, lanes], preferred_element_type=jnp.float32
        )
        total = part if total is None else total + part
        acc = out if acc is None else acc + out
    return top, total, acc


def merge(parts):
    top = functools.reduce(jnp.maximum, [part[0] for part in parts])
    total = None
    acc = None
    for part_top, part_total, part_acc in parts:
        decay = jnp.exp2(part_top - top)
        total = part_total * decay if total is None else total + part_total * decay
        acc = part_acc * decay if acc is None else acc + part_acc * decay
    return acc / total, top + jnp.log2(total)


def head_lanes(q, head_width):
    count = q.shape[1] // head_width
    return [slice(h * head_width, (h + 1) * head_width) for h in range(count)]


def near_kernel(q, *refs, distances, head_width, factor):
    count = len(distances)
    tops, totals, accs = refs[2 * count :]
    for lanes in head_lanes(q, head_width):
        blocks = []
        for n, d in enumerate(distances):
            bias = refs[2 * n + 1][...]
            blocks.append((refs[2 * n], jnp.where(lax.axis_index("sp") >= d, bias, MASKED) if d else bias))
        top, total, acc = softmax_part(q, blocks, lanes, factor)
        tops[:, lanes] = wide(top)
        totals[:, lanes] = wide(total)
        accs[:, lanes] = acc


def help_kernel(q, *refs, blocks, head_width, factor, helper):
    out, logs = refs[2 * blocks :]

    @pl.when(lax.axis_index("sp") == helper)
    def _():
        for h, lanes in enumerate(head_lanes(q, head_width)):
            ready = [(refs[2 * n], refs[2 * n + 1][...]) for n in range(blocks)]
            top, total, acc = softmax_part(q, ready, lanes, factor)
            out[:, lanes] = (acc / total).astype(jnp.bfloat16)
            logs[h : h + 1, :] = wide(top + jnp.log2(total)).T[:1, :]


def late_help_kernel(*refs, late_count, late, help_now):
    late_in, rest = refs[:late_count], refs[late_count:]
    q, kv, bias, bias_before = rest[:4]
    kv_before, out, logs = rest[4:]
    late(*late_in, kv_before)
    help_now(q, kv, bias, kv_before, bias_before, out, logs)


def final_kernel(q, *refs, far, only, helped, head_width, factor):
    shard = lax.axis_index("sp")
    near = refs[:3]
    kvs = refs[3 : 3 + 2 * len(far)]
    given = refs[3 + 2 * len(far) : -2]
    attended, logs = refs[-2:]
    rows = q.shape[0]

    def finish(use_far, use_given):
        for h, lanes in enumerate(head_lanes(q, head_width)):
            parts = [tuple(ref[:, lanes] for ref in near)]
            if use_far:
                blocks = [
                    (kvs[2 * n], jnp.where(shard >= d, kvs[2 * n + 1][...], MASKED))
                    for n, d in enumerate(far)
                ]
                top, total, acc = softmax_part(q, blocks, lanes, factor)
                parts.append((wide(top), wide(total), acc))
            if use_given:
                top = jnp.broadcast_to(given[1][h : h + 1, :], (LANES, rows)).T
                parts.append((top, jnp.ones_like(top), given[0][:, lanes].astype(jnp.float32)))
            out, log_sum = merge(parts)
            attended[:, lanes] = out.astype(jnp.bfloat16)
            logs[:, lanes] = log_sum

    with_far = (shard == only) if only is not None else (shard >= 2)
    with_given = (shard == helped) if helped is not None else (shard < 0)
    if far:
        pl.when(with_far)(lambda: finish(True, False))
    if helped is not None:
        pl.when(with_given)(lambda: finish(False, True))
    pl.when(jnp.logical_not(with_far | with_given))(lambda: finish(False, False))


def products(blocks, pieces):
    total = None
    for block, piece in zip(blocks, pieces):
        product = jnp.dot(block[...], piece[...], preferred_element_type=jnp.float32)
        total = product if total is None else total + product
    return total


def mix_early_kernel(logs, *refs, count):
    total, rows = refs[2 * count :]
    total[...] = products(refs[:count], refs[count : 2 * count])
    for h in range(rows.shape[0]):
        lanes = slice(h * LANES, (h + 1) * LANES)
        rows[h : h + 1, :] = (logs[:, lanes] * math.log(2.0)).T[:1, :]


def mix_late_kernel(before, *refs, count, shared):
    blocks = [ref[...] for ref in refs[:count]]
    if shared:
        crossed = lax.axis_index("grp") == 0
        low, high = blocks
        blocks = [jnp.where(crossed, high, low), jnp.where(crossed, low, high)]
    total = before[...] + products(blocks, refs[count : 2 * count])
    refs[-1][...] = total.astype(jnp.bfloat16)


def swap(value, distance):
    count = lax.axis_size("tp")
    return lax.ppermute(value, "tp", [(i, i ^ distance) for i in range(count)])


def send(value, pairs):
    return lax.ppermute(value, "sp", pairs)


def behind(value, steps):
    count = lax.axis_size("sp")
    return send(value, [(s, s + steps) for s in range(count - steps)])


def near_blocks(block):
    blocks = {0: block}
    distance = lax.axis_size("tp") // 4
    while distance:
        for k in list(blocks):
            blocks[k ^ distance] = swap(blocks[k], distance)
        distance //= 2
    return [blocks[k] for k in sorted(blocks)]


def turn_tables(positions, head_width):
    inverse = ROTARY_BASE ** (-jnp.arange(0, head_width, 2, dtype=jnp.float32) / head_width)
    angles = positions[:, None] * inverse[None, :]
    return jnp.cos(angles), jnp.sin(angles)


def layer(hidden, norm_gain, w_query, w_key, w_value, query_gain, key_gain, w_out):
    rows, piece = hidden.shape
    head_count, head_width = query_gain.shape
    local_width = head_count * head_width
    count = lax.axis_size("tp")
    shards = lax.axis_size("sp")
    half = count // 2
    me = lax.axis_index("tp")
    shard = lax.axis_index("sp")
    factor = head_width ** (-0.5) * LOG2_E
    reach = -(-KEYS_BEHIND * DILATIONS[-1] // rows)
    distances = list(range(min(shards - 1, reach) + 1))
    helped = shards - 1 if shards == 4 and reach >= shards - 1 else None
    far = [2] if helped is not None else distances[2:]

    first = shard * rows
    steps = jnp.arange(rows, dtype=jnp.int32)
    tables = turn_tables((steps + first).astype(jnp.float32), head_width)
    tables_before = turn_tables((steps + first - rows).astype(jnp.float32), head_width)
    gain = norm_gain.astype(jnp.float32).reshape(count, piece)
    gains = (query_gain, key_gain)
    weights = (w_query, w_key, w_value)
    sums = shape_of((rows, local_width), jnp.float32)
    half_sum = shape_of((rows, local_width), jnp.bfloat16)
    pair = shape_of((2, rows, local_width), jnp.bfloat16)
    lane_wide = shape_of((rows, LANES), jnp.float32)
    square = shape_of((rows, rows), jnp.float32)
    early = tuple(range(half))
    late = tuple(range(half, count))
    columns = w_out.shape[1] // count
    copies = lax.axis_size("grp")
    copy = lax.axis_index("grp")
    shared = copies == 2 and count == 4

    def piece_for(k):
        return lax.dynamic_slice_in_dim(w_out, (me ^ k) * columns, columns, axis=1)

    own_slice, near_slice = piece_for(0), [piece_for(k) for k in range(1, half)]
    far_slice = [piece_for(3 - copy)] if shared else [piece_for(k) for k in late]

    def begin(blocks, kinds, biases, copied):
        return call(
            functools.partial(
                early_kernel, offsets=early, kinds=kinds, biases=biases, copies=len(copied)
            ),
            [*blocks, gain, *weights[3 - kinds :], *copied],
            [sums] * kinds
            + [lane_wide]
            + [shape_of(x.shape, x.dtype) for x in copied]
            + [square] * len(biases),
        )

    def finish(blocks, kinds, begun, turn):
        return call(
            functools.partial(late_kernel, offsets=late, kinds=kinds, width=piece * count),
            [*blocks, gain, *weights[3 - kinds :], *begun, *gains[3 - kinds :], *turn],
            [half_sum] * (kinds - 2) + [pair],
        )

    across = swap(hidden, half)
    own_near = near_blocks(hidden)
    before = behind(hidden, 1)

    begun = begin(own_near, 3, tuple(distances), gains)
    gains = begun[4:6]
    biases = begun[6:]
    own_far = near_blocks(across)
    before_across = swap(before, half)
    q, kv = finish(own_far, 3, begun[:4], tables)

    if helped is not None:
        visitor = send(q, [(helped, 1)])
        far_blocks = [(send(kv, [(0, 2)]), biases[2])]
    else:
        far_blocks = [(behind(kv, d), biases[d]) for d in far]

    begun_before = begin(near_blocks(before), 2, (), ())
    before_far = near_blocks(before_across)
    given = []
    if helped is None:
        (kv_before,) = finish(before_far, 2, begun_before, tables_before)
    else:
        operands = [*before_far, gain, *weights[1:], *begun_before, gains[1], *tables_before]
        kv_before, out, logs = call(
            functools.partial(
                late_help_kernel,
                late_count=len(operands),
                late=functools.partial(late_kernel, offsets=late, kinds=2, width=piece * count),
                help_now=functools.partial(
                    help_kernel, blocks=2, head_width=head_width, factor=factor, helper=1
                ),
            ),
            [*operands, visitor, kv, biases[2], biases[3]],
            [pair, half_sum, shape_of((8, rows), jnp.float32)],
        )
        given = [send(out, [(1, helped)]), send(logs, [(1, helped)])]
    near = call(
        functools.partial(
            near_kernel, distances=(0, 1), head_width=head_width, factor=factor
        ),
        [q, kv, biases[0], kv_before, biases[1]],
        [sums] * 3,
    )

    *far_slice, _ = lax.optimization_barrier((*far_slice, begun_before[2]))
    *near_slice, _ = lax.optimization_barrier((*near_slice, begun_before[2]))
    near_pieces = [own_slice] + [swap(x, k + 1) for k, x in enumerate(near_slice)]
    if shared:
        routes = [(g * 4 + t, g * 4 + (t ^ (3 - g))) for g in range(2) for t in range(4)]
        fetched = lax.ppermute(far_slice[0], ("grp", "tp"), routes)
        other = lax.ppermute(fetched, "grp", [(0, 1), (1, 0)])
        far_pieces = [fetched, other]
    else:
        far_pieces = [swap(x, k) for k, x in zip(late, far_slice)]

    attended, logs = call(
        functools.partial(
            final_kernel,
            far=tuple(far),
            only=2 if helped is not None else None,
            helped=helped,
            head_width=head_width,
            factor=factor,
        ),
        [q, *near, *[x for block in far_blocks for x in block], *given],
        [half_sum, sums],
    )
    attended_across = swap(attended, half)
    mixed_shape = (rows, columns)
    partial_mix, log_rows = call(
        functools.partial(mix_early_kernel, count=half),
        [logs, *near_blocks(attended), *near_pieces],
        [shape_of(mixed_shape, jnp.float32), shape_of((head_count, rows), jnp.float32)],
    )
    (mixed,) = call(
        functools.partial(mix_late_kernel, count=half, shared=shared),
        [partial_mix, *near_blocks(attended_across), *far_pieces],
        [shape_of(mixed_shape, jnp.bfloat16)],
    )
    return mixed, log_rows.T


def solution(mesh):
    placed = (
        P(("grp", "sp"), "tp"),
        P(),
        P(None, "tp"),
        P(None, "tp"),
        P(None, "tp"),
        P("tp", None),
        P("tp", None),
        P("tp", None),
    )
    return jax.shard_map(
        layer,
        mesh=mesh,
        in_specs=placed,
        out_specs=(P(("grp", "sp"), "tp"), P(("grp", "sp"), "tp")),
        check_vma=False,
    )
```

```python
import functools
import math

import jax
import jax.numpy as jnp
from jax import lax
from jax.experimental import pallas as pl
from jax.experimental.pallas import tpu as pltpu
from jax.sharding import PartitionSpec as P


KEYS_BEHIND = 128
DILATIONS = (1, 4, 16)
EPSILON = 1e-06
ROTARY_BASE = 500000.0
MASKED = -1e30
LANES = 128
LOG2_E = math.log2(math.e)


VMEM = pl.BlockSpec(memory_space=pltpu.VMEM)
HBM = pl.BlockSpec(memory_space=pltpu.HBM)


def shape_of(shape, dtype):
    return jax.ShapeDtypeStruct(shape, dtype)


def call(body, operands, outs, held=(), scratch=(), limit=24 << 20):
    return pl.pallas_call(
        body,
        out_shape=tuple(outs),
        in_specs=[HBM if n in held else VMEM for n in range(len(operands))],
        out_specs=(VMEM,) * len(outs),
        scratch_shapes=scratch,
        compiler_params=pltpu.CompilerParams(vmem_limit_bytes=limit),
    )(*[
        pltpu.with_memory_space_constraint(x, pltpu.HBM) if n in held else x
        for n, x in enumerate(operands)
    ])


def wide(column):
    return jnp.broadcast_to(column, (column.shape[0], LANES))


def pair_bias(rows, distance):
    row = lax.broadcasted_iota(jnp.int32, (rows, rows), 0)
    col = lax.broadcasted_iota(jnp.int32, (rows, rows), 1)
    behind = row - col + distance * rows
    times = jnp.zeros((rows, rows), jnp.int32)
    for dilation in DILATIONS:
        read = (behind >= 0) & (behind <= KEYS_BEHIND * dilation)
        read = read & ((behind & (dilation - 1)) == 0)
        times = times + read.astype(jnp.int32)
    return jnp.where(
        times == 0,
        MASKED,
        jnp.where(times == 3, math.log2(3.0), (times - 1).astype(jnp.float32)),
    )


def sums_of(hidden, gain, weights, offsets):
    me = lax.axis_index("tp")
    sums = [None] * len(weights)
    squares = None
    for block, k in zip(hidden, offsets):
        piece = block.shape[1]
        source = me ^ k
        raw = block[...].astype(jnp.float32)
        scaled = (raw * gain[pl.ds(source, 1), :]).astype(jnp.bfloat16)
        part = jnp.sum(raw * raw, axis=1, keepdims=True)
        squares = part if squares is None else squares + part
        at = pl.ds(pl.multiple_of(source * piece, piece), piece)
        for n, weight in enumerate(weights):
            product = jnp.dot(scaled, weight[at, :], preferred_element_type=jnp.float32)
            sums[n] = product if sums[n] is None else sums[n] + product
    return sums, squares


def first_kernel(*refs, count, kinds, pieces, columns):
    own = refs[0]
    others = refs[1:count]
    gain = refs[count]
    small = refs[count + 1 : count + 3]
    weights = refs[count + 3 : count + 3 + kinds]
    w_out = refs[count + 3 + kinds]
    outs = refs[count + 4 + kinds : -2]
    held, sems = refs[-2:]
    sums_out, outs = outs[: kinds + 1], outs[kinds + 1 :]
    small_out, outs = outs[:2], outs[2:]
    weights_out, outs = outs[:kinds], outs[kinds:]
    pieces_out, biases = outs[: len(pieces)], outs[len(pieces) :]
    me = lax.axis_index("tp")
    moves = [(own, held), *zip(weights, weights_out), *zip(small, small_out)]
    for k, out in zip(pieces, pieces_out):
        peer = me ^ (3 - lax.axis_index("grp") if k is None else k)
        at = pl.ds(pl.multiple_of(peer * columns, columns), columns)
        moves.append((w_out.at[:, at], out))
    moves = [pltpu.make_async_copy(src, dst, sems.at[n]) for n, (src, dst) in enumerate(moves)]
    for move in moves:
        move.start()
    for d, out in enumerate(biases):
        out[...] = pair_bias(out.shape[0], d)
    for move in moves[: kinds + 1]:
        move.wait()
    sums, squares = sums_of((held, *others), gain, weights_out, range(count))
    for out, total in zip(sums_out, sums):
        out[...] = total
    sums_out[kinds][...] = wide(squares)
    for move in moves[kinds + 1 :]:
        move.wait()


def early_kernel(*refs, offsets, kinds):
    count = len(offsets)
    hidden = refs[:count]
    gain = refs[count]
    weights = refs[count + 1 : count + 1 + kinds]
    outs = refs[count + 1 + kinds :]
    sums, squares = sums_of(hidden, gain, weights, offsets)
    for out, total in zip(outs[:kinds], sums):
        out[...] = total
    outs[kinds][...] = wide(squares)


def head_turn(values, gains, cosine, sine):
    mean = jnp.mean(values * values, axis=1, keepdims=True)
    values = values * lax.rsqrt(mean + EPSILON) * gains
    return values * cosine + pltpu.roll(values, values.shape[1] // 2, 1) * sine


def late_kernel(*refs, offsets, kinds, width, given):
    count = len(offsets)
    hidden = refs[:count]
    gain = refs[count]
    weights = refs[count + 1 : count + 1 + kinds]
    rest = refs[count + 1 + kinds :]
    before = rest[:kinds]
    squares_before = rest[kinds]
    gains = rest[kinds + 1 : 2 * kinds]
    cosine, sine = rest[2 * kinds : 2 * kinds + 2]
    outs = rest[2 * kinds + 2 :]
    computed = before[0].shape[0]
    tail = None
    if given:
        received, pair = outs[-2:]
        outs = [pair.at[0], pair.at[1]]
        pair[:, computed:, :] = received[...]
    else:
        pair, tail = outs[-2:]
        outs = [*outs[:-2], pair.at[0], pair.at[1]]
    sums, squares = sums_of(hidden, gain, weights, offsets)
    scale = lax.rsqrt((squares + squares_before[...]) / width + EPSILON)
    head_width = gains[0].shape[1]
    turn_c = jnp.concatenate([cosine[...], cosine[...]], axis=1)
    turn_s = jnp.concatenate([-sine[...], sine[...]], axis=1)
    for n in range(kinds):
        for start in range(0, sums[n].shape[1], head_width):
            lanes = slice(start, start + head_width)
            h = start // head_width
            values = (sums[n][:, lanes] + before[n][:, lanes]) * scale
            if n < kinds - 1:
                values = head_turn(values, gains[n][h : h + 1, :], turn_c, turn_s)
            outs[n][:computed, lanes] = values.astype(jnp.bfloat16)
    if tail is not None:
        tail[...] = pair[:, computed - tail.shape[1] :, :]


def softmax_part(q, blocks, lanes, factor):
    scores = []
    for kv, bias in blocks:
        product = lax.dot_general(
            q[:, lanes], kv[0, :, lanes], (((1,), (1,)), ((), ())),
            preferred_element_type=jnp.float32,
        )
        scores.append(product * factor + bias)
    top = functools.reduce(jnp.maximum, [jnp.max(s, axis=1, keepdims=True) for s in scores])
    total = None
    acc = None
    for s, (kv, _) in zip(scores, blocks):
        weights = jnp.exp2(s - top)
        part = jnp.sum(weights, axis=1, keepdims=True)
        out = jnp.dot(
            weights.astype(jnp.bfloat16), kv[1, :, lanes], preferred_element_type=jnp.float32
        )
        total = part if total is None else total + part
        acc = out if acc is None else acc + out
    return top, total, acc


def merge(parts):
    top = functools.reduce(jnp.maximum, [part[0] for part in parts])
    total = None
    acc = None
    for part_top, part_total, part_acc in parts:
        decay = jnp.exp2(part_top - top)
        total = part_total * decay if total is None else total + part_total * decay
        acc = part_acc * decay if acc is None else acc + part_acc * decay
    return acc / total, top + jnp.log2(total)


def head_lanes(q, head_width):
    count = q.shape[1] // head_width
    return [slice(h * head_width, (h + 1) * head_width) for h in range(count)]


def near_kernel(q, *refs, distances, head_width, factor):
    count = len(distances)
    tops, totals, accs = refs[2 * count :]
    for lanes in head_lanes(q, head_width):
        blocks = []
        for n, d in enumerate(distances):
            bias = refs[2 * n + 1][...]
            blocks.append((refs[2 * n], jnp.where(lax.axis_index("sp") >= d, bias, MASKED) if d else bias))
        top, total, acc = softmax_part(q, blocks, lanes, factor)
        tops[:, lanes] = wide(top)
        totals[:, lanes] = wide(total)
        accs[:, lanes] = acc


def help_kernel(q, *refs, blocks, head_width, factor, helper):
    out, logs = refs[2 * blocks :]

    @pl.when(lax.axis_index("sp") == helper)
    def _():
        for h, lanes in enumerate(head_lanes(q, head_width)):
            ready = [(refs[2 * n], refs[2 * n + 1][...]) for n in range(blocks)]
            top, total, acc = softmax_part(q, ready, lanes, factor)
            out[:, lanes] = (acc / total).astype(jnp.bfloat16)
            logs[h : h + 1, :] = wide(top + jnp.log2(total)).T[:1, :]


def late_help_kernel(*refs, late_count, late, help_now):
    late_in, rest = refs[:late_count], refs[late_count:]
    q, kv, bias, bias_before = rest[:4]
    kv_before, out, logs = rest[4:]
    late(*late_in, kv_before)
    help_now(q, kv, bias, kv_before, bias_before, out, logs)


def final_kernel(q, *refs, far, only, helped, head_width, factor):
    shard = lax.axis_index("sp")
    near = refs[:3]
    kvs = refs[3 : 3 + 2 * len(far)]
    given = refs[3 + 2 * len(far) : -2]
    attended, logs = refs[-2:]
    rows = q.shape[0]

    def finish(use_far, use_given):
        for h, lanes in enumerate(head_lanes(q, head_width)):
            parts = [tuple(ref[:, lanes] for ref in near)]
            if use_far:
                blocks = [
                    (kvs[2 * n], jnp.where(shard >= d, kvs[2 * n + 1][...], MASKED))
                    for n, d in enumerate(far)
                ]
                top, total, acc = softmax_part(q, blocks, lanes, factor)
                parts.append((wide(top), wide(total), acc))
            if use_given:
                top = jnp.broadcast_to(given[1][h : h + 1, :], (LANES, rows)).T
                parts.append((top, jnp.ones_like(top), given[0][:, lanes].astype(jnp.float32)))
            out, log_sum = merge(parts)
            attended[:, lanes] = out.astype(jnp.bfloat16)
            logs[:, lanes] = log_sum

    with_far = (shard == only) if only is not None else (shard >= 2)
    with_given = (shard == helped) if helped is not None else (shard < 0)
    if far:
        pl.when(with_far)(lambda: finish(True, False))
    if helped is not None:
        pl.when(with_given)(lambda: finish(False, True))
    pl.when(jnp.logical_not(with_far | with_given))(lambda: finish(False, False))


def products(blocks, pieces):
    total = None
    for block, piece in zip(blocks, pieces):
        product = jnp.dot(block[...], piece[...], preferred_element_type=jnp.float32)
        total = product if total is None else total + product
    return total


def mix_early_kernel(logs, *refs, count):
    total, rows = refs[2 * count :]
    total[...] = products(refs[:count], refs[count : 2 * count])
    for h in range(rows.shape[0]):
        lanes = slice(h * LANES, (h + 1) * LANES)
        rows[h : h + 1, :] = (logs[:, lanes] * math.log(2.0)).T[:1, :]


def mix_late_kernel(before, *refs, count, shared):
    blocks = [ref[...] for ref in refs[:count]]
    if shared:
        crossed = lax.axis_index("grp") == 0
        low, high = blocks
        blocks = [jnp.where(crossed, high, low), jnp.where(crossed, low, high)]
    total = before[...] + products(blocks, refs[count : 2 * count])
    refs[-1][...] = total.astype(jnp.bfloat16)


def swap(value, distance):
    count = lax.axis_size("tp")
    return lax.ppermute(value, "tp", [(i, i ^ distance) for i in range(count)])


def send(value, pairs):
    return lax.ppermute(value, "sp", pairs)


def behind(value, steps):
    count = lax.axis_size("sp")
    return send(value, [(s, s + steps) for s in range(count - steps)])


def near_blocks(block):
    blocks = {0: block}
    distance = lax.axis_size("tp") // 4
    while distance:
        for k in list(blocks):
            blocks[k ^ distance] = swap(blocks[k], distance)
        distance //= 2
    return [blocks[k] for k in sorted(blocks)]


def turn_tables(positions, head_width):
    inverse = ROTARY_BASE ** (-jnp.arange(0, head_width, 2, dtype=jnp.float32) / head_width)
    angles = positions[:, None] * inverse[None, :]
    return jnp.cos(angles), jnp.sin(angles)


def layer(hidden, norm_gain, w_query, w_key, w_value, query_gain, key_gain, w_out):
    rows, piece = hidden.shape
    head_count, head_width = query_gain.shape
    local_width = head_count * head_width
    count = lax.axis_size("tp")
    shards = lax.axis_size("sp")
    half = count // 2
    shard = lax.axis_index("sp")
    factor = head_width ** (-0.5) * LOG2_E
    reach = -(-KEYS_BEHIND * DILATIONS[-1] // rows)
    distances = list(range(min(shards - 1, reach) + 1))
    helped = shards - 1 if shards == 4 and reach >= shards - 1 else None
    far = [2] if helped is not None else distances[2:]

    first = shard * rows
    steps = jnp.arange(rows, dtype=jnp.int32)
    tables = turn_tables((steps + first).astype(jnp.float32), head_width)
    tables_before = turn_tables((steps[: rows - rows // 3 // 16 * 16] + first - rows).astype(jnp.float32), head_width)
    gain = norm_gain.astype(jnp.float32).reshape(count, piece)
    gains = (query_gain, key_gain)
    weights = (w_query, w_key, w_value)
    sums = shape_of((rows, local_width), jnp.float32)
    half_sum = shape_of((rows, local_width), jnp.bfloat16)
    pair = shape_of((2, rows, local_width), jnp.bfloat16)
    lane_wide = shape_of((rows, LANES), jnp.float32)
    square = shape_of((rows, rows), jnp.float32)
    early = tuple(range(half))
    late = tuple(range(half, count))
    columns = w_out.shape[1] // count
    copies = lax.axis_size("grp")
    shared = copies == 2 and count == 4

    piece_keys = (0, *range(1, half), *((None,) if shared else late))
    piece_shape = shape_of((w_out.shape[0], columns), w_out.dtype)
    direct = rows // 3 // 16 * 16
    hidden_rows = rows - direct
    sums_before = shape_of((hidden_rows, local_width), jnp.float32)
    wide_before = shape_of((hidden_rows, LANES), jnp.float32)
    direct_pair = shape_of((2, direct, local_width), jnp.bfloat16)

    across = swap(hidden, half)
    rows_to_send = hidden[:hidden_rows]
    before = behind(rows_to_send, 1)
    own_near = near_blocks(hidden)

    operands = [*own_near, gain, *gains, *weights, w_out]
    fixed = [0, *range(half + 1, len(operands))]
    moves = len(weights) + 3 + len(piece_keys)
    begun = call(
        functools.partial(first_kernel, count=half, kinds=3, pieces=piece_keys, columns=columns),
        operands,
        [sums] * 3
        + [lane_wide]
        + [shape_of(x.shape, x.dtype) for x in (*gains, *weights)]
        + [piece_shape] * len(piece_keys)
        + [square] * len(distances),
        held=fixed,
        scratch=[pltpu.VMEM(hidden.shape, hidden.dtype), pltpu.SemaphoreType.DMA((moves,))],
    )
    begun, rest = begun[:4], begun[4:]
    gains, weights, rest = rest[:2], rest[2:5], rest[5:]
    slices, biases = rest[: len(piece_keys)], rest[len(piece_keys) :]
    own_slice, near_slice, far_slice = slices[0], slices[1:half], slices[half:]

    own_far = near_blocks(across)
    before_across = swap(before, half)
    width = piece * count
    q, kv, tail = call(
        functools.partial(late_kernel, offsets=late, kinds=3, width=width, given=False),
        [*own_far, gain, *weights, *begun, *gains, *tables],
        [half_sum, pair, direct_pair],
    )
    received = behind(tail, 1)

    if helped is not None:
        visitor = send(q, [(helped, 1)])
        far_blocks = [(send(kv, [(0, 2)]), biases[2])]
    else:
        far_blocks = [(behind(kv, d), biases[d]) for d in far]

    begun_before = call(
        functools.partial(early_kernel, offsets=early, kinds=2),
        [*near_blocks(before), gain, *weights[1:]],
        [sums_before] * 2 + [wide_before],
    )
    before_far = near_blocks(before_across)
    operands = [*before_far, gain, *weights[1:], *begun_before, gains[1], *tables_before, received]
    late_before = functools.partial(late_kernel, offsets=late, kinds=2, width=width, given=True)
    given = []
    if helped is None:
        (kv_before,) = call(late_before, operands, [pair])
    else:
        kv_before, out, logs = call(
            functools.partial(
                late_help_kernel,
                late_count=len(operands),
                late=late_before,
                help_now=functools.partial(
                    help_kernel, blocks=2, head_width=head_width, factor=factor, helper=1
                ),
            ),
            [*operands, visitor, kv, biases[2], biases[3]],
            [pair, half_sum, shape_of((8, rows), jnp.float32)],
        )
        given = [send(out, [(1, helped)]), send(logs, [(1, helped)])]
    near = call(
        functools.partial(
            near_kernel, distances=(0, 1), head_width=head_width, factor=factor
        ),
        [q, kv, biases[0], kv_before, biases[1]],
        [sums] * 3,
    )

    *far_slice, _ = lax.optimization_barrier((*far_slice, begun_before[2]))
    *near_slice, _ = lax.optimization_barrier((*near_slice, begun_before[2]))
    near_pieces = [own_slice] + [swap(x, k + 1) for k, x in enumerate(near_slice)]
    if shared:
        routes = [(g * 4 + t, g * 4 + (t ^ (3 - g))) for g in range(2) for t in range(4)]
        fetched = lax.ppermute(far_slice[0], ("grp", "tp"), routes)
        other = lax.ppermute(fetched, "grp", [(0, 1), (1, 0)])
        far_pieces = [fetched, other]
    else:
        far_pieces = [swap(x, k) for k, x in zip(late, far_slice)]

    attended, logs = call(
        functools.partial(
            final_kernel,
            far=tuple(far),
            only=2 if helped is not None else None,
            helped=helped,
            head_width=head_width,
            factor=factor,
        ),
        [q, *near, *[x for block in far_blocks for x in block], *given],
        [half_sum, sums],
    )
    attended_across = swap(attended, half)
    mixed_shape = (rows, columns)
    partial_mix, log_rows = call(
        functools.partial(mix_early_kernel, count=half),
        [logs, *near_blocks(attended), *near_pieces],
        [shape_of(mixed_shape, jnp.float32), shape_of((head_count, rows), jnp.float32)],
    )
    (mixed,) = call(
        functools.partial(mix_late_kernel, count=half, shared=shared),
        [partial_mix, *near_blocks(attended_across), *far_pieces],
        [shape_of(mixed_shape, jnp.bfloat16)],
    )
    return mixed, log_rows.T


def solution(mesh):
    placed = (
        P(("grp", "sp"), "tp"),
        P(),
        P(None, "tp"),
        P(None, "tp"),
        P(None, "tp"),
        P("tp", None),
        P("tp", None),
        P("tp", None),
    )
    return jax.shard_map(
        layer,
        mesh=mesh,
        in_specs=placed,
        out_specs=(P(("grp", "sp"), "tp"), P(("grp", "sp"), "tp")),
        check_vma=False,
    )
```

```python
import functools
import math

import jax
import jax.numpy as jnp
from jax import lax
from jax.experimental import pallas as pl
from jax.experimental.pallas import tpu as pltpu
from jax.sharding import PartitionSpec as P


KEYS_BEHIND = 128
DILATIONS = (1, 4, 16)
EPSILON = 1e-06
ROTARY_BASE = 500000.0
MASKED = -1e30
LANES = 128
LOG2_E = math.log2(math.e)


VMEM = pl.BlockSpec(memory_space=pltpu.VMEM)
HBM = pl.BlockSpec(memory_space=pltpu.HBM)


def shape_of(shape, dtype):
    return jax.ShapeDtypeStruct(shape, dtype)


def call(body, operands, outs, held=(), scratch=(), limit=24 << 20):
    return pl.pallas_call(
        body,
        out_shape=tuple(outs),
        in_specs=[HBM if n in held else VMEM for n in range(len(operands))],
        out_specs=(VMEM,) * len(outs),
        scratch_shapes=scratch,
        compiler_params=pltpu.CompilerParams(vmem_limit_bytes=limit),
    )(*[
        pltpu.with_memory_space_constraint(x, pltpu.HBM) if n in held else x
        for n, x in enumerate(operands)
    ])


def wide(column):
    return jnp.broadcast_to(column, (column.shape[0], LANES))


def pair_bias(rows, distance):
    row = lax.broadcasted_iota(jnp.int32, (rows, rows), 0)
    col = lax.broadcasted_iota(jnp.int32, (rows, rows), 1)
    behind = row - col + distance * rows
    times = jnp.zeros((rows, rows), jnp.int32)
    for dilation in DILATIONS:
        read = (behind >= 0) & (behind <= KEYS_BEHIND * dilation)
        read = read & ((behind & (dilation - 1)) == 0)
        times = times + read.astype(jnp.int32)
    return jnp.where(
        times == 0,
        MASKED,
        jnp.where(times == 3, math.log2(3.0), (times - 1).astype(jnp.float32)),
    )


def sums_of(hidden, gain, weights, offsets):
    me = lax.axis_index("tp")
    sums = [None] * len(weights)
    squares = None
    for block, k in zip(hidden, offsets):
        piece = block.shape[1]
        source = me ^ k
        raw = block[...].astype(jnp.float32)
        scaled = (raw * gain[pl.ds(source, 1), :]).astype(jnp.bfloat16)
        part = jnp.sum(raw * raw, axis=1, keepdims=True)
        squares = part if squares is None else squares + part
        at = pl.ds(pl.multiple_of(source * piece, piece), piece)
        for n, weight in enumerate(weights):
            product = jnp.dot(scaled, weight[at, :], preferred_element_type=jnp.float32)
            sums[n] = product if sums[n] is None else sums[n] + product
    return sums, squares


def first_kernel(*refs, count, kinds, pieces, columns):
    own = refs[0]
    others = refs[1:count]
    gain = refs[count]
    small = refs[count + 1 : count + 3]
    weights = refs[count + 3 : count + 3 + kinds]
    w_out = refs[count + 3 + kinds]
    outs = refs[count + 4 + kinds : -2]
    held, sems = refs[-2:]
    sums_out, outs = outs[: kinds + 1], outs[kinds + 1 :]
    small_out, outs = outs[:2], outs[2:]
    weights_out, outs = outs[:kinds], outs[kinds:]
    pieces_out, biases = outs[: len(pieces)], outs[len(pieces) :]
    me = lax.axis_index("tp")
    moves = [(own, held), *zip(weights, weights_out), *zip(small, small_out)]
    for k, out in zip(pieces, pieces_out):
        peer = me ^ (3 - lax.axis_index("grp") if k is None else k)
        at = pl.ds(pl.multiple_of(peer * columns, columns), columns)
        moves.append((w_out.at[:, at], out))
    moves = [pltpu.make_async_copy(src, dst, sems.at[n]) for n, (src, dst) in enumerate(moves)]
    for move in moves:
        move.start()
    for d, out in enumerate(biases):
        out[...] = pair_bias(out.shape[0], d)
    for move in moves[: kinds + 1]:
        move.wait()
    sums, squares = sums_of((held, *others), gain, weights_out, range(count))
    for out, total in zip(sums_out, sums):
        out[...] = total
    sums_out[kinds][...] = wide(squares)
    for move in moves[kinds + 1 :]:
        move.wait()


def early_kernel(*refs, offsets, kinds):
    count = len(offsets)
    hidden = refs[:count]
    gain = refs[count]
    weights = refs[count + 1 : count + 1 + kinds]
    outs = refs[count + 1 + kinds :]
    sums, squares = sums_of(hidden, gain, weights, offsets)
    for out, total in zip(outs[:kinds], sums):
        out[...] = total
    outs[kinds][...] = wide(squares)


def head_turn(values, gains, cosine, sine):
    mean = jnp.mean(values * values, axis=1, keepdims=True)
    values = values * lax.rsqrt(mean + EPSILON) * gains
    return values * cosine + pltpu.roll(values, values.shape[1] // 2, 1) * sine


def late_kernel(*refs, offsets, kinds, width):
    count = len(offsets)
    hidden = refs[:count]
    gain = refs[count]
    weights = refs[count + 1 : count + 1 + kinds]
    rest = refs[count + 1 + kinds :]
    before = rest[:kinds]
    squares_before = rest[kinds]
    gains = rest[kinds + 1 : 2 * kinds]
    cosine, sine = rest[2 * kinds : 2 * kinds + 2]
    outs = rest[2 * kinds + 2 :]
    outs = [*outs[:-1], outs[-1].at[0], outs[-1].at[1]]
    sums, squares = sums_of(hidden, gain, weights, offsets)
    scale = lax.rsqrt((squares + squares_before[...]) / width + EPSILON)
    head_width = gains[0].shape[1]
    turn_c = jnp.concatenate([cosine[...], cosine[...]], axis=1)
    turn_s = jnp.concatenate([-sine[...], sine[...]], axis=1)
    for n in range(kinds):
        for start in range(0, sums[n].shape[1], head_width):
            lanes = slice(start, start + head_width)
            h = start // head_width
            values = (sums[n][:, lanes] + before[n][:, lanes]) * scale
            if n < kinds - 1:
                values = head_turn(values, gains[n][h : h + 1, :], turn_c, turn_s)
            outs[n][:, lanes] = values.astype(jnp.bfloat16)


def softmax_part(q, blocks, lanes, factor):
    scores = []
    for kv, bias in blocks:
        product = lax.dot_general(
            q[:, lanes], kv[0, :, lanes], (((1,), (1,)), ((), ())),
            preferred_element_type=jnp.float32,
        )
        scores.append(product * factor + bias)
    top = functools.reduce(jnp.maximum, [jnp.max(s, axis=1, keepdims=True) for s in scores])
    total = None
    acc = None
    for s, (kv, _) in zip(scores, blocks):
        weights = jnp.exp2(s - top)
        part = jnp.sum(weights, axis=1, keepdims=True)
        out = jnp.dot(
            weights.astype(jnp.bfloat16), kv[1, :, lanes], preferred_element_type=jnp.float32
        )
        total = part if total is None else total + part
        acc = out if acc is None else acc + out
    return top, total, acc


def merge(parts):
    top = functools.reduce(jnp.maximum, [part[0] for part in parts])
    total = None
    acc = None
    for part_top, part_total, part_acc in parts:
        decay = jnp.exp2(part_top - top)
        total = part_total * decay if total is None else total + part_total * decay
        acc = part_acc * decay if acc is None else acc + part_acc * decay
    return acc / total, top + jnp.log2(total)


def head_lanes(q, head_width):
    count = q.shape[1] // head_width
    return [slice(h * head_width, (h + 1) * head_width) for h in range(count)]


def near_kernel(q, *refs, distances, head_width, factor):
    count = len(distances)
    tops, totals, accs = refs[2 * count :]
    for lanes in head_lanes(q, head_width):
        blocks = []
        for n, d in enumerate(distances):
            bias = refs[2 * n + 1][...]
            blocks.append((refs[2 * n], jnp.where(lax.axis_index("sp") >= d, bias, MASKED) if d else bias))
        top, total, acc = softmax_part(q, blocks, lanes, factor)
        tops[:, lanes] = wide(top)
        totals[:, lanes] = wide(total)
        accs[:, lanes] = acc


def help_kernel(q, *refs, blocks, head_width, factor, helper):
    out, logs = refs[2 * blocks :]

    @pl.when(lax.axis_index("sp") == helper)
    def _():
        for h, lanes in enumerate(head_lanes(q, head_width)):
            ready = [(refs[2 * n], refs[2 * n + 1][...]) for n in range(blocks)]
            top, total, acc = softmax_part(q, ready, lanes, factor)
            out[:, lanes] = (acc / total).astype(jnp.bfloat16)
            logs[h : h + 1, :] = wide(top + jnp.log2(total)).T[:1, :]


def late_help_kernel(*refs, late_count, late, help_now):
    late_in, rest = refs[:late_count], refs[late_count:]
    q, kv, bias, bias_before = rest[:4]
    kv_before, out, logs = rest[4:]
    late(*late_in, kv_before)
    help_now(q, kv, bias, kv_before, bias_before, out, logs)


def final_kernel(q, *refs, far, only, helped, head_width, factor):
    shard = lax.axis_index("sp")
    near = refs[:3]
    kvs = refs[3 : 3 + 2 * len(far)]
    given = refs[3 + 2 * len(far) : -2]
    attended, logs = refs[-2:]
    rows = q.shape[0]

    def finish(use_far, use_given):
        for h, lanes in enumerate(head_lanes(q, head_width)):
            parts = [tuple(ref[:, lanes] for ref in near)]
            if use_far:
                blocks = [
                    (kvs[2 * n], jnp.where(shard >= d, kvs[2 * n + 1][...], MASKED))
                    for n, d in enumerate(far)
                ]
                top, total, acc = softmax_part(q, blocks, lanes, factor)
                parts.append((wide(top), wide(total), acc))
            if use_given:
                top = jnp.broadcast_to(given[1][h : h + 1, :], (LANES, rows)).T
                parts.append((top, jnp.ones_like(top), given[0][:, lanes].astype(jnp.float32)))
            out, log_sum = merge(parts)
            attended[:, lanes] = out.astype(jnp.bfloat16)
            logs[:, lanes] = log_sum

    with_far = (shard == only) if only is not None else (shard >= 2)
    with_given = (shard == helped) if helped is not None else (shard < 0)
    if far:
        pl.when(with_far)(lambda: finish(True, False))
    if helped is not None:
        pl.when(with_given)(lambda: finish(False, True))
    pl.when(jnp.logical_not(with_far | with_given))(lambda: finish(False, False))


def products(blocks, pieces):
    total = None
    for block, piece in zip(blocks, pieces):
        product = jnp.dot(block[...], piece[...], preferred_element_type=jnp.float32)
        total = product if total is None else total + product
    return total


def mix_early_kernel(logs, *refs, count):
    total, rows = refs[2 * count :]
    total[...] = products(refs[:count], refs[count : 2 * count])
    for h in range(rows.shape[0]):
        lanes = slice(h * LANES, (h + 1) * LANES)
        rows[h : h + 1, :] = (logs[:, lanes] * math.log(2.0)).T[:1, :]


def mix_late_kernel(before, *refs, count, shared):
    blocks = [ref[...] for ref in refs[:count]]
    if shared:
        crossed = lax.axis_index("grp") == 0
        low, high = blocks
        blocks = [jnp.where(crossed, high, low), jnp.where(crossed, low, high)]
    total = before[...] + products(blocks, refs[count : 2 * count])
    refs[-1][...] = total.astype(jnp.bfloat16)


def swap(value, distance):
    count = lax.axis_size("tp")
    return lax.ppermute(value, "tp", [(i, i ^ distance) for i in range(count)])


def send(value, pairs):
    return lax.ppermute(value, "sp", pairs)


def behind(value, steps):
    count = lax.axis_size("sp")
    return send(value, [(s, s + steps) for s in range(count - steps)])


def near_blocks(block):
    blocks = {0: block}
    distance = lax.axis_size("tp") // 4
    while distance:
        for k in list(blocks):
            blocks[k ^ distance] = swap(blocks[k], distance)
        distance //= 2
    return [blocks[k] for k in sorted(blocks)]


def turn_tables(positions, head_width):
    inverse = ROTARY_BASE ** (-jnp.arange(0, head_width, 2, dtype=jnp.float32) / head_width)
    angles = positions[:, None] * inverse[None, :]
    return jnp.cos(angles), jnp.sin(angles)


def layer(hidden, norm_gain, w_query, w_key, w_value, query_gain, key_gain, w_out):
    rows, piece = hidden.shape
    head_count, head_width = query_gain.shape
    local_width = head_count * head_width
    count = lax.axis_size("tp")
    shards = lax.axis_size("sp")
    half = count // 2
    shard = lax.axis_index("sp")
    factor = head_width ** (-0.5) * LOG2_E
    reach = -(-KEYS_BEHIND * DILATIONS[-1] // rows)
    distances = list(range(min(shards - 1, reach) + 1))
    helped = shards - 1 if shards == 4 and reach >= shards - 1 else None
    far = [2] if helped is not None else distances[2:]

    first = shard * rows
    steps = jnp.arange(rows, dtype=jnp.int32)
    tables = turn_tables((steps + first).astype(jnp.float32), head_width)
    tables_before = turn_tables((steps + first - rows).astype(jnp.float32), head_width)
    gain = norm_gain.astype(jnp.float32).reshape(count, piece)
    gains = (query_gain, key_gain)
    weights = (w_query, w_key, w_value)
    sums = shape_of((rows, local_width), jnp.float32)
    half_sum = shape_of((rows, local_width), jnp.bfloat16)
    pair = shape_of((2, rows, local_width), jnp.bfloat16)
    lane_wide = shape_of((rows, LANES), jnp.float32)
    square = shape_of((rows, rows), jnp.float32)
    early = tuple(range(half))
    late = tuple(range(half, count))
    columns = w_out.shape[1] // count
    copies = lax.axis_size("grp")
    shared = copies == 2 and count == 4

    piece_keys = (0, *range(1, half), *((None,) if shared else late))
    piece_shape = shape_of((w_out.shape[0], columns), w_out.dtype)
    across = swap(hidden, half)
    before = behind(hidden, 1)
    own_near = near_blocks(hidden)

    operands = [*own_near, gain, *gains, *weights, w_out]
    fixed = [0, *range(half + 1, len(operands))]
    moves = len(weights) + 3 + len(piece_keys)
    begun = call(
        functools.partial(first_kernel, count=half, kinds=3, pieces=piece_keys, columns=columns),
        operands,
        [sums] * 3
        + [lane_wide]
        + [shape_of(x.shape, x.dtype) for x in (*gains, *weights)]
        + [piece_shape] * len(piece_keys)
        + [square] * len(distances),
        held=fixed,
        scratch=[pltpu.VMEM(hidden.shape, hidden.dtype), pltpu.SemaphoreType.DMA((moves,))],
    )
    begun, rest = begun[:4], begun[4:]
    gains, weights, rest = rest[:2], rest[2:5], rest[5:]
    slices, biases = rest[: len(piece_keys)], rest[len(piece_keys) :]
    own_slice, near_slice, far_slice = slices[0], slices[1:half], slices[half:]

    own_far = near_blocks(across)
    before_across = swap(before, half)
    width = piece * count
    q, kv = call(
        functools.partial(late_kernel, offsets=late, kinds=3, width=width),
        [*own_far, gain, *weights, *begun, *gains, *tables],
        [half_sum, pair],
    )

    if helped is not None:
        visitor = send(q, [(helped, 1)])
        far_blocks = [(send(kv, [(0, 2)]), biases[2])]
    else:
        far_blocks = [(behind(kv, d), biases[d]) for d in far]

    begun_before = call(
        functools.partial(early_kernel, offsets=early, kinds=2),
        [*near_blocks(before), gain, *weights[1:]],
        [sums] * 2 + [lane_wide],
    )
    before_far = near_blocks(before_across)
    operands = [*before_far, gain, *weights[1:], *begun_before, gains[1], *tables_before]
    late_before = functools.partial(late_kernel, offsets=late, kinds=2, width=width)
    given = []
    if helped is None:
        (kv_before,) = call(late_before, operands, [pair])
    else:
        kv_before, out, logs = call(
            functools.partial(
                late_help_kernel,
                late_count=len(operands),
                late=late_before,
                help_now=functools.partial(
                    help_kernel, blocks=2, head_width=head_width, factor=factor, helper=1
                ),
            ),
            [*operands, visitor, kv, biases[2], biases[3]],
            [pair, half_sum, shape_of((8, rows), jnp.float32)],
        )
        given = [send(out, [(1, helped)]), send(logs, [(1, helped)])]
    near = call(
        functools.partial(
            near_kernel, distances=(0, 1), head_width=head_width, factor=factor
        ),
        [q, kv, biases[0], kv_before, biases[1]],
        [sums] * 3,
    )

    *near_slice, _ = lax.optimization_barrier((*near_slice, begun_before[2]))
    near_pieces = [own_slice] + [swap(x, k + 1) for k, x in enumerate(near_slice)]
    if shared:
        routes = [(g * 4 + t, g * 4 + (t ^ (3 - g))) for g in range(2) for t in range(4)]
        fetched = lax.ppermute(far_slice[0], ("grp", "tp"), routes)
        other = lax.ppermute(fetched, "grp", [(0, 1), (1, 0)])
        far_pieces = [fetched, other]
    else:
        far_pieces = [swap(x, k) for k, x in zip(late, far_slice)]

    attended, logs = call(
        functools.partial(
            final_kernel,
            far=tuple(far),
            only=2 if helped is not None else None,
            helped=helped,
            head_width=head_width,
            factor=factor,
        ),
        [q, *near, *[x for block in far_blocks for x in block], *given],
        [half_sum, sums],
    )
    attended_across = swap(attended, half)
    mixed_shape = (rows, columns)
    partial_mix, log_rows = call(
        functools.partial(mix_early_kernel, count=half),
        [logs, *near_blocks(attended), *near_pieces],
        [shape_of(mixed_shape, jnp.float32), shape_of((head_count, rows), jnp.float32)],
    )
    (mixed,) = call(
        functools.partial(mix_late_kernel, count=half, shared=shared),
        [partial_mix, *near_blocks(attended_across), *far_pieces],
        [shape_of(mixed_shape, jnp.bfloat16)],
    )
    return mixed, log_rows.T


def solution(mesh):
    placed = (
        P(("grp", "sp"), "tp"),
        P(),
        P(None, "tp"),
        P(None, "tp"),
        P(None, "tp"),
        P("tp", None),
        P("tp", None),
        P("tp", None),
    )
    return jax.shard_map(
        layer,
        mesh=mesh,
        in_specs=placed,
        out_specs=(P(("grp", "sp"), "tp"), P(("grp", "sp"), "tp")),
        check_vma=False,
    )
```

```python
import functools
import math

import jax
import jax.numpy as jnp
from jax import lax
from jax.experimental import pallas as pl
from jax.experimental.pallas import tpu as pltpu
from jax.sharding import PartitionSpec as P


KEYS_BEHIND = 128
DILATIONS = (1, 4, 16)
EPSILON = 1e-06
ROTARY_BASE = 500000.0
MASKED = -1e30
LANES = 128
LOG2_E = math.log2(math.e)


VMEM = pl.BlockSpec(memory_space=pltpu.VMEM)
HBM = pl.BlockSpec(memory_space=pltpu.HBM)


def shape_of(shape, dtype):
    return jax.ShapeDtypeStruct(shape, dtype)


def call(body, operands, outs, held=(), scratch=(), limit=24 << 20):
    return pl.pallas_call(
        body,
        out_shape=tuple(outs),
        in_specs=[HBM if n in held else VMEM for n in range(len(operands))],
        out_specs=(VMEM,) * len(outs),
        scratch_shapes=scratch,
        compiler_params=pltpu.CompilerParams(vmem_limit_bytes=limit),
    )(*[
        pltpu.with_memory_space_constraint(x, pltpu.HBM) if n in held else x
        for n, x in enumerate(operands)
    ])


def wide(column):
    return jnp.broadcast_to(column, (column.shape[0], LANES))


def pair_bias(rows, distance):
    row = lax.broadcasted_iota(jnp.int32, (rows, rows), 0)
    col = lax.broadcasted_iota(jnp.int32, (rows, rows), 1)
    behind = row - col + distance * rows
    times = jnp.zeros((rows, rows), jnp.int32)
    for dilation in DILATIONS:
        read = (behind >= 0) & (behind <= KEYS_BEHIND * dilation)
        read = read & ((behind & (dilation - 1)) == 0)
        times = times + read.astype(jnp.int32)
    return jnp.where(
        times == 0,
        MASKED,
        jnp.where(times == 3, math.log2(3.0), (times - 1).astype(jnp.float32)),
    )


def sums_of(hidden, gain, weights, offsets):
    me = lax.axis_index("tp")
    sums = [None] * len(weights)
    squares = None
    for block, k in zip(hidden, offsets):
        piece = block.shape[1]
        source = me ^ k
        raw = block[...].astype(jnp.float32)
        scaled = (raw * gain[pl.ds(source, 1), :]).astype(jnp.bfloat16)
        part = jnp.sum(raw * raw, axis=1, keepdims=True)
        squares = part if squares is None else squares + part
        at = pl.ds(pl.multiple_of(source * piece, piece), piece)
        for n, weight in enumerate(weights):
            product = jnp.dot(scaled, weight[at, :], preferred_element_type=jnp.float32)
            sums[n] = product if sums[n] is None else sums[n] + product
    return sums, squares


def first_kernel(*refs, count, kinds, pieces, columns):
    own = refs[0]
    others = refs[1:count]
    gain = refs[count]
    small = refs[count + 1 : count + 3]
    weights = refs[count + 3 : count + 3 + kinds]
    w_out = refs[count + 3 + kinds]
    outs = refs[count + 4 + kinds : -2]
    held, sems = refs[-2:]
    sums_out, outs = outs[: kinds + 1], outs[kinds + 1 :]
    small_out, outs = outs[:2], outs[2:]
    weights_out, outs = outs[:kinds], outs[kinds:]
    pieces_out, biases = outs[: len(pieces)], outs[len(pieces) :]
    me = lax.axis_index("tp")
    moves = [(own, held), *zip(weights, weights_out), *zip(small, small_out)]
    for k, out in zip(pieces, pieces_out):
        peer = me ^ (3 - lax.axis_index("grp") if k is None else k)
        at = pl.ds(pl.multiple_of(peer * columns, columns), columns)
        moves.append((w_out.at[:, at], out))
    moves = [pltpu.make_async_copy(src, dst, sems.at[n]) for n, (src, dst) in enumerate(moves)]
    for move in moves:
        move.start()
    for d, out in enumerate(biases):
        out[...] = pair_bias(out.shape[0], d)
    for move in moves[: kinds + 1]:
        move.wait()
    sums, squares = sums_of((held, *others), gain, weights_out, range(count))
    for out, total in zip(sums_out, sums):
        out[...] = total
    sums_out[kinds][...] = wide(squares)
    for move in moves[kinds + 1 :]:
        move.wait()


def early_kernel(*refs, offsets, kinds):
    count = len(offsets)
    hidden = refs[:count]
    gain = refs[count]
    weights = refs[count + 1 : count + 1 + kinds]
    outs = refs[count + 1 + kinds :]
    sums, squares = sums_of(hidden, gain, weights, offsets)
    for out, total in zip(outs[:kinds], sums):
        out[...] = total
    outs[kinds][...] = wide(squares)


def head_turn(values, gains, cosine, sine):
    mean = jnp.mean(values * values, axis=1, keepdims=True)
    values = values * lax.rsqrt(mean + EPSILON) * gains
    return values * cosine + pltpu.roll(values, values.shape[1] // 2, 1) * sine


def late_kernel(*refs, offsets, kinds, width):
    count = len(offsets)
    hidden = refs[:count]
    gain = refs[count]
    weights = refs[count + 1 : count + 1 + kinds]
    rest = refs[count + 1 + kinds :]
    before = rest[:kinds]
    squares_before = rest[kinds]
    gains = rest[kinds + 1 : 2 * kinds]
    cosine, sine = rest[2 * kinds : 2 * kinds + 2]
    outs = rest[2 * kinds + 2 :]
    outs = [*outs[:-1], outs[-1].at[0], outs[-1].at[1]]
    sums, squares = sums_of(hidden, gain, weights, offsets)
    scale = lax.rsqrt((squares + squares_before[...]) / width + EPSILON)
    head_width = gains[0].shape[1]
    turn_c = jnp.concatenate([cosine[...], cosine[...]], axis=1)
    turn_s = jnp.concatenate([-sine[...], sine[...]], axis=1)
    for n in range(kinds):
        for start in range(0, sums[n].shape[1], head_width):
            lanes = slice(start, start + head_width)
            h = start // head_width
            values = (sums[n][:, lanes] + before[n][:, lanes]) * scale
            if n < kinds - 1:
                values = head_turn(values, gains[n][h : h + 1, :], turn_c, turn_s)
            outs[n][:, lanes] = values.astype(jnp.bfloat16)


def softmax_part(q, blocks, lanes, factor):
    scores = []
    for kv, bias in blocks:
        product = lax.dot_general(
            q[:, lanes], kv[0, :, lanes], (((1,), (1,)), ((), ())),
            preferred_element_type=jnp.float32,
        )
        scores.append(product * factor + bias)
    top = functools.reduce(jnp.maximum, [jnp.max(s, axis=1, keepdims=True) for s in scores])
    total = None
    acc = None
    for s, (kv, _) in zip(scores, blocks):
        weights = jnp.exp2(s - top)
        part = jnp.sum(weights, axis=1, keepdims=True)
        out = jnp.dot(
            weights.astype(jnp.bfloat16), kv[1, :, lanes], preferred_element_type=jnp.float32
        )
        total = part if total is None else total + part
        acc = out if acc is None else acc + out
    return top, total, acc


def merge(parts):
    top = functools.reduce(jnp.maximum, [part[0] for part in parts])
    total = None
    acc = None
    for part_top, part_total, part_acc in parts:
        decay = jnp.exp2(part_top - top)
        total = part_total * decay if total is None else total + part_total * decay
        acc = part_acc * decay if acc is None else acc + part_acc * decay
    return acc / total, top + jnp.log2(total)


def head_lanes(q, head_width):
    count = q.shape[1] // head_width
    return [slice(h * head_width, (h + 1) * head_width) for h in range(count)]


def near_kernel(q, kv, bias, kv_before, bias_before, *refs, last, head_width, factor):
    shard = lax.axis_index("sp")
    tops, totals, accs = refs[-3:]

    def work(previous):
        for lanes in head_lanes(q, head_width):
            seen = jnp.where(shard >= 1, bias_before[...], MASKED)
            blocks = [(kv, bias[...]), (previous, seen)]
            top, total, acc = softmax_part(q, blocks, lanes, factor)
            tops[:, lanes] = wide(top)
            totals[:, lanes] = wide(total)
            accs[:, lanes] = acc

    if last is None:
        work(kv_before)
    else:
        pl.when(shard == last)(lambda: work(refs[0]))
        pl.when(shard != last)(lambda: work(kv_before))


def help_kernel(q, *refs, blocks, head_width, factor, helper):
    out, logs = refs[2 * blocks :]

    @pl.when(lax.axis_index("sp") == helper)
    def _():
        for h, lanes in enumerate(head_lanes(q, head_width)):
            ready = [(refs[2 * n], refs[2 * n + 1][...]) for n in range(blocks)]
            top, total, acc = softmax_part(q, ready, lanes, factor)
            out[:, lanes] = (acc / total).astype(jnp.bfloat16)
            logs[h : h + 1, :] = wide(top + jnp.log2(total)).T[:1, :]


def late_help_kernel(*refs, late_count, late, help_now):
    late_in, rest = refs[:late_count], refs[late_count:]
    q, kv, bias, bias_before = rest[:4]
    kv_before, out, logs = rest[4:]
    late(*late_in, kv_before)
    help_now(q, kv, bias, kv_before, bias_before, out, logs)


def final_kernel(q, *refs, far, only, helped, head_width, factor):
    shard = lax.axis_index("sp")
    near = refs[:3]
    kvs = refs[3 : 3 + 2 * len(far)]
    given = refs[3 + 2 * len(far) : -2]
    attended, logs = refs[-2:]
    rows = q.shape[0]

    def finish(use_far, use_given):
        for h, lanes in enumerate(head_lanes(q, head_width)):
            parts = [tuple(ref[:, lanes] for ref in near)]
            if use_far:
                blocks = [
                    (kvs[2 * n], jnp.where(shard >= d, kvs[2 * n + 1][...], MASKED))
                    for n, d in enumerate(far)
                ]
                top, total, acc = softmax_part(q, blocks, lanes, factor)
                parts.append((wide(top), wide(total), acc))
            if use_given:
                top = jnp.broadcast_to(given[1][h : h + 1, :], (LANES, rows)).T
                parts.append((top, jnp.ones_like(top), given[0][:, lanes].astype(jnp.float32)))
            out, log_sum = merge(parts)
            attended[:, lanes] = out.astype(jnp.bfloat16)
            logs[:, lanes] = log_sum

    with_far = (shard == only) if only is not None else (shard >= 2)
    with_given = (shard == helped) if helped is not None else (shard < 0)
    if far:
        pl.when(with_far)(lambda: finish(True, False))
    if helped is not None:
        pl.when(with_given)(lambda: finish(False, True))
    pl.when(jnp.logical_not(with_far | with_given))(lambda: finish(False, False))


def products(blocks, pieces):
    total = None
    for block, piece in zip(blocks, pieces):
        product = jnp.dot(block[...], piece[...], preferred_element_type=jnp.float32)
        total = product if total is None else total + product
    return total


def mix_early_kernel(logs, *refs, count):
    total, rows = refs[2 * count :]
    total[...] = products(refs[:count], refs[count : 2 * count])
    for h in range(rows.shape[0]):
        lanes = slice(h * LANES, (h + 1) * LANES)
        rows[h : h + 1, :] = (logs[:, lanes] * math.log(2.0)).T[:1, :]


def mix_late_kernel(before, *refs, count, shared):
    blocks = [ref[...] for ref in refs[:count]]
    if shared:
        crossed = lax.axis_index("grp") == 0
        low, high = blocks
        blocks = [jnp.where(crossed, high, low), jnp.where(crossed, low, high)]
    total = before[...] + products(blocks, refs[count : 2 * count])
    refs[-1][...] = total.astype(jnp.bfloat16)


def swap(value, distance):
    count = lax.axis_size("tp")
    return lax.ppermute(value, "tp", [(i, i ^ distance) for i in range(count)])


def send(value, pairs):
    return lax.ppermute(value, "sp", pairs)


def behind(value, steps):
    count = lax.axis_size("sp")
    return send(value, [(s, s + steps) for s in range(count - steps)])


def near_blocks(block):
    blocks = {0: block}
    distance = lax.axis_size("tp") // 4
    while distance:
        for k in list(blocks):
            blocks[k ^ distance] = swap(blocks[k], distance)
        distance //= 2
    return [blocks[k] for k in sorted(blocks)]


def turn_tables(positions, head_width):
    inverse = ROTARY_BASE ** (-jnp.arange(0, head_width, 2, dtype=jnp.float32) / head_width)
    angles = positions[:, None] * inverse[None, :]
    return jnp.cos(angles), jnp.sin(angles)


def layer(hidden, norm_gain, w_query, w_key, w_value, query_gain, key_gain, w_out):
    rows, piece = hidden.shape
    head_count, head_width = query_gain.shape
    local_width = head_count * head_width
    count = lax.axis_size("tp")
    shards = lax.axis_size("sp")
    half = count // 2
    shard = lax.axis_index("sp")
    factor = head_width ** (-0.5) * LOG2_E
    reach = -(-KEYS_BEHIND * DILATIONS[-1] // rows)
    distances = list(range(min(shards - 1, reach) + 1))
    helped = shards - 1 if shards == 4 and reach >= shards - 1 else None
    far = [2] if helped is not None else distances[2:]

    first = shard * rows
    steps = jnp.arange(rows, dtype=jnp.int32)
    tables = turn_tables((steps + first).astype(jnp.float32), head_width)
    tables_before = turn_tables((steps + first - rows).astype(jnp.float32), head_width)
    gain = norm_gain.astype(jnp.float32).reshape(count, piece)
    gains = (query_gain, key_gain)
    weights = (w_query, w_key, w_value)
    sums = shape_of((rows, local_width), jnp.float32)
    half_sum = shape_of((rows, local_width), jnp.bfloat16)
    pair = shape_of((2, rows, local_width), jnp.bfloat16)
    lane_wide = shape_of((rows, LANES), jnp.float32)
    square = shape_of((rows, rows), jnp.float32)
    early = tuple(range(half))
    late = tuple(range(half, count))
    columns = w_out.shape[1] // count
    copies = lax.axis_size("grp")
    shared = copies == 2 and count == 4

    piece_keys = (0, *range(1, half), *((None,) if shared else late))
    piece_shape = shape_of((w_out.shape[0], columns), w_out.dtype)
    across = swap(hidden, half)
    if helped is None:
        before = behind(hidden, 1)
    else:
        before = send(hidden, [(n, n + 1) for n in range(shards - 2)])
    own_near = near_blocks(hidden)

    operands = [*own_near, gain, *gains, *weights, w_out]
    fixed = [0, *range(half + 1, len(operands))]
    moves = len(weights) + 3 + len(piece_keys)
    begun = call(
        functools.partial(first_kernel, count=half, kinds=3, pieces=piece_keys, columns=columns),
        operands,
        [sums] * 3
        + [lane_wide]
        + [shape_of(x.shape, x.dtype) for x in (*gains, *weights)]
        + [piece_shape] * len(piece_keys)
        + [square] * len(distances),
        held=fixed,
        scratch=[pltpu.VMEM(hidden.shape, hidden.dtype), pltpu.SemaphoreType.DMA((moves,))],
    )
    begun, rest = begun[:4], begun[4:]
    gains, weights, rest = rest[:2], rest[2:5], rest[5:]
    slices, biases = rest[: len(piece_keys)], rest[len(piece_keys) :]
    own_slice, near_slice, far_slice = slices[0], slices[1:half], slices[half:]

    own_far = near_blocks(across)
    if helped is None:
        before_across = swap(before, half)
    else:
        inner = [(n * count + t, n * count + (t ^ half)) for n in (1, 2) for t in range(count)]
        before_across = lax.ppermute(before, ("sp", "tp"), inner)
    width = piece * count
    q, kv = call(
        functools.partial(late_kernel, offsets=late, kinds=3, width=width),
        [*own_far, gain, *weights, *begun, *gains, *tables],
        [half_sum, pair],
    )

    if helped is not None:
        visitor = send(q, [(helped, 1)])
        far_blocks = [(send(kv, [(0, 2)]), biases[2])]
        direct = [send(kv, [(shards - 2, shards - 1)])]
    else:
        far_blocks = [(behind(kv, d), biases[d]) for d in far]
        direct = []

    begun_before = call(
        functools.partial(early_kernel, offsets=early, kinds=2),
        [*near_blocks(before), gain, *weights[1:]],
        [sums] * 2 + [lane_wide],
    )
    before_far = near_blocks(before_across)
    operands = [*before_far, gain, *weights[1:], *begun_before, gains[1], *tables_before]
    late_before = functools.partial(late_kernel, offsets=late, kinds=2, width=width)
    given = []
    if helped is None:
        (kv_before,) = call(late_before, operands, [pair])
    else:
        kv_before, out, logs = call(
            functools.partial(
                late_help_kernel,
                late_count=len(operands),
                late=late_before,
                help_now=functools.partial(
                    help_kernel, blocks=2, head_width=head_width, factor=factor, helper=1
                ),
            ),
            [*operands, visitor, kv, biases[2], biases[3]],
            [pair, half_sum, shape_of((8, rows), jnp.float32)],
        )
        given = [send(out, [(1, helped)]), send(logs, [(1, helped)])]
    near = call(
        functools.partial(
            near_kernel, last=helped, head_width=head_width, factor=factor
        ),
        [q, kv, biases[0], kv_before, biases[1], *direct],
        [sums] * 3,
    )

    *near_slice, _ = lax.optimization_barrier((*near_slice, begun_before[2]))
    near_pieces = [own_slice] + [swap(x, k + 1) for k, x in enumerate(near_slice)]
    if shared:
        routes = [(g * 4 + t, g * 4 + (t ^ (3 - g))) for g in range(2) for t in range(4)]
        fetched = lax.ppermute(far_slice[0], ("grp", "tp"), routes)
        fetched, _ = lax.optimization_barrier((fetched, near[0]))
        other = lax.ppermute(fetched, "grp", [(0, 1), (1, 0)])
        far_pieces = [fetched, other]
    else:
        far_pieces = [swap(x, k) for k, x in zip(late, far_slice)]

    attended, logs = call(
        functools.partial(
            final_kernel,
            far=tuple(far),
            only=2 if helped is not None else None,
            helped=helped,
            head_width=head_width,
            factor=factor,
        ),
        [q, *near, *[x for block in far_blocks for x in block], *given],
        [half_sum, sums],
    )
    attended_across = swap(attended, half)
    mixed_shape = (rows, columns)
    partial_mix, log_rows = call(
        functools.partial(mix_early_kernel, count=half),
        [logs, *near_blocks(attended), *near_pieces],
        [shape_of(mixed_shape, jnp.float32), shape_of((head_count, rows), jnp.float32)],
    )
    (mixed,) = call(
        functools.partial(mix_late_kernel, count=half, shared=shared),
        [partial_mix, *near_blocks(attended_across), *far_pieces],
        [shape_of(mixed_shape, jnp.bfloat16)],
    )
    return mixed, log_rows.T


def solution(mesh):
    placed = (
        P(("grp", "sp"), "tp"),
        P(),
        P(None, "tp"),
        P(None, "tp"),
        P(None, "tp"),
        P("tp", None),
        P("tp", None),
        P("tp", None),
    )
    return jax.shard_map(
        layer,
        mesh=mesh,
        in_specs=placed,
        out_specs=(P(("grp", "sp"), "tp"), P(("grp", "sp"), "tp")),
        check_vma=False,
    )
```

```python
import functools
import math

import jax
import jax.numpy as jnp
from jax import lax
from jax.experimental import pallas as pl
from jax.experimental.pallas import tpu as pltpu
from jax.sharding import PartitionSpec as P


KEYS_BEHIND = 128
DILATIONS = (1, 4, 16)
EPSILON = 1e-06
ROTARY_BASE = 500000.0
MASKED = -1e30
LANES = 128
LOG2_E = math.log2(math.e)


VMEM = pl.BlockSpec(memory_space=pltpu.VMEM)
HBM = pl.BlockSpec(memory_space=pltpu.HBM)


def shape_of(shape, dtype):
    return jax.ShapeDtypeStruct(shape, dtype)


def call(body, operands, outs, held=(), scratch=(), limit=24 << 20):
    return pl.pallas_call(
        body,
        out_shape=tuple(outs),
        in_specs=[HBM if n in held else VMEM for n in range(len(operands))],
        out_specs=(VMEM,) * len(outs),
        scratch_shapes=scratch,
        compiler_params=pltpu.CompilerParams(vmem_limit_bytes=limit),
    )(*[
        pltpu.with_memory_space_constraint(x, pltpu.HBM) if n in held else x
        for n, x in enumerate(operands)
    ])


def wide(column):
    return jnp.broadcast_to(column, (column.shape[0], LANES))


def pair_bias(rows, distance):
    row = lax.broadcasted_iota(jnp.int32, (rows, rows), 0)
    col = lax.broadcasted_iota(jnp.int32, (rows, rows), 1)
    behind = row - col + distance * rows
    times = jnp.zeros((rows, rows), jnp.int32)
    for dilation in DILATIONS:
        read = (behind >= 0) & (behind <= KEYS_BEHIND * dilation)
        read = read & ((behind & (dilation - 1)) == 0)
        times = times + read.astype(jnp.int32)
    return jnp.where(
        times == 0,
        MASKED,
        jnp.where(times == 3, math.log2(3.0), (times - 1).astype(jnp.float32)),
    )


def sums_of(hidden, gain, weights, offsets):
    me = lax.axis_index("tp")
    sums = [None] * len(weights)
    squares = None
    for block, k in zip(hidden, offsets):
        piece = block.shape[1]
        source = me ^ k
        raw = block[...].astype(jnp.float32)
        scaled = (raw * gain[pl.ds(source, 1), :]).astype(jnp.bfloat16)
        part = jnp.sum(raw * raw, axis=1, keepdims=True)
        squares = part if squares is None else squares + part
        at = pl.ds(pl.multiple_of(source * piece, piece), piece)
        for n, weight in enumerate(weights):
            product = jnp.dot(scaled, weight[at, :], preferred_element_type=jnp.float32)
            sums[n] = product if sums[n] is None else sums[n] + product
    return sums, squares


def first_kernel(*refs, count, kinds, pieces, columns):
    own = refs[0]
    others = refs[1:count]
    gain = refs[count]
    small = refs[count + 1 : count + 3]
    weights = refs[count + 3 : count + 3 + kinds]
    w_out = refs[count + 3 + kinds]
    outs = refs[count + 4 + kinds : -2]
    held, sems = refs[-2:]
    sums_out, outs = outs[: kinds + 1], outs[kinds + 1 :]
    small_out, outs = outs[:2], outs[2:]
    weights_out, outs = outs[:kinds], outs[kinds:]
    pieces_out, biases = outs[: len(pieces)], outs[len(pieces) :]
    me = lax.axis_index("tp")
    moves = [(own, held), *zip(weights, weights_out), *zip(small, small_out)]
    for k, out in zip(pieces, pieces_out):
        peer = me ^ (3 - lax.axis_index("grp") if k is None else k)
        at = pl.ds(pl.multiple_of(peer * columns, columns), columns)
        moves.append((w_out.at[:, at], out))
    moves = [pltpu.make_async_copy(src, dst, sems.at[n]) for n, (src, dst) in enumerate(moves)]
    for move in moves:
        move.start()
    for d, out in enumerate(biases):
        out[...] = pair_bias(out.shape[0], d)
    for move in moves[: kinds + 1]:
        move.wait()
    sums, squares = sums_of((held, *others), gain, weights_out, range(count))
    for out, total in zip(sums_out, sums):
        out[...] = total
    sums_out[kinds][...] = wide(squares)
    for move in moves[kinds + 1 :]:
        move.wait()


def early_kernel(*refs, offsets, kinds):
    count = len(offsets)
    hidden = refs[:count]
    gain = refs[count]
    weights = refs[count + 1 : count + 1 + kinds]
    outs = refs[count + 1 + kinds :]
    sums, squares = sums_of(hidden, gain, weights, offsets)
    for out, total in zip(outs[:kinds], sums):
        out[...] = total
    outs[kinds][...] = wide(squares)


def head_turn(values, gains, cosine, sine):
    mean = jnp.mean(values * values, axis=1, keepdims=True)
    values = values * lax.rsqrt(mean + EPSILON) * gains
    return values * cosine + pltpu.roll(values, values.shape[1] // 2, 1) * sine


def late_kernel(*refs, offsets, kinds, width):
    count = len(offsets)
    hidden = refs[:count]
    gain = refs[count]
    weights = refs[count + 1 : count + 1 + kinds]
    rest = refs[count + 1 + kinds :]
    before = rest[:kinds]
    squares_before = rest[kinds]
    gains = rest[kinds + 1 : 2 * kinds]
    cosine, sine = rest[2 * kinds : 2 * kinds + 2]
    outs = rest[2 * kinds + 2 :]
    outs = [*outs[:-1], outs[-1].at[0], outs[-1].at[1]]
    sums, squares = sums_of(hidden, gain, weights, offsets)
    scale = lax.rsqrt((squares + squares_before[...]) / width + EPSILON)
    head_width = gains[0].shape[1]
    turn_c = jnp.concatenate([cosine[...], cosine[...]], axis=1)
    turn_s = jnp.concatenate([-sine[...], sine[...]], axis=1)
    for n in range(kinds):
        for start in range(0, sums[n].shape[1], head_width):
            lanes = slice(start, start + head_width)
            h = start // head_width
            values = (sums[n][:, lanes] + before[n][:, lanes]) * scale
            if n < kinds - 1:
                values = head_turn(values, gains[n][h : h + 1, :], turn_c, turn_s)
            outs[n][:, lanes] = values.astype(jnp.bfloat16)


def softmax_part(q, blocks, lanes, factor):
    scores = []
    for kv, bias in blocks:
        product = lax.dot_general(
            q[:, lanes], kv[0, :, lanes], (((1,), (1,)), ((), ())),
            preferred_element_type=jnp.float32,
        )
        scores.append(product * factor + bias)
    top = functools.reduce(jnp.maximum, [jnp.max(s, axis=1, keepdims=True) for s in scores])
    total = None
    acc = None
    for s, (kv, _) in zip(scores, blocks):
        weights = jnp.exp2(s - top)
        part = jnp.sum(weights, axis=1, keepdims=True)
        out = jnp.dot(
            weights.astype(jnp.bfloat16), kv[1, :, lanes], preferred_element_type=jnp.float32
        )
        total = part if total is None else total + part
        acc = out if acc is None else acc + out
    return top, total, acc


def merge(parts):
    top = functools.reduce(jnp.maximum, [part[0] for part in parts])
    total = None
    acc = None
    for part_top, part_total, part_acc in parts:
        decay = jnp.exp2(part_top - top)
        total = part_total * decay if total is None else total + part_total * decay
        acc = part_acc * decay if acc is None else acc + part_acc * decay
    return acc / total, top + jnp.log2(total)


def head_lanes(q, head_width):
    count = q.shape[1] // head_width
    return [slice(h * head_width, (h + 1) * head_width) for h in range(count)]


def near_kernel(q, *refs, distances, head_width, factor):
    count = len(distances)
    tops, totals, accs = refs[2 * count :]
    for lanes in head_lanes(q, head_width):
        blocks = []
        for n, d in enumerate(distances):
            bias = refs[2 * n + 1][...]
            blocks.append((refs[2 * n], jnp.where(lax.axis_index("sp") >= d, bias, MASKED) if d else bias))
        top, total, acc = softmax_part(q, blocks, lanes, factor)
        tops[:, lanes] = wide(top)
        totals[:, lanes] = wide(total)
        accs[:, lanes] = acc


def help_kernel(q, *refs, blocks, head_width, factor):
    out, logs = refs[2 * blocks :]

    for h, lanes in enumerate(head_lanes(q, head_width)):
        ready = [(refs[2 * n], refs[2 * n + 1][...]) for n in range(blocks)]
        top, total, acc = softmax_part(q, ready, lanes, factor)
        out[:, lanes] = (acc / total).astype(jnp.bfloat16)
        logs[h : h + 1, :] = wide(top + jnp.log2(total)).T[:1, :]


def late_help_kernel(*refs, late_count, late, help_now, helper):
    late_in, rest = refs[:late_count], refs[late_count:]
    q, kv, bias, bias_before = rest[:4]
    kv_before, out, logs = rest[4:]

    @pl.when(lax.axis_index("sp") == helper)
    def _():
        late(*late_in, kv_before)
        help_now(q, kv, bias, kv_before, bias_before, out, logs)


def near_late_kernel(q, kv, bias, kv_helper, bias_before, *refs, late, near, helper):
    late_in, outs, held = refs[:-4], refs[-4:-1], refs[-1]
    ready = lax.axis_index("sp") == helper

    @pl.when(ready)
    def _():
        near(q, kv, bias, kv_helper, bias_before, *outs)

    @pl.when(jnp.logical_not(ready))
    def _():
        late(*late_in, held)
        near(q, kv, bias, held, bias_before, *outs)


def final_kernel(q, *refs, far, only, helped, head_width, factor):
    shard = lax.axis_index("sp")
    near = refs[:3]
    kvs = refs[3 : 3 + 2 * len(far)]
    given = refs[3 + 2 * len(far) : -2]
    attended, logs = refs[-2:]
    rows = q.shape[0]

    def finish(use_far, use_given):
        for h, lanes in enumerate(head_lanes(q, head_width)):
            parts = [tuple(ref[:, lanes] for ref in near)]
            if use_far:
                blocks = [
                    (kvs[2 * n], jnp.where(shard >= d, kvs[2 * n + 1][...], MASKED))
                    for n, d in enumerate(far)
                ]
                top, total, acc = softmax_part(q, blocks, lanes, factor)
                parts.append((wide(top), wide(total), acc))
            if use_given:
                top = jnp.broadcast_to(given[1][h : h + 1, :], (LANES, rows)).T
                parts.append((top, jnp.ones_like(top), given[0][:, lanes].astype(jnp.float32)))
            out, log_sum = merge(parts)
            attended[:, lanes] = out.astype(jnp.bfloat16)
            logs[:, lanes] = log_sum

    with_far = (shard == only) if only is not None else (shard >= 2)
    with_given = (shard == helped) if helped is not None else (shard < 0)
    if far:
        pl.when(with_far)(lambda: finish(True, False))
    if helped is not None:
        pl.when(with_given)(lambda: finish(False, True))
    pl.when(jnp.logical_not(with_far | with_given))(lambda: finish(False, False))


def products(blocks, pieces):
    total = None
    for block, piece in zip(blocks, pieces):
        product = jnp.dot(block[...], piece[...], preferred_element_type=jnp.float32)
        total = product if total is None else total + product
    return total


def mix_early_kernel(logs, *refs, count):
    total, rows = refs[2 * count :]
    total[...] = products(refs[:count], refs[count : 2 * count])
    for h in range(rows.shape[0]):
        lanes = slice(h * LANES, (h + 1) * LANES)
        rows[h : h + 1, :] = (logs[:, lanes] * math.log(2.0)).T[:1, :]


def mix_late_kernel(before, *refs, count, shared):
    blocks = [ref[...] for ref in refs[:count]]
    if shared:
        crossed = lax.axis_index("grp") == 0
        low, high = blocks
        blocks = [jnp.where(crossed, high, low), jnp.where(crossed, low, high)]
    total = before[...] + products(blocks, refs[count : 2 * count])
    refs[-1][...] = total.astype(jnp.bfloat16)


def swap(value, distance):
    count = lax.axis_size("tp")
    return lax.ppermute(value, "tp", [(i, i ^ distance) for i in range(count)])


def send(value, pairs):
    return lax.ppermute(value, "sp", pairs)


def behind(value, steps):
    count = lax.axis_size("sp")
    return send(value, [(s, s + steps) for s in range(count - steps)])


def near_blocks(block):
    blocks = {0: block}
    distance = lax.axis_size("tp") // 4
    while distance:
        for k in list(blocks):
            blocks[k ^ distance] = swap(blocks[k], distance)
        distance //= 2
    return [blocks[k] for k in sorted(blocks)]


def turn_tables(positions, head_width):
    inverse = ROTARY_BASE ** (-jnp.arange(0, head_width, 2, dtype=jnp.float32) / head_width)
    angles = positions[:, None] * inverse[None, :]
    return jnp.cos(angles), jnp.sin(angles)


def layer(hidden, norm_gain, w_query, w_key, w_value, query_gain, key_gain, w_out):
    rows, piece = hidden.shape
    head_count, head_width = query_gain.shape
    local_width = head_count * head_width
    count = lax.axis_size("tp")
    shards = lax.axis_size("sp")
    half = count // 2
    shard = lax.axis_index("sp")
    factor = head_width ** (-0.5) * LOG2_E
    reach = -(-KEYS_BEHIND * DILATIONS[-1] // rows)
    distances = list(range(min(shards - 1, reach) + 1))
    helped = shards - 1 if shards == 4 and reach >= shards - 1 else None
    far = [2] if helped is not None else distances[2:]

    first = shard * rows
    steps = jnp.arange(rows, dtype=jnp.int32)
    tables = turn_tables((steps + first).astype(jnp.float32), head_width)
    tables_before = turn_tables((steps + first - rows).astype(jnp.float32), head_width)
    gain = norm_gain.astype(jnp.float32).reshape(count, piece)
    gains = (query_gain, key_gain)
    weights = (w_query, w_key, w_value)
    sums = shape_of((rows, local_width), jnp.float32)
    half_sum = shape_of((rows, local_width), jnp.bfloat16)
    pair = shape_of((2, rows, local_width), jnp.bfloat16)
    lane_wide = shape_of((rows, LANES), jnp.float32)
    square = shape_of((rows, rows), jnp.float32)
    early = tuple(range(half))
    late = tuple(range(half, count))
    columns = w_out.shape[1] // count
    copies = lax.axis_size("grp")
    shared = copies == 2 and count == 4

    piece_keys = (0, *range(1, half), *((None,) if shared else late))
    piece_shape = shape_of((w_out.shape[0], columns), w_out.dtype)
    across = swap(hidden, half)
    before = behind(hidden, 1)
    own_near = near_blocks(hidden)

    operands = [*own_near, gain, *gains, *weights, w_out]
    fixed = [0, *range(half + 1, len(operands))]
    moves = len(weights) + 3 + len(piece_keys)
    begun = call(
        functools.partial(first_kernel, count=half, kinds=3, pieces=piece_keys, columns=columns),
        operands,
        [sums] * 3
        + [lane_wide]
        + [shape_of(x.shape, x.dtype) for x in (*gains, *weights)]
        + [piece_shape] * len(piece_keys)
        + [square] * len(distances),
        held=fixed,
        scratch=[pltpu.VMEM(hidden.shape, hidden.dtype), pltpu.SemaphoreType.DMA((moves,))],
    )
    begun, rest = begun[:4], begun[4:]
    gains, weights, rest = rest[:2], rest[2:5], rest[5:]
    slices, biases = rest[: len(piece_keys)], rest[len(piece_keys) :]
    own_slice, near_slice, far_slice = slices[0], slices[1:half], slices[half:]

    own_far = near_blocks(across)
    before_across = swap(before, half)
    width = piece * count
    q, kv = call(
        functools.partial(late_kernel, offsets=late, kinds=3, width=width),
        [*own_far, gain, *weights, *begun, *gains, *tables],
        [half_sum, pair],
    )

    if helped is not None:
        visitor = send(q, [(helped, 1)])
        far_blocks = [(send(kv, [(0, 2)]), biases[2])]
    else:
        far_blocks = [(behind(kv, d), biases[d]) for d in far]

    begun_before = call(
        functools.partial(early_kernel, offsets=early, kinds=2),
        [*near_blocks(before), gain, *weights[1:]],
        [sums] * 2 + [lane_wide],
    )
    before_far = near_blocks(before_across)
    operands = [*before_far, gain, *weights[1:], *begun_before, gains[1], *tables_before]
    late_before = functools.partial(late_kernel, offsets=late, kinds=2, width=width)
    given = []
    if helped is None:
        (kv_before,) = call(late_before, operands, [pair])
    else:
        kv_before, out, logs = call(
            functools.partial(
                late_help_kernel,
                late_count=len(operands),
                helper=1,
                late=late_before,
                help_now=functools.partial(
                    help_kernel, blocks=2, head_width=head_width, factor=factor
                ),
            ),
            [*operands, visitor, kv, biases[2], biases[3]],
            [pair, half_sum, shape_of((8, rows), jnp.float32)],
        )
        given = [send(out, [(1, helped)]), send(logs, [(1, helped)])]
    near_part = functools.partial(
        near_kernel, distances=(0, 1), head_width=head_width, factor=factor
    )
    near_in = [q, kv, biases[0], kv_before, biases[1]]
    if helped is None:
        near = call(near_part, near_in, [sums] * 3)
    else:
        near = call(
            functools.partial(near_late_kernel, late=late_before, near=near_part, helper=1),
            [*near_in, *operands],
            [sums] * 3,
            scratch=[pltpu.VMEM(pair.shape, pair.dtype)],
        )

    near_pieces = [own_slice] + [swap(x, k + 1) for k, x in enumerate(near_slice)]
    if shared:
        routes = [(g * 4 + t, g * 4 + (t ^ (3 - g))) for g in range(2) for t in range(4)]
        fetched = lax.ppermute(far_slice[0], ("grp", "tp"), routes)
        later, _ = lax.optimization_barrier((fetched, near[0]))
        other = lax.ppermute(later, "grp", [(0, 1), (1, 0)])
        far_pieces = [fetched, other]
    else:
        far_pieces = [swap(x, k) for k, x in zip(late, far_slice)]

    attended, logs = call(
        functools.partial(
            final_kernel,
            far=tuple(far),
            only=2 if helped is not None else None,
            helped=helped,
            head_width=head_width,
            factor=factor,
        ),
        [q, *near, *[x for block in far_blocks for x in block], *given],
        [half_sum, sums],
    )
    attended_across = swap(attended, half)
    mixed_shape = (rows, columns)
    partial_mix, log_rows = call(
        functools.partial(mix_early_kernel, count=half),
        [logs, *near_blocks(attended), *near_pieces],
        [shape_of(mixed_shape, jnp.float32), shape_of((head_count, rows), jnp.float32)],
    )
    (mixed,) = call(
        functools.partial(mix_late_kernel, count=half, shared=shared),
        [partial_mix, *near_blocks(attended_across), *far_pieces],
        [shape_of(mixed_shape, jnp.bfloat16)],
    )
    return mixed, log_rows.T


def solution(mesh):
    placed = (
        P(("grp", "sp"), "tp"),
        P(),
        P(None, "tp"),
        P(None, "tp"),
        P(None, "tp"),
        P("tp", None),
        P("tp", None),
        P("tp", None),
    )
    return jax.shard_map(
        layer,
        mesh=mesh,
        in_specs=placed,
        out_specs=(P(("grp", "sp"), "tp"), P(("grp", "sp"), "tp")),
        check_vma=False,
    )
```

```python
import functools
import math

import jax
import jax.numpy as jnp
from jax import lax
from jax.experimental import pallas as pl
from jax.experimental.pallas import tpu as pltpu
from jax.sharding import PartitionSpec as P


KEYS_BEHIND = 128
DILATIONS = (1, 4, 16)
EPSILON = 1e-06
ROTARY_BASE = 500000.0
MASKED = -1e30
LANES = 128
LOG2_E = math.log2(math.e)


VMEM = pl.BlockSpec(memory_space=pltpu.VMEM)
HBM = pl.BlockSpec(memory_space=pltpu.HBM)


def shape_of(shape, dtype):
    return jax.ShapeDtypeStruct(shape, dtype)


def call(body, operands, outs, held=(), scratch=(), limit=24 << 20):
    return pl.pallas_call(
        body,
        out_shape=tuple(outs),
        in_specs=[HBM if n in held else VMEM for n in range(len(operands))],
        out_specs=(VMEM,) * len(outs),
        scratch_shapes=scratch,
        compiler_params=pltpu.CompilerParams(vmem_limit_bytes=limit),
    )(*[
        pltpu.with_memory_space_constraint(x, pltpu.HBM) if n in held else x
        for n, x in enumerate(operands)
    ])


def wide(column):
    return jnp.broadcast_to(column, (column.shape[0], LANES))


def pair_bias(rows, distance):
    row = lax.broadcasted_iota(jnp.int32, (rows, rows), 0)
    col = lax.broadcasted_iota(jnp.int32, (rows, rows), 1)
    behind = row - col + distance * rows
    times = jnp.zeros((rows, rows), jnp.int32)
    for dilation in DILATIONS:
        read = (behind >= 0) & (behind <= KEYS_BEHIND * dilation)
        read = read & ((behind & (dilation - 1)) == 0)
        times = times + read.astype(jnp.int32)
    return jnp.where(
        times == 0,
        MASKED,
        jnp.where(times == 3, math.log2(3.0), (times - 1).astype(jnp.float32)),
    )


def sums_of(hidden, gain, weights, offsets):
    me = lax.axis_index("tp")
    sums = [None] * len(weights)
    squares = None
    for block, k in zip(hidden, offsets):
        piece = block.shape[1]
        source = me ^ k
        raw = block[...].astype(jnp.float32)
        scaled = (raw * gain[pl.ds(source, 1), :]).astype(jnp.bfloat16)
        part = jnp.sum(raw * raw, axis=1, keepdims=True)
        squares = part if squares is None else squares + part
        at = pl.ds(pl.multiple_of(source * piece, piece), piece)
        for n, weight in enumerate(weights):
            product = jnp.dot(scaled, weight[at, :], preferred_element_type=jnp.float32)
            sums[n] = product if sums[n] is None else sums[n] + product
    return sums, squares


def first_kernel(*refs, count, kinds, pieces, columns):
    own = refs[0]
    others = refs[1:count]
    gain = refs[count]
    small = refs[count + 1 : count + 3]
    weights = refs[count + 3 : count + 3 + kinds]
    w_out = refs[count + 3 + kinds]
    outs = refs[count + 4 + kinds : -2]
    held, sems = refs[-2:]
    sums_out, outs = outs[: kinds + 1], outs[kinds + 1 :]
    small_out, outs = outs[:2], outs[2:]
    weights_out, outs = outs[:kinds], outs[kinds:]
    pieces_out, biases = outs[: len(pieces)], outs[len(pieces) :]
    me = lax.axis_index("tp")
    moves = [(own, held), *zip(weights, weights_out), *zip(small, small_out)]
    for (k, start), out in zip(pieces, pieces_out):
        peer = me ^ (3 - lax.axis_index("grp") if k is None else k)
        at = pl.ds(pl.multiple_of(peer * columns, columns), columns)
        moves.append((w_out.at[pl.ds(start, out.shape[0]), at], out))
    moves = [pltpu.make_async_copy(src, dst, sems.at[n]) for n, (src, dst) in enumerate(moves)]
    for move in moves:
        move.start()
    for d, out in enumerate(biases):
        out[...] = pair_bias(out.shape[0], d)
    for move in moves[: kinds + 1]:
        move.wait()
    sums, squares = sums_of((held, *others), gain, weights_out, range(count))
    for out, total in zip(sums_out, sums):
        out[...] = total
    sums_out[kinds][...] = wide(squares)
    for move in moves[kinds + 1 :]:
        move.wait()


def early_kernel(*refs, offsets, kinds):
    count = len(offsets)
    hidden = refs[:count]
    gain = refs[count]
    weights = refs[count + 1 : count + 1 + kinds]
    outs = refs[count + 1 + kinds :]
    sums, squares = sums_of(hidden, gain, weights, offsets)
    for out, total in zip(outs[:kinds], sums):
        out[...] = total
    outs[kinds][...] = wide(squares)


def head_turn(values, gains, cosine, sine):
    mean = jnp.mean(values * values, axis=1, keepdims=True)
    values = values * lax.rsqrt(mean + EPSILON) * gains
    return values * cosine + pltpu.roll(values, values.shape[1] // 2, 1) * sine


def late_kernel(*refs, offsets, kinds, width):
    count = len(offsets)
    hidden = refs[:count]
    gain = refs[count]
    weights = refs[count + 1 : count + 1 + kinds]
    rest = refs[count + 1 + kinds :]
    before = rest[:kinds]
    squares_before = rest[kinds]
    gains = rest[kinds + 1 : 2 * kinds]
    cosine, sine = rest[2 * kinds : 2 * kinds + 2]
    outs = rest[2 * kinds + 2 :]
    outs = [*outs[:-1], outs[-1].at[0], outs[-1].at[1]]
    sums, squares = sums_of(hidden, gain, weights, offsets)
    scale = lax.rsqrt((squares + squares_before[...]) / width + EPSILON)
    head_width = gains[0].shape[1]
    turn_c = jnp.concatenate([cosine[...], cosine[...]], axis=1)
    turn_s = jnp.concatenate([-sine[...], sine[...]], axis=1)
    for n in range(kinds):
        for start in range(0, sums[n].shape[1], head_width):
            lanes = slice(start, start + head_width)
            h = start // head_width
            values = (sums[n][:, lanes] + before[n][:, lanes]) * scale
            if n < kinds - 1:
                values = head_turn(values, gains[n][h : h + 1, :], turn_c, turn_s)
            outs[n][:, lanes] = values.astype(jnp.bfloat16)


def softmax_part(q, blocks, lanes, factor):
    scores = []
    for kv, bias in blocks:
        product = lax.dot_general(
            q[:, lanes], kv[0, :, lanes], (((1,), (1,)), ((), ())),
            preferred_element_type=jnp.float32,
        )
        scores.append(product * factor + bias)
    top = functools.reduce(jnp.maximum, [jnp.max(s, axis=1, keepdims=True) for s in scores])
    total = None
    acc = None
    for s, (kv, _) in zip(scores, blocks):
        weights = jnp.exp2(s - top)
        part = jnp.sum(weights, axis=1, keepdims=True)
        out = jnp.dot(
            weights.astype(jnp.bfloat16), kv[1, :, lanes], preferred_element_type=jnp.float32
        )
        total = part if total is None else total + part
        acc = out if acc is None else acc + out
    return top, total, acc


def merge(parts):
    top = functools.reduce(jnp.maximum, [part[0] for part in parts])
    total = None
    acc = None
    for part_top, part_total, part_acc in parts:
        decay = jnp.exp2(part_top - top)
        total = part_total * decay if total is None else total + part_total * decay
        acc = part_acc * decay if acc is None else acc + part_acc * decay
    return acc / total, top + jnp.log2(total)


def head_lanes(q, head_width):
    count = q.shape[1] // head_width
    return [slice(h * head_width, (h + 1) * head_width) for h in range(count)]


def near_kernel(q, *refs, distances, head_width, factor):
    count = len(distances)
    tops, totals, accs = refs[2 * count :]
    for lanes in head_lanes(q, head_width):
        blocks = []
        for n, d in enumerate(distances):
            bias = refs[2 * n + 1][...]
            blocks.append((refs[2 * n], jnp.where(lax.axis_index("sp") >= d, bias, MASKED) if d else bias))
        top, total, acc = softmax_part(q, blocks, lanes, factor)
        tops[:, lanes] = wide(top)
        totals[:, lanes] = wide(total)
        accs[:, lanes] = acc


def help_kernel(q, *refs, blocks, head_width, factor):
    out, logs = refs[2 * blocks :]

    for h, lanes in enumerate(head_lanes(q, head_width)):
        ready = [(refs[2 * n], refs[2 * n + 1][...]) for n in range(blocks)]
        top, total, acc = softmax_part(q, ready, lanes, factor)
        out[:, lanes] = (acc / total).astype(jnp.bfloat16)
        logs[h : h + 1, :] = wide(top + jnp.log2(total)).T[:1, :]


def late_help_kernel(*refs, late_count, late, help_now, helper):
    late_in, rest = refs[:late_count], refs[late_count:]
    q, kv, bias, bias_before = rest[:4]
    kv_before, out, logs = rest[4:]

    @pl.when(lax.axis_index("sp") == helper)
    def _():
        late(*late_in, kv_before)
        help_now(q, kv, bias, kv_before, bias_before, out, logs)


def near_late_kernel(q, kv, bias, kv_helper, bias_before, *refs, late, near, helper):
    late_in, outs, held = refs[:-4], refs[-4:-1], refs[-1]
    ready = lax.axis_index("sp") == helper

    @pl.when(ready)
    def _():
        near(q, kv, bias, kv_helper, bias_before, *outs)

    @pl.when(jnp.logical_not(ready))
    def _():
        late(*late_in, held)
        near(q, kv, bias, held, bias_before, *outs)


def final_kernel(q, *refs, far, only, helped, head_width, factor):
    shard = lax.axis_index("sp")
    near = refs[:3]
    kvs = refs[3 : 3 + 2 * len(far)]
    given = refs[3 + 2 * len(far) : -2]
    attended, logs = refs[-2:]
    rows = q.shape[0]

    def finish(use_far, use_given):
        for h, lanes in enumerate(head_lanes(q, head_width)):
            parts = [tuple(ref[:, lanes] for ref in near)]
            if use_far:
                blocks = [
                    (kvs[2 * n], jnp.where(shard >= d, kvs[2 * n + 1][...], MASKED))
                    for n, d in enumerate(far)
                ]
                top, total, acc = softmax_part(q, blocks, lanes, factor)
                parts.append((wide(top), wide(total), acc))
            if use_given:
                top = jnp.broadcast_to(given[1][h : h + 1, :], (LANES, rows)).T
                parts.append((top, jnp.ones_like(top), given[0][:, lanes].astype(jnp.float32)))
            out, log_sum = merge(parts)
            attended[:, lanes] = out.astype(jnp.bfloat16)
            logs[:, lanes] = log_sum

    with_far = (shard == only) if only is not None else (shard >= 2)
    with_given = (shard == helped) if helped is not None else (shard < 0)
    if far:
        pl.when(with_far)(lambda: finish(True, False))
    if helped is not None:
        pl.when(with_given)(lambda: finish(False, True))
    pl.when(jnp.logical_not(with_far | with_given))(lambda: finish(False, False))


def products(blocks, pieces):
    total = None
    for block, piece in zip(blocks, pieces):
        product = jnp.dot(block[...], piece[...], preferred_element_type=jnp.float32)
        total = product if total is None else total + product
    return total


def mix_early_kernel(logs, *refs, count):
    total, rows = refs[2 * count :]
    total[...] = products(refs[:count], refs[count : 2 * count])
    for h in range(rows.shape[0]):
        lanes = slice(h * LANES, (h + 1) * LANES)
        rows[h : h + 1, :] = (logs[:, lanes] * math.log(2.0)).T[:1, :]


def mix_late_kernel(before, *refs, count, shared):
    blocks = [ref[...] for ref in refs[:count]]
    if shared:
        crossed = lax.axis_index("grp") == 0
        low, high = blocks
        blocks = [jnp.where(crossed, high, low), jnp.where(crossed, low, high)]
        halves = [ref[...] for ref in refs[count:-1]]
        pieces = [jnp.concatenate(halves[:2], axis=0), jnp.concatenate(halves[2:], axis=0)]
    else:
        pieces = refs[count : 2 * count]
    total = before[...] + products(blocks, pieces)
    refs[-1][...] = total.astype(jnp.bfloat16)


def swap(value, distance):
    count = lax.axis_size("tp")
    return lax.ppermute(value, "tp", [(i, i ^ distance) for i in range(count)])


def send(value, pairs):
    return lax.ppermute(value, "sp", pairs)


def behind(value, steps):
    count = lax.axis_size("sp")
    return send(value, [(s, s + steps) for s in range(count - steps)])


def near_blocks(block):
    blocks = {0: block}
    distance = lax.axis_size("tp") // 4
    while distance:
        for k in list(blocks):
            blocks[k ^ distance] = swap(blocks[k], distance)
        distance //= 2
    return [blocks[k] for k in sorted(blocks)]


def turn_tables(positions, head_width):
    inverse = ROTARY_BASE ** (-jnp.arange(0, head_width, 2, dtype=jnp.float32) / head_width)
    angles = positions[:, None] * inverse[None, :]
    return jnp.cos(angles), jnp.sin(angles)


def layer(hidden, norm_gain, w_query, w_key, w_value, query_gain, key_gain, w_out):
    rows, piece = hidden.shape
    head_count, head_width = query_gain.shape
    local_width = head_count * head_width
    count = lax.axis_size("tp")
    shards = lax.axis_size("sp")
    half = count // 2
    shard = lax.axis_index("sp")
    factor = head_width ** (-0.5) * LOG2_E
    reach = -(-KEYS_BEHIND * DILATIONS[-1] // rows)
    distances = list(range(min(shards - 1, reach) + 1))
    helped = shards - 1 if shards == 4 and reach >= shards - 1 else None
    far = [2] if helped is not None else distances[2:]

    first = shard * rows
    steps = jnp.arange(rows, dtype=jnp.int32)
    tables = turn_tables((steps + first).astype(jnp.float32), head_width)
    tables_before = turn_tables((steps + first - rows).astype(jnp.float32), head_width)
    gain = norm_gain.astype(jnp.float32).reshape(count, piece)
    gains = (query_gain, key_gain)
    weights = (w_query, w_key, w_value)
    sums = shape_of((rows, local_width), jnp.float32)
    half_sum = shape_of((rows, local_width), jnp.bfloat16)
    pair = shape_of((2, rows, local_width), jnp.bfloat16)
    lane_wide = shape_of((rows, LANES), jnp.float32)
    square = shape_of((rows, rows), jnp.float32)
    early = tuple(range(half))
    late = tuple(range(half, count))
    columns = w_out.shape[1] // count
    copies = lax.axis_size("grp")
    shared = copies == 2 and count == 4

    cut = w_out.shape[0] // 2 if shared else w_out.shape[0]
    piece_keys = tuple((k, 0) for k in range(half))
    piece_keys += ((None, 0), (None, cut)) if shared else tuple((k, 0) for k in late)
    piece_shapes = [shape_of((w_out.shape[0], columns), w_out.dtype)] * half
    piece_shapes += [shape_of((cut, columns), w_out.dtype)] * (len(piece_keys) - half)
    across = swap(hidden, half)
    before = behind(hidden, 1)
    own_near = near_blocks(hidden)

    operands = [*own_near, gain, *gains, *weights, w_out]
    fixed = [0, *range(half + 1, len(operands))]
    moves = len(weights) + 3 + len(piece_keys)
    begun = call(
        functools.partial(first_kernel, count=half, kinds=3, pieces=piece_keys, columns=columns),
        operands,
        [sums] * 3
        + [lane_wide]
        + [shape_of(x.shape, x.dtype) for x in (*gains, *weights)]
        + piece_shapes
        + [square] * len(distances),
        held=fixed,
        scratch=[pltpu.VMEM(hidden.shape, hidden.dtype), pltpu.SemaphoreType.DMA((moves,))],
    )
    begun, rest = begun[:4], begun[4:]
    gains, weights, rest = rest[:2], rest[2:5], rest[5:]
    slices, biases = rest[: len(piece_keys)], rest[len(piece_keys) :]
    own_slice, near_slice, far_slice = slices[0], slices[1:half], slices[half:]

    own_far = near_blocks(across)
    before_across = swap(before, half)
    width = piece * count
    q, kv = call(
        functools.partial(late_kernel, offsets=late, kinds=3, width=width),
        [*own_far, gain, *weights, *begun, *gains, *tables],
        [half_sum, pair],
    )

    if helped is not None:
        visitor = send(q, [(helped, 1)])
        far_blocks = [(send(kv, [(0, 2)]), biases[2])]
    else:
        far_blocks = [(behind(kv, d), biases[d]) for d in far]

    begun_before = call(
        functools.partial(early_kernel, offsets=early, kinds=2),
        [*near_blocks(before), gain, *weights[1:]],
        [sums] * 2 + [lane_wide],
    )
    before_far = near_blocks(before_across)
    operands = [*before_far, gain, *weights[1:], *begun_before, gains[1], *tables_before]
    late_before = functools.partial(late_kernel, offsets=late, kinds=2, width=width)
    given = []
    if helped is None:
        (kv_before,) = call(late_before, operands, [pair])
    else:
        kv_before, out, logs = call(
            functools.partial(
                late_help_kernel,
                late_count=len(operands),
                helper=1,
                late=late_before,
                help_now=functools.partial(
                    help_kernel, blocks=2, head_width=head_width, factor=factor
                ),
            ),
            [*operands, visitor, kv, biases[2], biases[3]],
            [pair, half_sum, shape_of((8, rows), jnp.float32)],
        )
        given = [send(out, [(1, helped)]), send(logs, [(1, helped)])]
    near_part = functools.partial(
        near_kernel, distances=(0, 1), head_width=head_width, factor=factor
    )
    near_in = [q, kv, biases[0], kv_before, biases[1]]
    if helped is None:
        near = call(near_part, near_in, [sums] * 3)
    else:
        near = call(
            functools.partial(near_late_kernel, late=late_before, near=near_part, helper=1),
            [*near_in, *operands],
            [sums] * 3,
            scratch=[pltpu.VMEM(pair.shape, pair.dtype)],
        )

    near_pieces = [own_slice] + [swap(x, k + 1) for k, x in enumerate(near_slice)]
    if shared:
        routes = [(g * 4 + t, g * 4 + (t ^ (3 - g))) for g in range(2) for t in range(4)]
        first_half = lax.ppermute(far_slice[0], ("grp", "tp"), routes)
        first_other = lax.ppermute(first_half, "grp", [(0, 1), (1, 0)])
        last_half = lax.ppermute(far_slice[1], ("grp", "tp"), routes)
    else:
        far_pieces = [swap(x, k) for k, x in zip(late, far_slice)]

    attended, logs = call(
        functools.partial(
            final_kernel,
            far=tuple(far),
            only=2 if helped is not None else None,
            helped=helped,
            head_width=head_width,
            factor=factor,
        ),
        [q, *near, *[x for block in far_blocks for x in block], *given],
        [half_sum, sums],
    )
    attended_across = swap(attended, half)
    if shared:
        later, _ = lax.optimization_barrier((last_half, logs))
        last_other = lax.ppermute(later, "grp", [(0, 1), (1, 0)])
        far_pieces = [first_half, last_half, first_other, last_other]
    mixed_shape = (rows, columns)
    partial_mix, log_rows = call(
        functools.partial(mix_early_kernel, count=half),
        [logs, *near_blocks(attended), *near_pieces],
        [shape_of(mixed_shape, jnp.float32), shape_of((head_count, rows), jnp.float32)],
    )
    (mixed,) = call(
        functools.partial(mix_late_kernel, count=half, shared=shared),
        [partial_mix, *near_blocks(attended_across), *far_pieces],
        [shape_of(mixed_shape, jnp.bfloat16)],
    )
    return mixed, log_rows.T


def solution(mesh):
    placed = (
        P(("grp", "sp"), "tp"),
        P(),
        P(None, "tp"),
        P(None, "tp"),
        P(None, "tp"),
        P("tp", None),
        P("tp", None),
        P("tp", None),
    )
    return jax.shard_map(
        layer,
        mesh=mesh,
        in_specs=placed,
        out_specs=(P(("grp", "sp"), "tp"), P(("grp", "sp"), "tp")),
        check_vma=False,
    )
```

```python
import functools
import math

import jax
import jax.numpy as jnp
from jax import lax
from jax.experimental import pallas as pl
from jax.experimental.pallas import tpu as pltpu
from jax.sharding import PartitionSpec as P


KEYS_BEHIND = 128
DILATIONS = (1, 4, 16)
EPSILON = 1e-06
ROTARY_BASE = 500000.0
MASKED = -1e30
LANES = 128
LOG2_E = math.log2(math.e)


VMEM = pl.BlockSpec(memory_space=pltpu.VMEM)
HBM = pl.BlockSpec(memory_space=pltpu.HBM)


def shape_of(shape, dtype):
    return jax.ShapeDtypeStruct(shape, dtype)


def call(body, operands, outs, held=(), scratch=(), limit=24 << 20):
    return pl.pallas_call(
        body,
        out_shape=tuple(outs),
        in_specs=[HBM if n in held else VMEM for n in range(len(operands))],
        out_specs=(VMEM,) * len(outs),
        scratch_shapes=scratch,
        compiler_params=pltpu.CompilerParams(vmem_limit_bytes=limit),
    )(*[
        pltpu.with_memory_space_constraint(x, pltpu.HBM) if n in held else x
        for n, x in enumerate(operands)
    ])


def wide(column):
    return jnp.broadcast_to(column, (column.shape[0], LANES))


def pair_bias(rows, distance):
    row = lax.broadcasted_iota(jnp.int32, (rows, rows), 0)
    col = lax.broadcasted_iota(jnp.int32, (rows, rows), 1)
    behind = row - col + distance * rows
    times = jnp.zeros((rows, rows), jnp.int32)
    for dilation in DILATIONS:
        read = (behind >= 0) & (behind <= KEYS_BEHIND * dilation)
        read = read & ((behind & (dilation - 1)) == 0)
        times = times + read.astype(jnp.int32)
    return jnp.where(
        times == 0,
        MASKED,
        jnp.where(times == 3, math.log2(3.0), (times - 1).astype(jnp.float32)),
    )


def sums_of(hidden, gain, weights, offsets):
    me = lax.axis_index("tp")
    sums = [None] * len(weights)
    squares = None
    for block, k in zip(hidden, offsets):
        piece = block.shape[1]
        source = me ^ k
        raw = block[...].astype(jnp.float32)
        scaled = (raw * gain[pl.ds(source, 1), :]).astype(jnp.bfloat16)
        part = jnp.sum(raw * raw, axis=1, keepdims=True)
        squares = part if squares is None else squares + part
        at = pl.ds(pl.multiple_of(source * piece, piece), piece)
        for n, weight in enumerate(weights):
            product = jnp.dot(scaled, weight[at, :], preferred_element_type=jnp.float32)
            sums[n] = product if sums[n] is None else sums[n] + product
    return sums, squares


def first_kernel(*refs, count, kinds, pieces, columns):
    own = refs[0]
    others = refs[1:count]
    gain = refs[count]
    small = refs[count + 1 : count + 3]
    weights = refs[count + 3 : count + 3 + kinds]
    w_out = refs[count + 3 + kinds]
    outs = refs[count + 4 + kinds : -2]
    held, sems = refs[-2:]
    sums_out, outs = outs[: kinds + 1], outs[kinds + 1 :]
    small_out, outs = outs[:2], outs[2:]
    weights_out, outs = outs[:kinds], outs[kinds:]
    pieces_out, biases = outs[: len(pieces)], outs[len(pieces) :]
    me = lax.axis_index("tp")
    moves = [(own, held), *zip(weights, weights_out), *zip(small, small_out)]
    for (k, start), out in zip(pieces, pieces_out):
        peer = me ^ (3 - lax.axis_index("grp") if k is None else k)
        at = pl.ds(pl.multiple_of(peer * columns, columns), columns)
        moves.append((w_out.at[pl.ds(start, out.shape[0]), at], out))
    moves = [pltpu.make_async_copy(src, dst, sems.at[n]) for n, (src, dst) in enumerate(moves)]
    for move in moves:
        move.start()
    for d, out in enumerate(biases):
        out[...] = pair_bias(out.shape[0], d)
    for move in moves[: kinds + 1]:
        move.wait()
    sums, squares = sums_of((held, *others), gain, weights_out, range(count))
    for out, total in zip(sums_out, sums):
        out[...] = total
    sums_out[kinds][...] = wide(squares)
    for move in moves[kinds + 1 :]:
        move.wait()


def early_kernel(*refs, offsets, kinds, carried=False):
    count = len(offsets)
    hidden = refs[:count]
    gain = refs[count]
    weights = refs[count + 1 : count + 1 + kinds]
    prior, outs = refs[count + 1 + kinds : -kinds - 1], refs[-kinds - 1 :]
    sums, squares = sums_of(hidden, gain, weights, offsets)
    for n, total in enumerate((*sums, wide(squares))):
        outs[n][...] = total + prior[n][...] if carried else total


def head_turn(values, gains, cosine, sine):
    mean = jnp.mean(values * values, axis=1, keepdims=True)
    values = values * lax.rsqrt(mean + EPSILON) * gains
    return values * cosine + pltpu.roll(values, values.shape[1] // 2, 1) * sine


def late_kernel(*refs, offsets, kinds, width):
    count = len(offsets)
    hidden = refs[:count]
    gain = refs[count]
    weights = refs[count + 1 : count + 1 + kinds]
    rest = refs[count + 1 + kinds :]
    before = rest[:kinds]
    squares_before = rest[kinds]
    gains = rest[kinds + 1 : 2 * kinds]
    cosine, sine = rest[2 * kinds : 2 * kinds + 2]
    outs = rest[2 * kinds + 2 :]
    outs = [*outs[:-1], outs[-1].at[0], outs[-1].at[1]]
    sums, squares = sums_of(hidden, gain, weights, offsets)
    scale = lax.rsqrt((squares + squares_before[...]) / width + EPSILON)
    head_width = gains[0].shape[1]
    turn_c = jnp.concatenate([cosine[...], cosine[...]], axis=1)
    turn_s = jnp.concatenate([-sine[...], sine[...]], axis=1)
    for n in range(kinds):
        for start in range(0, sums[n].shape[1], head_width):
            lanes = slice(start, start + head_width)
            h = start // head_width
            values = (sums[n][:, lanes] + before[n][:, lanes]) * scale
            if n < kinds - 1:
                values = head_turn(values, gains[n][h : h + 1, :], turn_c, turn_s)
            outs[n][:, lanes] = values.astype(jnp.bfloat16)


def softmax_part(q, blocks, lanes, factor):
    scores = []
    for kv, bias in blocks:
        product = lax.dot_general(
            q[:, lanes], kv[0, :, lanes], (((1,), (1,)), ((), ())),
            preferred_element_type=jnp.float32,
        )
        scores.append(product * factor + bias)
    top = functools.reduce(jnp.maximum, [jnp.max(s, axis=1, keepdims=True) for s in scores])
    total = None
    acc = None
    for s, (kv, _) in zip(scores, blocks):
        weights = jnp.exp2(s - top)
        part = jnp.sum(weights, axis=1, keepdims=True)
        out = jnp.dot(
            weights.astype(jnp.bfloat16), kv[1, :, lanes], preferred_element_type=jnp.float32
        )
        total = part if total is None else total + part
        acc = out if acc is None else acc + out
    return top, total, acc


def merge(parts):
    top = functools.reduce(jnp.maximum, [part[0] for part in parts])
    total = None
    acc = None
    for part_top, part_total, part_acc in parts:
        decay = jnp.exp2(part_top - top)
        total = part_total * decay if total is None else total + part_total * decay
        acc = part_acc * decay if acc is None else acc + part_acc * decay
    return acc / total, top + jnp.log2(total)


def head_lanes(q, head_width):
    count = q.shape[1] // head_width
    return [slice(h * head_width, (h + 1) * head_width) for h in range(count)]


def near_kernel(q, *refs, distances, head_width, factor):
    count = len(distances)
    tops, totals, accs = refs[2 * count :]
    for lanes in head_lanes(q, head_width):
        blocks = []
        for n, d in enumerate(distances):
            bias = refs[2 * n + 1][...]
            blocks.append((refs[2 * n], jnp.where(lax.axis_index("sp") >= d, bias, MASKED) if d else bias))
        top, total, acc = softmax_part(q, blocks, lanes, factor)
        tops[:, lanes] = wide(top)
        totals[:, lanes] = wide(total)
        accs[:, lanes] = acc


def help_kernel(q, *refs, blocks, head_width, factor):
    out, logs = refs[2 * blocks :]

    for h, lanes in enumerate(head_lanes(q, head_width)):
        ready = [(refs[2 * n], refs[2 * n + 1][...]) for n in range(blocks)]
        top, total, acc = softmax_part(q, ready, lanes, factor)
        out[:, lanes] = (acc / total).astype(jnp.bfloat16)
        logs[h : h + 1, :] = wide(top + jnp.log2(total)).T[:1, :]


def late_help_kernel(*refs, late_count, late, help_now, helper):
    late_in, rest = refs[:late_count], refs[late_count:]
    q, kv, bias, bias_before = rest[:4]
    kv_before, out, logs = rest[4:]

    @pl.when(lax.axis_index("sp") == helper)
    def _():
        late(*late_in, kv_before)
        help_now(q, kv, bias, kv_before, bias_before, out, logs)


def near_late_kernel(q, kv, bias, kv_helper, bias_before, *refs, late, near, helper):
    late_in, outs, held = refs[:-4], refs[-4:-1], refs[-1]
    ready = lax.axis_index("sp") == helper

    @pl.when(ready)
    def _():
        near(q, kv, bias, kv_helper, bias_before, *outs)

    @pl.when(jnp.logical_not(ready))
    def _():
        late(*late_in, held)
        near(q, kv, bias, held, bias_before, *outs)


def final_kernel(q, *refs, far, only, helped, head_width, factor):
    shard = lax.axis_index("sp")
    near = refs[:3]
    kvs = refs[3 : 3 + 2 * len(far)]
    given = refs[3 + 2 * len(far) : -2]
    attended, logs = refs[-2:]
    rows = q.shape[0]

    def finish(use_far, use_given):
        for h, lanes in enumerate(head_lanes(q, head_width)):
            parts = [tuple(ref[:, lanes] for ref in near)]
            if use_far:
                blocks = [
                    (kvs[2 * n], jnp.where(shard >= d, kvs[2 * n + 1][...], MASKED))
                    for n, d in enumerate(far)
                ]
                top, total, acc = softmax_part(q, blocks, lanes, factor)
                parts.append((wide(top), wide(total), acc))
            if use_given:
                top = jnp.broadcast_to(given[1][h : h + 1, :], (LANES, rows)).T
                parts.append((top, jnp.ones_like(top), given[0][:, lanes].astype(jnp.float32)))
            out, log_sum = merge(parts)
            attended[:, lanes] = out.astype(jnp.bfloat16)
            logs[:, lanes] = log_sum

    with_far = (shard == only) if only is not None else (shard >= 2)
    with_given = (shard == helped) if helped is not None else (shard < 0)
    if far:
        pl.when(with_far)(lambda: finish(True, False))
    if helped is not None:
        pl.when(with_given)(lambda: finish(False, True))
    pl.when(jnp.logical_not(with_far | with_given))(lambda: finish(False, False))


def products(blocks, pieces):
    total = None
    for block, piece in zip(blocks, pieces):
        product = jnp.dot(block[...], piece[...], preferred_element_type=jnp.float32)
        total = product if total is None else total + product
    return total


def mix_early_kernel(logs, *refs, count):
    total, rows = refs[2 * count :]
    total[...] = products(refs[:count], refs[count : 2 * count])
    for h in range(rows.shape[0]):
        lanes = slice(h * LANES, (h + 1) * LANES)
        rows[h : h + 1, :] = (logs[:, lanes] * math.log(2.0)).T[:1, :]


def mix_late_kernel(before, *refs, count, shared):
    blocks = [ref[...] for ref in refs[:count]]
    if shared:
        crossed = lax.axis_index("grp") == 0
        low, high = blocks
        blocks = [jnp.where(crossed, high, low), jnp.where(crossed, low, high)]
        halves = [ref[...] for ref in refs[count:-1]]
        pieces = [jnp.concatenate(halves[:2], axis=0), jnp.concatenate(halves[2:], axis=0)]
    else:
        pieces = refs[count : 2 * count]
    total = before[...] + products(blocks, pieces)
    refs[-1][...] = total.astype(jnp.bfloat16)


def swap(value, distance):
    count = lax.axis_size("tp")
    return lax.ppermute(value, "tp", [(i, i ^ distance) for i in range(count)])


def send(value, pairs):
    return lax.ppermute(value, "sp", pairs)


def behind(value, steps):
    count = lax.axis_size("sp")
    return send(value, [(s, s + steps) for s in range(count - steps)])


def near_blocks(block):
    blocks = {0: block}
    distance = lax.axis_size("tp") // 4
    while distance:
        for k in list(blocks):
            blocks[k ^ distance] = swap(blocks[k], distance)
        distance //= 2
    return [blocks[k] for k in sorted(blocks)]


def turn_tables(positions, head_width):
    inverse = ROTARY_BASE ** (-jnp.arange(0, head_width, 2, dtype=jnp.float32) / head_width)
    angles = positions[:, None] * inverse[None, :]
    return jnp.cos(angles), jnp.sin(angles)


def layer(hidden, norm_gain, w_query, w_key, w_value, query_gain, key_gain, w_out):
    rows, piece = hidden.shape
    head_count, head_width = query_gain.shape
    local_width = head_count * head_width
    count = lax.axis_size("tp")
    shards = lax.axis_size("sp")
    half = count // 2
    shard = lax.axis_index("sp")
    factor = head_width ** (-0.5) * LOG2_E
    reach = -(-KEYS_BEHIND * DILATIONS[-1] // rows)
    distances = list(range(min(shards - 1, reach) + 1))
    helped = shards - 1 if shards == 4 and reach >= shards - 1 else None
    far = [2] if helped is not None else distances[2:]

    first = shard * rows
    steps = jnp.arange(rows, dtype=jnp.int32)
    tables = turn_tables((steps + first).astype(jnp.float32), head_width)
    tables_before = turn_tables((steps + first - rows).astype(jnp.float32), head_width)
    gain = norm_gain.astype(jnp.float32).reshape(count, piece)
    gains = (query_gain, key_gain)
    weights = (w_query, w_key, w_value)
    sums = shape_of((rows, local_width), jnp.float32)
    half_sum = shape_of((rows, local_width), jnp.bfloat16)
    pair = shape_of((2, rows, local_width), jnp.bfloat16)
    lane_wide = shape_of((rows, LANES), jnp.float32)
    square = shape_of((rows, rows), jnp.float32)
    early = tuple(range(half))
    late = tuple(range(half, count))
    columns = w_out.shape[1] // count
    copies = lax.axis_size("grp")
    shared = copies == 2 and count == 4

    cut = w_out.shape[0] // 2 if shared else w_out.shape[0]
    piece_keys = tuple((k, 0) for k in range(half))
    piece_keys += ((None, 0), (None, cut)) if shared else tuple((k, 0) for k in late)
    piece_shapes = [shape_of((w_out.shape[0], columns), w_out.dtype)] * half
    piece_shapes += [shape_of((cut, columns), w_out.dtype)] * (len(piece_keys) - half)
    across = swap(hidden, half)
    before = behind(hidden, 1)
    own_near = near_blocks(hidden)

    operands = [*own_near, gain, *gains, *weights, w_out]
    fixed = [0, *range(half + 1, len(operands))]
    moves = len(weights) + 3 + len(piece_keys)
    begun = call(
        functools.partial(first_kernel, count=half, kinds=3, pieces=piece_keys, columns=columns),
        operands,
        [sums] * 3
        + [lane_wide]
        + [shape_of(x.shape, x.dtype) for x in (*gains, *weights)]
        + piece_shapes
        + [square] * len(distances),
        held=fixed,
        scratch=[pltpu.VMEM(hidden.shape, hidden.dtype), pltpu.SemaphoreType.DMA((moves,))],
    )
    begun, rest = begun[:4], begun[4:]
    gains, weights, rest = rest[:2], rest[2:5], rest[5:]
    slices, biases = rest[: len(piece_keys)], rest[len(piece_keys) :]
    own_slice, near_slice, far_slice = slices[0], slices[1:half], slices[half:]

    own_far = near_blocks(across)
    before_across = swap(before, half)
    width = piece * count
    q, kv = call(
        functools.partial(late_kernel, offsets=late, kinds=3, width=width),
        [*own_far, gain, *weights, *begun, *gains, *tables],
        [half_sum, pair],
    )

    if helped is not None:
        visitor = send(q, [(helped, 1)])
        far_blocks = [(send(kv, [(0, 2)]), biases[2])]
    else:
        far_blocks = [(behind(kv, d), biases[d]) for d in far]

    begun_before = call(
        functools.partial(early_kernel, offsets=early, kinds=2),
        [*near_blocks(before), gain, *weights[1:]],
        [sums] * 2 + [lane_wide],
    )
    before_far = near_blocks(before_across)
    begun_before = call(
        functools.partial(early_kernel, offsets=late[:1], kinds=2, carried=True),
        [before_far[0], gain, *weights[1:], *begun_before],
        [sums] * 2 + [lane_wide],
    )
    operands = [*before_far[1:], gain, *weights[1:], *begun_before, gains[1], *tables_before]
    late_before = functools.partial(late_kernel, offsets=late[1:], kinds=2, width=width)
    given = []
    if helped is None:
        (kv_before,) = call(late_before, operands, [pair])
    else:
        kv_before, out, logs = call(
            functools.partial(
                late_help_kernel,
                late_count=len(operands),
                helper=1,
                late=late_before,
                help_now=functools.partial(
                    help_kernel, blocks=2, head_width=head_width, factor=factor
                ),
            ),
            [*operands, visitor, kv, biases[2], biases[3]],
            [pair, half_sum, shape_of((8, rows), jnp.float32)],
        )
        given = [send(out, [(1, helped)]), send(logs, [(1, helped)])]
    near_part = functools.partial(
        near_kernel, distances=(0, 1), head_width=head_width, factor=factor
    )
    near_in = [q, kv, biases[0], kv_before, biases[1]]
    if helped is None:
        near = call(near_part, near_in, [sums] * 3)
    else:
        near = call(
            functools.partial(near_late_kernel, late=late_before, near=near_part, helper=1),
            [*near_in, *operands],
            [sums] * 3,
            scratch=[pltpu.VMEM(pair.shape, pair.dtype)],
        )

    near_pieces = [own_slice] + [swap(x, k + 1) for k, x in enumerate(near_slice)]
    if shared:
        routes = [(g * 4 + t, g * 4 + (t ^ (3 - g))) for g in range(2) for t in range(4)]
        first_half = lax.ppermute(far_slice[0], ("grp", "tp"), routes)
        first_other = lax.ppermute(first_half, "grp", [(0, 1), (1, 0)])
        last_half = lax.ppermute(far_slice[1], ("grp", "tp"), routes)
    else:
        far_pieces = [swap(x, k) for k, x in zip(late, far_slice)]

    attended, logs = call(
        functools.partial(
            final_kernel,
            far=tuple(far),
            only=2 if helped is not None else None,
            helped=helped,
            head_width=head_width,
            factor=factor,
        ),
        [q, *near, *[x for block in far_blocks for x in block], *given],
        [half_sum, sums],
    )
    attended_across = swap(attended, half)
    if shared:
        later, _ = lax.optimization_barrier((last_half, logs))
        last_other = lax.ppermute(later, "grp", [(0, 1), (1, 0)])
        far_pieces = [first_half, last_half, first_other, last_other]
    mixed_shape = (rows, columns)
    partial_mix, log_rows = call(
        functools.partial(mix_early_kernel, count=half),
        [logs, *near_blocks(attended), *near_pieces],
        [shape_of(mixed_shape, jnp.float32), shape_of((head_count, rows), jnp.float32)],
    )
    (mixed,) = call(
        functools.partial(mix_late_kernel, count=half, shared=shared),
        [partial_mix, *near_blocks(attended_across), *far_pieces],
        [shape_of(mixed_shape, jnp.bfloat16)],
    )
    return mixed, log_rows.T


def solution(mesh):
    placed = (
        P(("grp", "sp"), "tp"),
        P(),
        P(None, "tp"),
        P(None, "tp"),
        P(None, "tp"),
        P("tp", None),
        P("tp", None),
        P("tp", None),
    )
    return jax.shard_map(
        layer,
        mesh=mesh,
        in_specs=placed,
        out_specs=(P(("grp", "sp"), "tp"), P(("grp", "sp"), "tp")),
        check_vma=False,
    )
```

```python
import functools
import math

import jax
import jax.numpy as jnp
from jax import lax
from jax.experimental import pallas as pl
from jax.experimental.pallas import tpu as pltpu
from jax.sharding import PartitionSpec as P


KEYS_BEHIND = 128
DILATIONS = (1, 4, 16)
EPSILON = 1e-06
ROTARY_BASE = 500000.0
MASKED = -1e30
LANES = 128
LOG2_E = math.log2(math.e)


VMEM = pl.BlockSpec(memory_space=pltpu.VMEM)
HBM = pl.BlockSpec(memory_space=pltpu.HBM)


def shape_of(shape, dtype):
    return jax.ShapeDtypeStruct(shape, dtype)


def call(body, operands, outs, held=(), scratch=(), limit=24 << 20):
    return pl.pallas_call(
        body,
        out_shape=tuple(outs),
        in_specs=[HBM if n in held else VMEM for n in range(len(operands))],
        out_specs=(VMEM,) * len(outs),
        scratch_shapes=scratch,
        compiler_params=pltpu.CompilerParams(vmem_limit_bytes=limit),
    )(*[
        pltpu.with_memory_space_constraint(x, pltpu.HBM) if n in held else x
        for n, x in enumerate(operands)
    ])


def wide(column):
    return jnp.broadcast_to(column, (column.shape[0], LANES))


def pair_bias(rows, distance):
    row = lax.broadcasted_iota(jnp.int32, (rows, rows), 0)
    col = lax.broadcasted_iota(jnp.int32, (rows, rows), 1)
    behind = row - col + distance * rows
    times = jnp.zeros((rows, rows), jnp.int32)
    for dilation in DILATIONS:
        read = (behind >= 0) & (behind <= KEYS_BEHIND * dilation)
        read = read & ((behind & (dilation - 1)) == 0)
        times = times + read.astype(jnp.int32)
    return jnp.where(
        times == 0,
        MASKED,
        jnp.where(times == 3, math.log2(3.0), (times - 1).astype(jnp.float32)),
    )


def sums_of(hidden, gain, weights, offsets):
    me = lax.axis_index("tp")
    sums = [None] * len(weights)
    squares = None
    for block, k in zip(hidden, offsets):
        piece = block.shape[1]
        source = me ^ k
        raw = block[...].astype(jnp.float32)
        scaled = (raw * gain[pl.ds(source, 1), :]).astype(jnp.bfloat16)
        part = jnp.sum(raw * raw, axis=1, keepdims=True)
        squares = part if squares is None else squares + part
        at = pl.ds(pl.multiple_of(source * piece, piece), piece)
        for n, weight in enumerate(weights):
            product = jnp.dot(scaled, weight[at, :], preferred_element_type=jnp.float32)
            sums[n] = product if sums[n] is None else sums[n] + product
    return sums, squares


def first_kernel(*refs, count, kinds, pieces, columns):
    own = refs[0]
    others = refs[1:count]
    gain = refs[count]
    small = refs[count + 1 : count + 3]
    weights = refs[count + 3 : count + 3 + kinds]
    w_out = refs[count + 3 + kinds]
    outs = refs[count + 4 + kinds : -2]
    held, sems = refs[-2:]
    sums_out, outs = outs[: kinds + 1], outs[kinds + 1 :]
    small_out, outs = outs[:2], outs[2:]
    weights_out, outs = outs[:kinds], outs[kinds:]
    pieces_out, biases = outs[: len(pieces)], outs[len(pieces) :]
    me = lax.axis_index("tp")
    moves = [(own, held), *zip(weights, weights_out), *zip(small, small_out)]
    for (k, start), out in zip(pieces, pieces_out):
        peer = me ^ (3 - lax.axis_index("grp") if k is None else k)
        at = pl.ds(pl.multiple_of(peer * columns, columns), columns)
        moves.append((w_out.at[pl.ds(start, out.shape[0]), at], out))
    moves = [pltpu.make_async_copy(src, dst, sems.at[n]) for n, (src, dst) in enumerate(moves)]
    for move in moves:
        move.start()
    for d, out in enumerate(biases):
        out[...] = pair_bias(out.shape[0], d)
    for move in moves[: kinds + 1]:
        move.wait()
    sums, squares = sums_of((held, *others), gain, weights_out, range(count))
    for out, total in zip(sums_out, sums):
        out[...] = total
    sums_out[kinds][...] = wide(squares)
    for move in moves[kinds + 1 :]:
        move.wait()


def early_kernel(*refs, offsets, kinds):
    count = len(offsets)
    hidden = refs[:count]
    gain = refs[count]
    weights = refs[count + 1 : count + 1 + kinds]
    outs = refs[count + 1 + kinds :]
    sums, squares = sums_of(hidden, gain, weights, offsets)
    for out, total in zip(outs[:kinds], sums):
        out[...] = total
    outs[kinds][...] = wide(squares)


def head_turn(values, gains, cosine, sine):
    mean = jnp.mean(values * values, axis=1, keepdims=True)
    values = values * lax.rsqrt(mean + EPSILON) * gains
    return values * cosine + pltpu.roll(values, values.shape[1] // 2, 1) * sine


def late_kernel(*refs, offsets, kinds, width):
    count = len(offsets)
    hidden = refs[:count]
    gain = refs[count]
    weights = refs[count + 1 : count + 1 + kinds]
    rest = refs[count + 1 + kinds :]
    before = rest[:kinds]
    squares_before = rest[kinds]
    gains = rest[kinds + 1 : 2 * kinds]
    cosine, sine = rest[2 * kinds : 2 * kinds + 2]
    outs = rest[2 * kinds + 2 :]
    outs = [*outs[:-1], outs[-1].at[0], outs[-1].at[1]]
    sums, squares = sums_of(hidden, gain, weights, offsets)
    scale = lax.rsqrt((squares + squares_before[...]) / width + EPSILON)
    head_width = gains[0].shape[1]
    turn_c = jnp.concatenate([cosine[...], cosine[...]], axis=1)
    turn_s = jnp.concatenate([-sine[...], sine[...]], axis=1)
    for n in range(kinds):
        for start in range(0, sums[n].shape[1], head_width):
            lanes = slice(start, start + head_width)
            h = start // head_width
            values = (sums[n][:, lanes] + before[n][:, lanes]) * scale
            if n < kinds - 1:
                values = head_turn(values, gains[n][h : h + 1, :], turn_c, turn_s)
            outs[n][:, lanes] = values.astype(jnp.bfloat16)


def softmax_part(q, blocks, lanes, factor):
    scores = []
    for kv, bias in blocks:
        product = lax.dot_general(
            q[:, lanes], kv[0, :, lanes], (((1,), (1,)), ((), ())),
            preferred_element_type=jnp.float32,
        )
        scores.append(product * factor + bias)
    top = functools.reduce(jnp.maximum, [jnp.max(s, axis=1, keepdims=True) for s in scores])
    total = None
    acc = None
    for s, (kv, _) in zip(scores, blocks):
        weights = jnp.exp2(s - top)
        part = jnp.sum(weights, axis=1, keepdims=True)
        out = jnp.dot(
            weights.astype(jnp.bfloat16), kv[1, :, lanes], preferred_element_type=jnp.float32
        )
        total = part if total is None else total + part
        acc = out if acc is None else acc + out
    return top, total, acc


def merge(parts):
    top = functools.reduce(jnp.maximum, [part[0] for part in parts])
    total = None
    acc = None
    for part_top, part_total, part_acc in parts:
        decay = jnp.exp2(part_top - top)
        total = part_total * decay if total is None else total + part_total * decay
        acc = part_acc * decay if acc is None else acc + part_acc * decay
    return acc / total, top + jnp.log2(total)


def head_lanes(q, head_width):
    count = q.shape[1] // head_width
    return [slice(h * head_width, (h + 1) * head_width) for h in range(count)]


def near_kernel(q, *refs, distances, head_width, factor):
    count = len(distances)
    tops, totals, accs = refs[2 * count :]
    for lanes in head_lanes(q, head_width):
        blocks = []
        for n, d in enumerate(distances):
            bias = refs[2 * n + 1][...]
            blocks.append((refs[2 * n], jnp.where(lax.axis_index("sp") >= d, bias, MASKED) if d else bias))
        top, total, acc = softmax_part(q, blocks, lanes, factor)
        tops[:, lanes] = wide(top)
        totals[:, lanes] = wide(total)
        accs[:, lanes] = acc


def help_kernel(q, *refs, blocks, head_width, factor):
    out, logs = refs[2 * blocks :]

    for h, lanes in enumerate(head_lanes(q, head_width)):
        ready = [(refs[2 * n], refs[2 * n + 1][...]) for n in range(blocks)]
        top, total, acc = softmax_part(q, ready, lanes, factor)
        out[:, lanes] = (acc / total).astype(jnp.bfloat16)
        logs[h : h + 1, :] = wide(top + jnp.log2(total)).T[:1, :]


def late_help_kernel(*refs, late_count, late, help_now, helper):
    late_in, rest = refs[:late_count], refs[late_count:]
    q, kv, bias, bias_before = rest[:4]
    kv_before, out, logs = rest[4:]

    @pl.when(lax.axis_index("sp") == helper)
    def _():
        late(*late_in, kv_before)
        help_now(q, kv, bias, kv_before, bias_before, out, logs)


def near_late_kernel(q, kv, bias, kv_helper, bias_before, *refs, late, near, helper):
    late_in, outs, held = refs[:-4], refs[-4:-1], refs[-1]
    ready = lax.axis_index("sp") == helper

    @pl.when(ready)
    def _():
        near(q, kv, bias, kv_helper, bias_before, *outs)

    @pl.when(jnp.logical_not(ready))
    def _():
        late(*late_in, held)
        near(q, kv, bias, held, bias_before, *outs)


def final_kernel(q, *refs, far, only, helped, head_width, factor):
    shard = lax.axis_index("sp")
    near = refs[:3]
    kvs = refs[3 : 3 + 2 * len(far)]
    given = refs[3 + 2 * len(far) : -2]
    attended, logs = refs[-2:]
    rows = q.shape[0]

    def finish(use_far, use_given):
        for h, lanes in enumerate(head_lanes(q, head_width)):
            parts = [tuple(ref[:, lanes] for ref in near)]
            if use_far:
                blocks = [
                    (kvs[2 * n], jnp.where(shard >= d, kvs[2 * n + 1][...], MASKED))
                    for n, d in enumerate(far)
                ]
                top, total, acc = softmax_part(q, blocks, lanes, factor)
                parts.append((wide(top), wide(total), acc))
            if use_given:
                top = jnp.broadcast_to(given[1][h : h + 1, :], (LANES, rows)).T
                parts.append((top, jnp.ones_like(top), given[0][:, lanes].astype(jnp.float32)))
            out, log_sum = merge(parts)
            attended[:, lanes] = out.astype(jnp.bfloat16)
            logs[:, lanes] = log_sum

    with_far = (shard == only) if only is not None else (shard >= 2)
    with_given = (shard == helped) if helped is not None else (shard < 0)
    if far:
        pl.when(with_far)(lambda: finish(True, False))
    if helped is not None:
        pl.when(with_given)(lambda: finish(False, True))
    pl.when(jnp.logical_not(with_far | with_given))(lambda: finish(False, False))


def products(blocks, pieces):
    total = None
    for block, piece in zip(blocks, pieces):
        product = jnp.dot(block[...], piece[...], preferred_element_type=jnp.float32)
        total = product if total is None else total + product
    return total


def mix_early_kernel(logs, *refs, count):
    total, rows = refs[2 * count :]
    total[...] = products(refs[:count], refs[count : 2 * count])
    for h in range(rows.shape[0]):
        lanes = slice(h * LANES, (h + 1) * LANES)
        rows[h : h + 1, :] = (logs[:, lanes] * math.log(2.0)).T[:1, :]


def mix_late_kernel(before, *refs, count, shared):
    blocks = [ref[...] for ref in refs[:count]]
    if shared:
        crossed = lax.axis_index("grp") == 0
        low, high = blocks
        blocks = [jnp.where(crossed, high, low), jnp.where(crossed, low, high)]
        halves = [ref[...] for ref in refs[count:-1]]
        pieces = [jnp.concatenate(halves[:2], axis=0), jnp.concatenate(halves[2:], axis=0)]
    else:
        pieces = refs[count : 2 * count]
    total = before[...] + products(blocks, pieces)
    refs[-1][...] = total.astype(jnp.bfloat16)


def swap(value, distance):
    count = lax.axis_size("tp")
    return lax.ppermute(value, "tp", [(i, i ^ distance) for i in range(count)])


def send(value, pairs):
    return lax.ppermute(value, "sp", pairs)


def behind(value, steps):
    count = lax.axis_size("sp")
    return send(value, [(s, s + steps) for s in range(count - steps)])


def near_blocks(block):
    blocks = {0: block}
    distance = lax.axis_size("tp") // 4
    while distance:
        for k in list(blocks):
            blocks[k ^ distance] = swap(blocks[k], distance)
        distance //= 2
    return [blocks[k] for k in sorted(blocks)]


def turn_tables(positions, head_width):
    inverse = ROTARY_BASE ** (-jnp.arange(0, head_width, 2, dtype=jnp.float32) / head_width)
    angles = positions[:, None] * inverse[None, :]
    return jnp.cos(angles), jnp.sin(angles)


def layer(hidden, norm_gain, w_query, w_key, w_value, query_gain, key_gain, w_out):
    rows, piece = hidden.shape
    head_count, head_width = query_gain.shape
    local_width = head_count * head_width
    count = lax.axis_size("tp")
    shards = lax.axis_size("sp")
    half = count // 2
    shard = lax.axis_index("sp")
    factor = head_width ** (-0.5) * LOG2_E
    reach = -(-KEYS_BEHIND * DILATIONS[-1] // rows)
    distances = list(range(min(shards - 1, reach) + 1))
    helped = shards - 1 if shards == 4 and reach >= shards - 1 else None
    far = [2] if helped is not None else distances[2:]

    first = shard * rows
    steps = jnp.arange(rows, dtype=jnp.int32)
    tables = turn_tables((steps + first).astype(jnp.float32), head_width)
    tables_before = turn_tables((steps + first - rows).astype(jnp.float32), head_width)
    gain = norm_gain.astype(jnp.float32).reshape(count, piece)
    gains = (query_gain, key_gain)
    weights = (w_query, w_key, w_value)
    sums = shape_of((rows, local_width), jnp.float32)
    half_sum = shape_of((rows, local_width), jnp.bfloat16)
    pair = shape_of((2, rows, local_width), jnp.bfloat16)
    lane_wide = shape_of((rows, LANES), jnp.float32)
    square = shape_of((rows, rows), jnp.float32)
    early = tuple(range(half))
    late = tuple(range(half, count))
    columns = w_out.shape[1] // count
    copies = lax.axis_size("grp")
    shared = copies == 2 and count == 4

    cut = w_out.shape[0] * 3 // 8 if shared else w_out.shape[0]
    piece_keys = tuple((k, 0) for k in range(half))
    piece_keys += ((None, 0), (None, cut)) if shared else tuple((k, 0) for k in late)
    piece_shapes = [shape_of((w_out.shape[0], columns), w_out.dtype)] * half
    sizes = (cut, w_out.shape[0] - cut) if shared else (cut,) * len(late)
    piece_shapes += [shape_of((size, columns), w_out.dtype) for size in sizes]
    across = swap(hidden, half)
    before = behind(hidden, 1)
    own_near = near_blocks(hidden)

    operands = [*own_near, gain, *gains, *weights, w_out]
    fixed = [0, *range(half + 1, len(operands))]
    moves = len(weights) + 3 + len(piece_keys)
    begun = call(
        functools.partial(first_kernel, count=half, kinds=3, pieces=piece_keys, columns=columns),
        operands,
        [sums] * 3
        + [lane_wide]
        + [shape_of(x.shape, x.dtype) for x in (*gains, *weights)]
        + piece_shapes
        + [square] * len(distances),
        held=fixed,
        scratch=[pltpu.VMEM(hidden.shape, hidden.dtype), pltpu.SemaphoreType.DMA((moves,))],
    )
    begun, rest = begun[:4], begun[4:]
    gains, weights, rest = rest[:2], rest[2:5], rest[5:]
    slices, biases = rest[: len(piece_keys)], rest[len(piece_keys) :]
    own_slice, near_slice, far_slice = slices[0], slices[1:half], slices[half:]

    own_far = near_blocks(across)
    before_across = swap(before, half)
    width = piece * count
    q, kv = call(
        functools.partial(late_kernel, offsets=late, kinds=3, width=width),
        [*own_far, gain, *weights, *begun, *gains, *tables],
        [half_sum, pair],
    )

    if helped is not None:
        visitor = send(q, [(helped, 1)])
        far_blocks = [(send(kv, [(0, 2)]), biases[2])]
    else:
        far_blocks = [(behind(kv, d), biases[d]) for d in far]

    begun_before = call(
        functools.partial(early_kernel, offsets=early, kinds=2),
        [*near_blocks(before), gain, *weights[1:]],
        [sums] * 2 + [lane_wide],
    )
    before_far = near_blocks(before_across)
    operands = [*before_far, gain, *weights[1:], *begun_before, gains[1], *tables_before]
    late_before = functools.partial(late_kernel, offsets=late, kinds=2, width=width)
    given = []
    if helped is None:
        (kv_before,) = call(late_before, operands, [pair])
    else:
        kv_before, out, logs = call(
            functools.partial(
                late_help_kernel,
                late_count=len(operands),
                helper=1,
                late=late_before,
                help_now=functools.partial(
                    help_kernel, blocks=2, head_width=head_width, factor=factor
                ),
            ),
            [*operands, visitor, kv, biases[2], biases[3]],
            [pair, half_sum, shape_of((8, rows), jnp.float32)],
        )
        given = [send(out, [(1, helped)]), send(logs, [(1, helped)])]
    near_part = functools.partial(
        near_kernel, distances=(0, 1), head_width=head_width, factor=factor
    )
    near_in = [q, kv, biases[0], kv_before, biases[1]]
    if helped is None:
        near = call(near_part, near_in, [sums] * 3)
    else:
        near = call(
            functools.partial(near_late_kernel, late=late_before, near=near_part, helper=1),
            [*near_in, *operands],
            [sums] * 3,
            scratch=[pltpu.VMEM(pair.shape, pair.dtype)],
        )

    near_pieces = [own_slice] + [swap(x, k + 1) for k, x in enumerate(near_slice)]
    if shared:
        routes = [(g * 4 + t, g * 4 + (t ^ (3 - g))) for g in range(2) for t in range(4)]
        first_half = lax.ppermute(far_slice[0], ("grp", "tp"), routes)
        first_other = lax.ppermute(first_half, "grp", [(0, 1), (1, 0)])
        last_half = lax.ppermute(far_slice[1], ("grp", "tp"), routes)
    else:
        far_pieces = [swap(x, k) for k, x in zip(late, far_slice)]

    attended, logs = call(
        functools.partial(
            final_kernel,
            far=tuple(far),
            only=2 if helped is not None else None,
            helped=helped,
            head_width=head_width,
            factor=factor,
        ),
        [q, *near, *[x for block in far_blocks for x in block], *given],
        [half_sum, sums],
    )
    attended_across = swap(attended, half)
    if shared:
        later, _ = lax.optimization_barrier((last_half, logs))
        last_other = lax.ppermute(later, "grp", [(0, 1), (1, 0)])
        far_pieces = [first_half, last_half, first_other, last_other]
    mixed_shape = (rows, columns)
    partial_mix, log_rows = call(
        functools.partial(mix_early_kernel, count=half),
        [logs, *near_blocks(attended), *near_pieces],
        [shape_of(mixed_shape, jnp.float32), shape_of((head_count, rows), jnp.float32)],
    )
    (mixed,) = call(
        functools.partial(mix_late_kernel, count=half, shared=shared),
        [partial_mix, *near_blocks(attended_across), *far_pieces],
        [shape_of(mixed_shape, jnp.bfloat16)],
    )
    return mixed, log_rows.T


def solution(mesh):
    placed = (
        P(("grp", "sp"), "tp"),
        P(),
        P(None, "tp"),
        P(None, "tp"),
        P(None, "tp"),
        P("tp", None),
        P("tp", None),
        P("tp", None),
    )
    return jax.shard_map(
        layer,
        mesh=mesh,
        in_specs=placed,
        out_specs=(P(("grp", "sp"), "tp"), P(("grp", "sp"), "tp")),
        check_vma=False,
    )
```
